256 devices in a mesh: sp: 32 (over z, x), tp: 8 (over y, core).
Axes of the slice: x: 4, y: 4, z: 8, core: 2. Of those that a mesh axis runs over, the one named last changes fastest.
Arguments:
- upstream: bfloat16 [8192, 2048], P('sp'), may hold values from -6 to 6
- stream: bfloat16 [8192, 2048], P('sp'), may hold values from -10 to 10
- routes: int32 [8192, 2], P('sp'), may hold values from 0 to 31, all different within a row; in each aligned block of 256 rows (0 to 255, 256 to 511, ...) at most 32 rows name the same one
- route_weights: float32 [8192, 2], P('sp'), may hold values from 0.1 to 1
- glu_value: bfloat16 [8192, 512], P('sp', 'tp'), may hold values from -6 to 6
- glu_gate: bfloat16 [8192, 512], P('sp', 'tp'), may hold values from -10 to 10
- conv_taps: float32 [31, 512], P(None, 'tp'), may hold values from -1 to 1
- conv_saved: bfloat16 [8192, 512], P('sp', 'tp'), may hold values from -600 to 600
- out_proj: bfloat16 [2048, 512], P(None, 'tp'), may hold values from -0.25 to 0.25
- expert_gate: bfloat16 [32, 2048, 2048], P('sp', None, 'tp'), may hold values from -0.125 to 0.125
- expert_up: bfloat16 [32, 2048, 2048], P('sp', None, 'tp'), may hold values from -0.125 to 0.125
- expert_down: bfloat16 [32, 2048, 2048], P('sp', 'tp'), may hold values from -0.125 to 0.125
Outputs:
- grad_stream: bfloat16 [8192, 2048], P('sp', 'tp')
- grad_value: bfloat16 [8192, 512], P('sp', 'tp')
- grad_gate: bfloat16 [8192, 512], P('sp', 'tp')
- grad_out_proj: float32 [2048, 512], P('sp', 'tp')
- grad_expert_gate: float32 [32, 2048, 2048], P('sp', None, 'tp')
- grad_expert_up: float32 [32, 2048, 2048], P('sp', None, 'tp')
- grad_expert_down: float32 [32, 2048, 2048], P('sp', 'tp')
The draws below stay inside these ranges and needn't reach their ends.
Inputs may be any that keep to these rules, and one draw needn't show every extreme that they name: `routes`: each row names 2 different experts; among the 256 rows of one index of sp no expert is named more than 32 times, a bound that some block reaches.
All inputs are finite; a program needn't handle non-finite values.
Results may differ from the reference program's by a relative error of at most 0.014.
Values may be sent and summed in bfloat16 or wider, within the bound.
No kernel may reach another device: no remote copies, remote signals or barrier semaphores. Data moves between devices by JAX's collectives and lax.ppermute only.
A program may use at most 128 MiB of HBM per device.

```python
import math
from functools import partial
import jax
import jax.numpy as jnp
import numpy as np
from jax import lax

D = 2048
FF = 2048
CW = 512
KW = 31
TOPK = 2
TOK_DEV = 256
TOKENS = 8192
EXPERTS = 32
CAP = 32
N_SP = 32
N_TP = 8


def draw_conv_saved(key, part):
    key_values, key_rows = jax.random.split(key, 2)
    column_scale = 10.0 ** (jnp.arange(CW, dtype=jnp.float32) / CW)
    values = jnp.clip(jax.random.normal(key_values, (TOKENS, CW), jnp.float32), -4.0, 4.0)
    row_scale = jnp.exp(jax.random.uniform(key_rows, (TOKENS, 1), jnp.float32, 0.0, math.log(10.0)))
    result = values * column_scale[None, :] * row_scale
    return result.astype(jnp.bfloat16)


def raised(drawn, key, source, target, shards_of, factor):
    def block_of(axis_at):
        return (jnp.arange(drawn.shape[axis_at]) // (drawn.shape[axis_at] // shards_of)).reshape((-1,) + (1,) * (drawn.ndim - 1 - axis_at))

    first = jax.random.permutation(key, shards_of)[block_of(target)]
    other_side = (block_of(target) + shards_of // 2) % shards_of
    return jnp.where((block_of(source) == first) | (block_of(source) == other_side), factor * drawn, drawn)


def block_scale(stream_key, shape, pieces, least, largest):
    factor_of, own = 1.0, jax.random.fold_in(stream_key, 6)
    for dim, parts in pieces:
        heights = jnp.exp(jax.random.uniform(jax.random.fold_in(own, dim), (parts,), jnp.float32, least / len(pieces), largest / len(pieces)))
        factor_of = factor_of * jnp.repeat(heights, shape[dim] // parts).reshape([-1 if axis == dim else 1 for axis in range(len(shape))])
    return factor_of


def routed_block(stream_key, own, number, rows, count, top, reach, skew):
    order = jax.random.permutation(stream_key, count)
    packed, usual = load_shares(count, rows * top, reach, skew, True), load_shares(count, rows * top, reach, skew, False)
    places = jnp.arange(count)

    def named(sizes, offset_by):
        used = int((sizes > 0).sum())
        fixed = max(1, used // 4)
        moved = fixed + (places - fixed + offset_by * (used - fixed)) % max(1, count - fixed)
        return jnp.zeros((count,), jnp.int32).at[order[jnp.where(places < fixed, places, moved)]].set(jnp.asarray(sizes, jnp.int32))

    sizes = jnp.where(number % 4 == 0, named(packed, number // 4), named(usual, number - number // 4 - 1))
    mixed = jax.random.permutation(jax.random.fold_in(own, 3), count)
    source_of, receiver = mixed[0:count // 2 * 2:2], mixed[1:count // 2 * 2:2]
    slack = jnp.minimum(sizes[source_of] - 1, reach - sizes[receiver]) // 2
    slack = jnp.where((source_of == order[0]) | (receiver == order[0]) | (sizes[receiver] == 0), 0, jnp.maximum(slack, 0))
    moved = jax.random.randint(jax.random.fold_in(own, 4), (count // 2,), 0, 1 << 20) % (slack + 1)
    sizes = sizes.at[source_of].add(-moved).at[receiver].add(moved)
    items = jnp.searchsorted(jnp.cumsum(sizes), jnp.arange(rows * top), side="right").astype(jnp.int32)
    table = items.reshape(top, rows).T
    table = table[jax.random.permutation(jax.random.fold_in(own, 1), rows)]
    offset_by = jax.random.randint(jax.random.fold_in(own, 2), (rows, 1), 0, top)
    return jnp.take_along_axis(table, (jnp.arange(top)[None, :] + offset_by) % top, axis=1)


def load_shares(amount, total, most, lean, full):
    loads = [(1 << 20) // math.isqrt(standing ** lean) + 1 for standing in range(1, amount + 1)]
    largest = most if full else min(most, max(-(-total // amount), total * loads[0] // sum(loads)))
    least = 1 if total - largest >= amount - 1 else 0
    given, surplus = [largest] + [least] * (amount - 1), total - largest - least * (amount - 1)
    while surplus > 0:
        free = [i for i in range(1, amount) if given[i] < largest] or [i for i in range(1, amount) if given[i] < most]
        mass, left = sum([loads[i] for i in free]), surplus
        for i in free:
            more = min(most - given[i], max(1, left * loads[i] // mass), surplus)
            given[i] = given[i] + more
            surplus = surplus - more
    return np.array(given)


def bell_draw(rng, extent, deviation, limit, cuts=(), kind=jnp.bfloat16):
    entries = jax.random.normal(rng, extent, jnp.float32) * deviation
    if len(cuts) > 0:
        entries = block_scale(rng, extent, cuts, -0.22, 0.18) * entries
    return jnp.clip(entries, min=-limit, max=limit).astype(kind)


def heavy_noise(stream_key, shape, scale, most, cuts, heavy, kind=jnp.bfloat16):
    array = scale * jax.random.normal(stream_key, shape, jnp.float32)
    if cuts:
        array = array * block_scale(stream_key, shape, cuts, -0.22, 0.18)
    return jnp.clip(raised(array, jax.random.fold_in(stream_key, 3), *heavy), -most, most).astype(kind)


def setup_inputs(seed: int = 0) -> dict:
    seeds = jax.random.split(jax.random.key(seed), 13)
    upstream = heavy_noise(seeds[0], (TOKENS, D), 1.0, 6.0, ((0, 32),), (0, 1, 32, 2.75))
    stream = bell_draw(seeds[1], (TOKENS, D), 1.0, 10.0, ((0, 32),))
    routes_keys = jax.random.split(jax.random.fold_in(seeds[2], 1), TOKENS // TOK_DEV)
    routes_turns = jax.random.permutation(jax.random.fold_in(seeds[2], 3), TOKENS // TOK_DEV)
    routes = jax.vmap(lambda own, number: routed_block(jax.random.fold_in(seeds[2], 2), own, number, TOK_DEV, EXPERTS, TOPK, CAP, 2))(routes_keys, routes_turns).reshape((TOKENS, TOPK))
    route_weights = jnp.clip(0.1 + 0.9 * jax.random.uniform(seeds[3], (TOKENS, TOPK), jnp.float32) ** block_scale(seeds[3], (TOKENS, TOPK), ((0, 32),), -0.2, 0.2), 0.1, 1.0)
    glu_value = bell_draw(seeds[4], (TOKENS, CW), 1.0, 6.0, ((0, 32), (1, 8)))
    glu_gate = bell_draw(seeds[5], (TOKENS, CW), 2.0, 10.0, ((0, 32), (1, 8)))
    conv_taps = bell_draw(seeds[6], (KW, CW), KW ** -0.5, 1.0, ((1, 8),), jnp.float32)
    conv_saved = draw_conv_saved(jax.random.fold_in(seeds[12], 71), 0)
    out_proj = bell_draw(seeds[8], (D, CW), CW ** -0.5, 0.25, ((1, 8),))
    expert_gate = bell_draw(seeds[9], (EXPERTS, D, FF), D ** -0.5, 0.125, ((0, 32), (2, 8)))
    expert_up = bell_draw(seeds[10], (EXPERTS, D, FF), D ** -0.5, 0.125, ((0, 32), (2, 8)))
    expert_down = bell_draw(seeds[11], (EXPERTS, FF, D), FF ** -0.5, 0.125, ((0, 32), (1, 8)))
    return {"upstream": upstream, "stream": stream, "routes": routes, "route_weights": route_weights, "glu_value": glu_value, "glu_gate": glu_gate, "conv_taps": conv_taps, "conv_saved": conv_saved, "out_proj": out_proj, "expert_gate": expert_gate, "expert_up": expert_up, "expert_down": expert_down}


clamp_limit = 7.0
glu_alpha = 1.702
norm_eps = 1e-05

def contract_rows(left, right):
    return lax.dot_general(left, right, (((0,), (0,)), ((), ())), preferred_element_type=jnp.float32)

def times_transposed(left, right):
    return lax.dot_general(left, right, (((1,), (1,)), ((), ())), preferred_element_type=jnp.float32)

def block_slots(block_routes, expert_count, capacity):
    flat_routes = block_routes.reshape(-1).astype(jnp.int32)
    one_hot = (flat_routes[:, None] == jnp.arange(expert_count, dtype=jnp.int32)[None, :]).astype(jnp.int32)
    earlier = jnp.cumsum(one_hot, axis=0) - one_hot
    slot_index = lax.optimization_barrier(jnp.sum(earlier * one_hot, axis=1)).astype(jnp.int32)
    target = (flat_routes * capacity + slot_index).astype(jnp.int32)
    pair_count = flat_routes.shape[0]
    table = jnp.full((expert_count * capacity,), pair_count, jnp.int32).at[target].set(jnp.arange(pair_count, dtype=jnp.int32))
    return (target, table)

def gather_pairs(table, block_stream, block_upstream, block_weights, topk):
    token_of = table // topk
    zero_row = jnp.zeros((1, block_stream.shape[1]), jnp.bfloat16)
    stream_pad = jnp.concatenate([block_stream, zero_row], axis=0)
    upstream_pad = jnp.concatenate([block_upstream, zero_row], axis=0)
    weight_pad = jnp.concatenate([block_weights.reshape(-1), jnp.zeros((1,), jnp.float32)])
    send_rows = stream_pad[token_of]
    send_cot = (weight_pad[table][:, None] * upstream_pad[token_of].astype(jnp.float32)).astype(jnp.bfloat16)
    return (send_rows, send_cot)

def expert_backward(expert_rows, expert_cot, gate_weight, up_weight, down_weight):
    gate_pre = jnp.dot(expert_rows, gate_weight, preferred_element_type=jnp.float32)
    up_pre = jnp.dot(expert_rows, up_weight, preferred_element_type=jnp.float32)
    capped = jnp.minimum(gate_pre, clamp_limit)
    clipped = jnp.clip(up_pre, -clamp_limit, clamp_limit)
    gate_sigmoid = jax.nn.sigmoid(glu_alpha * capped)
    act = (capped * gate_sigmoid * (clipped + 1.0)).astype(jnp.bfloat16)
    grad_down = contract_rows(act, expert_cot)
    grad_act = times_transposed(expert_cot, down_weight)
    slope = gate_sigmoid + glu_alpha * capped * gate_sigmoid * (1.0 - gate_sigmoid)
    grad_gate_pre = jnp.where(gate_pre < clamp_limit, grad_act * (clipped + 1.0) * slope, 0.0).astype(jnp.bfloat16)
    grad_up_pre = jnp.where(jnp.abs(up_pre) < clamp_limit, grad_act * capped * gate_sigmoid, 0.0).astype(jnp.bfloat16)
    grad_gate = contract_rows(expert_rows, grad_gate_pre)
    grad_up = contract_rows(expert_rows, grad_up_pre)
    return (grad_gate, grad_up, grad_down, grad_gate_pre, grad_up_pre)

def one_expert(operands):
    expert_rows, expert_cot, gate_weight, up_weight, down_weight = operands
    grad_gate, grad_up, grad_down, grad_gate_pre, grad_up_pre = expert_backward(expert_rows, expert_cot, gate_weight, up_weight, down_weight)
    group_width = FF // N_TP
    gate_groups = grad_gate_pre.astype(jnp.float32).reshape(-1, N_TP, group_width)
    up_groups = grad_up_pre.astype(jnp.float32).reshape(-1, N_TP, group_width)
    gate_split = gate_weight.astype(jnp.float32).reshape(D, N_TP, group_width)
    up_split = up_weight.astype(jnp.float32).reshape(D, N_TP, group_width)
    partial_rows = jnp.einsum('rgf,dgf->grd', gate_groups, gate_split) + jnp.einsum('rgf,dgf->grd', up_groups, up_split)
    rounded = lax.optimization_barrier(partial_rows.astype(jnp.bfloat16))
    row_grad = lax.optimization_barrier(jnp.sum(rounded.astype(jnp.float32), axis=0)).astype(jnp.bfloat16)
    return (grad_gate, grad_up, grad_down, row_grad)

def take_rows(source_rows, target_rows):
    return source_rows[target_rows]

def reference(upstream, stream, routes, route_weights, glu_value, glu_gate, conv_taps, conv_saved, out_proj, expert_gate, expert_up, expert_down):
    block_routes = routes.reshape(N_SP, TOK_DEV, TOPK)
    targets, tables = jax.vmap(partial(block_slots, expert_count=EXPERTS, capacity=CAP))(block_routes)
    send_rows, send_cot = jax.vmap(partial(gather_pairs, topk=TOPK))(tables, stream.reshape(N_SP, TOK_DEV, D), upstream.reshape(N_SP, TOK_DEV, D), route_weights.reshape(N_SP, TOK_DEV, TOPK))
    expert_rows = send_rows.reshape(N_SP, EXPERTS, CAP, D).transpose(1, 0, 2, 3).reshape(EXPERTS, N_SP * CAP, D)
    expert_cot = send_cot.reshape(N_SP, EXPERTS, CAP, D).transpose(1, 0, 2, 3).reshape(EXPERTS, N_SP * CAP, D)
    grad_expert_gate, grad_expert_up, grad_expert_down, row_grads = lax.map(one_expert, (expert_rows, expert_cot, expert_gate, expert_up, expert_down))
    returned = row_grads.reshape(EXPERTS, N_SP, CAP, D).transpose(1, 0, 2, 3).reshape(N_SP, EXPERTS * CAP, D)
    pair_grads = jax.vmap(take_rows)(returned, targets)
    routed_sum = lax.optimization_barrier(jnp.sum(pair_grads.astype(jnp.float32).reshape(TOKENS, TOPK, D), axis=1))
    grad_stream = (upstream.astype(jnp.float32) + routed_sum).astype(jnp.bfloat16)
    saved_conv = conv_saved.astype(jnp.float32)
    mean_c = lax.optimization_barrier(jnp.mean(saved_conv, axis=1, keepdims=True))
    var_c = lax.optimization_barrier(jnp.mean(saved_conv * saved_conv, axis=1, keepdims=True)) - mean_c * mean_c
    inv_std = lax.rsqrt(var_c + norm_eps)
    normed = (saved_conv - mean_c) * inv_std
    norm_sigmoid = jax.nn.sigmoid(normed)
    mixed = (normed * norm_sigmoid).astype(jnp.bfloat16)
    grad_mixed = jnp.dot(grad_stream, out_proj, preferred_element_type=jnp.float32)
    grad_normed = grad_mixed * norm_sigmoid * (1.0 + normed * (1.0 - norm_sigmoid))
    first_mean = lax.optimization_barrier(jnp.mean(grad_normed, axis=1, keepdims=True))
    second_mean = lax.optimization_barrier(jnp.mean(grad_normed * normed, axis=1, keepdims=True))
    grad_conv = inv_std * (grad_normed - first_mean - normed * second_mean)
    padded = jnp.concatenate([grad_conv, jnp.zeros((KW - 1, CW), jnp.float32)], axis=0)
    grad_glu = jnp.zeros((TOKENS, CW), jnp.float32)
    for offset in range(KW):
        grad_glu = grad_glu + conv_taps[offset][None, :] * padded[offset:offset + TOKENS]
    gate_sig = jax.nn.sigmoid(glu_gate.astype(jnp.float32))
    grad_value = (grad_glu * gate_sig).astype(jnp.bfloat16)
    grad_gate = (grad_glu * glu_value.astype(jnp.float32) * gate_sig * (1.0 - gate_sig)).astype(jnp.bfloat16)
    grad_out_proj = contract_rows(grad_stream, mixed)
    return (grad_stream, grad_value, grad_gate, grad_out_proj, grad_expert_gate, grad_expert_up, grad_expert_down)
```

```python
import jax
import jax.numpy as jnp
from jax import lax
from jax.experimental import pallas as pl
from jax.experimental.pallas import tpu as pltpu
from jax.sharding import PartitionSpec as P

CLAMP = 7.0
ALPHA = 1.702
EPS = 1e-05
CW = 512
CAP = 32
HALF = 16
SP = 32
TP = 8
TOK = 256
ROWS = SP * HALF
BF = jnp.bfloat16
F32 = jnp.float32
MIB = 1 << 20


def dot(a, b, ca=1, cb=0):
    return lax.dot_general(a, b, (((ca,), (cb,)), ((), ())), preferred_element_type=F32)


def flag(mask):
    return jnp.where(mask, 1.0, 0.0)


def iota(shape, dim):
    return lax.broadcasted_iota(jnp.int32, shape, dim)


def call(body, out_shape, flops=0, limit=40, **kw):
    return pl.pallas_call(
        body,
        out_shape=out_shape,
        compiler_params=pltpu.CompilerParams(vmem_limit_bytes=limit * MIB),
        cost_estimate=pl.CostEstimate(flops=flops, bytes_accessed=MIB, transcendentals=0),
        **kw,
    )


def shape(dims, dtype):
    return jax.ShapeDtypeStruct(dims, dtype)


SMEM = pl.BlockSpec(memory_space=pltpu.SMEM)
VMEM = pl.BlockSpec(memory_space=pltpu.VMEM)


def pick_rows_body(t_ref, routes_ref, stream_ref, rows_ref, target_ref):
    core = t_ref[0] % 2
    r = routes_ref[...]
    r0, r1 = r[0:1, :], r[1:2, :]
    expert = iota((SP, TOK), 0)
    named0, named1 = expert == r0, expert == r1
    both = (flag(named0) + flag(named1)).astype(BF)
    before = flag(iota((TOK, TOK), 0) < iota((TOK, TOK), 1)).astype(BF)
    earlier = dot(both, before)
    slot0 = jnp.sum(jnp.where(named0, earlier, 0.0), axis=0, keepdims=True).astype(jnp.int32)
    slot1 = jnp.sum(jnp.where(named1, earlier, 0.0), axis=0, keepdims=True).astype(jnp.int32)
    l0 = jnp.where(slot0 // HALF == core, r0 * HALF + slot0 - HALF * core, -1)
    l1 = jnp.where(slot1 // HALF == core, r1 * HALF + slot1 - HALF * core, -1)
    b0 = r0 * CAP + (slot0 + HALF * core) % CAP
    b1 = r1 * CAP + (slot1 + HALF * core) % CAP
    target_ref[...] = jnp.concatenate([l0, l1, b0, b1, l0, l1, b0, b1], axis=0)
    place = iota((ROWS, TOK), 0)
    pick = flag((place == l0) | (place == l1)).astype(BF)
    rows_ref[...] = dot(pick, stream_ref[...]).astype(BF)


def pick_rows(tp, routes, stream):
    return call(
        pick_rows_body,
        (shape((ROWS, 512), BF), shape((8, TOK), jnp.int32)),
        grid_spec=pltpu.PrefetchScalarGridSpec(
            num_scalar_prefetch=1,
            grid=(1,),
            in_specs=[
                pl.BlockSpec((2, TOK), lambda i, t: (0, 0)),
                pl.BlockSpec((TOK, 512), lambda i, t: (0, t[0] // 2)),
            ],
            out_specs=[
                pl.BlockSpec((ROWS, 512), lambda i, t: (0, 0)),
                pl.BlockSpec((8, TOK), lambda i, t: (0, 0)),
            ],
        ),
        flops=10**9,
    )(tp, routes, stream)


def pick_cot_body(t_ref, target_ref, weights_ref, upstream_ref, cot_ref, back_ref):
    tgt = target_ref[...]
    w = weights_ref[...]
    table = jnp.concatenate(
        [tgt[2:4, :].astype(F32), w, tgt[2:4, :].astype(F32), w], axis=0
    )
    columns = jnp.transpose(jnp.concatenate([table] * 16, axis=0))
    up = upstream_ref[...].astype(F32)
    cot0 = (columns[:, 2:3] * up).astype(BF)
    cot1 = (columns[:, 3:4] * up).astype(BF)
    place = iota((ROWS, TOK), 0)
    cot = dot(flag(place == tgt[0:1, :]).astype(BF), cot0)
    cot = cot + dot(flag(place == tgt[1:2, :]).astype(BF), cot1)
    cot_ref[...] = cot.astype(BF)
    b0 = columns[:, 0:1].astype(jnp.int32)
    b1 = columns[:, 1:2].astype(jnp.int32)
    spot = iota((TOK, SP * CAP), 1)
    back_ref[...] = flag((spot == b0) | (spot == b1)).astype(BF)


def pick_cot(tp, target, weights, upstream):
    return call(
        pick_cot_body,
        (shape((ROWS, 512), BF), shape((TOK, SP * CAP), BF)),
        grid_spec=pltpu.PrefetchScalarGridSpec(
            num_scalar_prefetch=1,
            grid=(1,),
            in_specs=[
                pl.BlockSpec((8, TOK), lambda i, t: (0, 0)),
                pl.BlockSpec((2, TOK), lambda i, t: (0, 0)),
                pl.BlockSpec((TOK, 512), lambda i, t: (0, t[0] // 2)),
            ],
            out_specs=[
                pl.BlockSpec((ROWS, 512), lambda i, t: (0, 0)),
                pl.BlockSpec((TOK, SP * CAP), lambda i, t: (0, 0)),
            ],
        ),
        flops=10**9,
    )(tp, target, weights, upstream)


def quarters(t_ref):
    y = t_ref[0] // 2
    return y, (y + 3) % 4, (y + 1) % 4, (y + 2) % 4


def joined(refs):
    own, left, right, top, bottom = refs
    return (
        own[...],
        left[...],
        right[...],
        jnp.concatenate([top[...], bottom[...]], axis=0),
    )


def forward_body(t_ref, *refs):
    blocks, (g0, g1, u0, u1), (act_ref, a1_ref, a2_ref), (pg, pu) = (
        refs[0:5],
        refs[5:9],
        refs[9:12],
        refs[12:14],
    )
    q = quarters(t_ref)
    x = joined(blocks)
    for j, (g, u) in enumerate(((g0, u0), (g1, u1))):
        cols = slice(256 * j, 256 * j + 256)
        pg[:, cols] = sum(dot(x[i], g[q[i]]) for i in range(4))
        pu[:, cols] = sum(dot(x[i], u[q[i]]) for i in range(4))

    @pl.loop(0, ROWS // 32)
    def _(i):
        at = pl.ds(pl.multiple_of(i * 32, 32), 32)
        gate_pre, up_pre = pg[at, :], pu[at, :]
        capped = jnp.minimum(gate_pre, CLAMP)
        clipped = jnp.clip(up_pre, -CLAMP, CLAMP)
        sig = jax.nn.sigmoid(ALPHA * capped)
        gated = capped * sig
        act_ref[at, :] = (gated * (clipped + 1.0)).astype(BF)
        slope = sig + ALPHA * gated * (1.0 - sig)
        a1_ref[at, :] = jnp.where(gate_pre < CLAMP, (clipped + 1.0) * slope, 0.0)
        a2_ref[at, :] = jnp.where(jnp.abs(up_pre) < CLAMP, gated, 0.0)


def forward(tp, blocks, weights):
    return call(
        forward_body,
        (shape((ROWS, 512), BF), shape((ROWS, 512), F32), shape((ROWS, 512), F32)),
        in_specs=[SMEM] + [VMEM] * 9,
        out_specs=(VMEM,) * 3,
        scratch_shapes=[pltpu.VMEM((ROWS, 512), F32)] * 2,
        flops=2 * 10**9,
    )(tp, *blocks, *weights)


def partial_of(g, u, g0, g1, u0, u1, piece):
    return (
        dot(g[:, 0:256], g0[piece], 1, 1)
        + dot(g[:, 256:512], g1[piece], 1, 1)
        + dot(u[:, 0:256], u0[piece], 1, 1)
        + dot(u[:, 256:512], u1[piece], 1, 1)
    )


def backward_body(t_ref, *refs):
    blocks, (d0, d1, a1, a2, g0, g1, u0, u1) = refs[0:5], refs[5:13]
    (top_ref, bottom_ref, gg_ref, gu_ref), ga = refs[13:17], refs[17]
    q = quarters(t_ref)
    x = joined(blocks)
    for j, d in enumerate((d0, d1)):
        ga[:, 256 * j : 256 * j + 256] = sum(
            dot(x[i], d[:, pl.ds(pl.multiple_of(q[i] * 512, 512), 512)], 1, 1) for i in range(4)
        )

    @pl.loop(0, ROWS // 32)
    def _(i):
        at = pl.ds(pl.multiple_of(i * 32, 32), 32)
        grad = ga[at, :]
        gg_ref[at, :] = (grad * a1[at, :]).astype(BF)
        gu_ref[at, :] = (grad * a2[at, :]).astype(BF)

    g, u = gg_ref[...], gu_ref[...]
    for half in range(2):
        part = partial_of(g, u, g0, g1, u0, u1, 2 * q[3] + half).astype(BF)
        top_ref[half] = part[0:256]
        bottom_ref[half] = part[256:512]


def backward(tp, blocks, downs, a1, a2, weights):
    return call(
        backward_body,
        (
            shape((2, 256, 256), BF),
            shape((2, 256, 256), BF),
            shape((ROWS, 512), BF),
            shape((ROWS, 512), BF),
        ),
        in_specs=[SMEM] + [VMEM] * 13,
        out_specs=(VMEM,) * 4,
        scratch_shapes=[pltpu.VMEM((ROWS, 512), F32)],
        flops=2 * 10**9,
    )(tp, *blocks, *downs, a1, a2, *weights)


def near_body(t_ref, gg, gu, g0, g1, u0, u1, rs, rc, ls, lc, os, oc):
    t = t_ref[0]
    g, u = gg[...], gu[...]
    right, left = (t + 2) % 8, (t + 6) % 8
    for ref, piece in (
        (rs, right),
        (rc, right + 1 - 2 * (t % 2)),
        (ls, left),
        (lc, left + 1 - 2 * (t % 2)),
        (os, t),
        (oc, t + 1 - 2 * (t % 2)),
    ):
        ref[...] = partial_of(g, u, g0, g1, u0, u1, piece).astype(BF)


def near(tp, gg, gu, weights):
    return call(
        near_body,
        (shape((ROWS, 256), BF),) * 6,
        in_specs=[SMEM] + [VMEM] * 6,
        out_specs=(VMEM,) * 6,
        flops=3 * 10**9,
    )(tp, gg, gu, *weights)


def merge_body(t_ref, top, bottom, rs, rc, ls, lc, rs2, rc2, ls2, lc2):
    core = t_ref[0] % 2
    for src, dst, got, first in (
        (rs, rs2, top[core], True),
        (rc, rc2, top[1 - core], True),
        (ls, ls2, bottom[core], False),
        (lc, lc2, bottom[1 - core], False),
    ):
        hit, other = (slice(0, 256), slice(256, 512)) if first else (slice(256, 512), slice(0, 256))
        dst[hit, :] = (src[hit, :].astype(F32) + got.astype(F32)).astype(BF)
        dst[other, :] = src[other, :]


def merge(tp, top, bottom, parts):
    return call(
        merge_body,
        (shape((ROWS, 256), BF),) * 4,
        in_specs=[SMEM] + [VMEM] * 6,
        out_specs=(VMEM,) * 4,
        flops=10**7,
    )(tp, top, bottom, *parts)


def settle_body(a0, a1, a2, b0, b1, b2, out_ref):
    own = a0[...].astype(F32) + a1[...].astype(F32) + a2[...].astype(F32)
    other = b0[...].astype(F32) + b1[...].astype(F32) + b2[...].astype(F32)
    out_ref[:, 0:HALF, :] = own.astype(BF).reshape(SP, HALF, 256)
    out_ref[:, HALF:CAP, :] = other.astype(BF).reshape(SP, HALF, 256)


def settle(parts):
    return call(settle_body, shape((SP, CAP, 256), BF), flops=10**7)(*parts)


def weights_of(t_ref, xs, cs, gg, gu, act, cols):
    q = quarters(t_ref)
    gu_cols = jnp.concatenate([gg[:, cols], gu[:, cols]], axis=1)
    act_cols = act[:, cols]
    for i in range(4):
        both = dot(xs[i], gu_cols, 0, 0)
        yield q[i], both[:, 0:256], both[:, 256:512], dot(act_cols, cs[i], 0, 0)


def lend_body(t_ref, *refs):
    xs, cs = joined(refs[0:5]), joined(refs[5:10])
    gg, gu, act, gate_ref, up_ref, down_ref = refs[10:16]
    for q, a, b, d in weights_of(t_ref, xs, cs, gg, gu, act, slice(256, 512)):
        gate_ref[q] = a.astype(BF)
        up_ref[q] = b.astype(BF)
        down_ref[:, pl.ds(pl.multiple_of(q * 512, 512), 512)] = d.astype(BF)


def lend(tp, xs, cs, gg, gu, act):
    return call(
        lend_body,
        (shape((4, 512, 256), BF), shape((4, 512, 256), BF), shape((256, 2048), BF)),
        in_specs=[SMEM] + [VMEM] * 13,
        out_specs=(VMEM,) * 3,
        flops=2 * 10**9,
    )(tp, *xs, *cs, gg, gu, act)


def keep_body(t_ref, *refs):
    xs, cs = joined(refs[0:5]), joined(refs[5:10])
    gg, gu, act, pg, pu, pd, gate_ref, up_ref, down_ref = refs[10:19]
    for q, a, b, d in weights_of(t_ref, xs, cs, gg, gu, act, slice(0, 256)):
        gate_ref[q] = a + pg[q].astype(F32)
        up_ref[q] = b + pu[q].astype(F32)
        at = pl.ds(pl.multiple_of(q * 512, 512), 512)
        down_ref[:, at] = d + pd[:, at].astype(F32)


def keep(tp, xs, cs, gg, gu, act, lent):
    return call(
        keep_body,
        (shape((4, 512, 256), F32), shape((4, 512, 256), F32), shape((256, 2048), F32)),
        in_specs=[SMEM] + [VMEM] * 16,
        out_specs=(VMEM,) * 3,
        flops=2 * 10**9,
    )(tp, *xs, *cs, gg, gu, act, *lent)


def norm_parts(saved):
    mean = jnp.sum(saved, axis=0, keepdims=True) / CW
    var = jnp.sum(saved * saved, axis=0, keepdims=True) / CW - mean * mean
    return mean, lax.rsqrt(var + EPS)


def prepare_body(got_ref, proj_ref, mixed_ref, slope_ref, slope_n_ref, stat_ref):
    saved = got_ref[:, 64:128, :].reshape(CW, TOK).astype(F32)
    proj_ref[...] = got_ref[:, 0:64, :].reshape(CW, TOK)
    mean, inv = norm_parts(saved)
    normed = (saved - mean) * inv
    sig = jax.nn.sigmoid(normed)
    mixed_ref[...] = (normed * sig).astype(BF)
    slope = sig * (1.0 + normed * (1.0 - sig))
    slope_ref[...] = slope
    slope_n_ref[...] = slope * normed
    stat_ref[...] = jnp.concatenate([mean, inv, mean, inv, mean, inv, mean, inv], axis=0)


def prepare(got):
    return call(
        prepare_body,
        (
            shape((CW, TOK), BF),
            shape((CW, TOK), BF),
            shape((CW, TOK), F32),
            shape((CW, TOK), F32),
            shape((8, TOK), F32),
        ),
        flops=10**8,
    )(got)


def tokens_body(
    t_ref, back_ref, up_ref, ret_ref, proj_ref, mixed_ref, slope_ref, slope_n_ref,
    gs_ref, part_ref, outer_ref,
):
    routed = dot(back_ref[...], ret_ref[...])
    gs = (up_ref[...].astype(F32) + routed).astype(BF)
    gs_ref[...] = gs
    part = dot(proj_ref[...], gs, 1, 1)
    part_ref[:, 0:64, :] = part.astype(BF).reshape(TP, 64, TOK)
    first = jnp.sum(part * slope_ref[...], axis=0, keepdims=True)
    second = jnp.sum(part * slope_n_ref[...], axis=0, keepdims=True)
    sums = jnp.concatenate([first, second], axis=0)
    high = sums.astype(BF).astype(F32)
    low = sums - high
    stats = jnp.concatenate([high, low, high, low], axis=0).astype(BF)
    part_ref[:, 64:72, :] = jnp.broadcast_to(stats[None], (TP, 8, TOK))
    outer = dot(gs, mixed_ref[...], 0, 1)
    lane = iota((64, 128), 1) < 64
    for u in range(4):
        for i in range(4):
            block = outer[64 * i : 64 * i + 64, 128 * u : 128 * u + 128]
            turned = pltpu.roll(block, 64, 1)
            even = jnp.where(lane[0:32], block[0:32], turned[32:64])
            odd = jnp.where(lane[0:32], turned[0:32], block[32:64])
            outer_ref[8 * i + 2 * u] = even.astype(BF)
            outer_ref[8 * i + 2 * u + 1] = odd.astype(BF)


def tokens(tp, back, upstream, ret, proj, mixed, slope, slope_n):
    whole = lambda *dims: pl.BlockSpec(dims, lambda i, t: (0,) * len(dims))
    return call(
        tokens_body,
        (shape((TOK, 256), BF), shape((TP, 72, TOK), BF), shape((SP, 32, 128), BF)),
        grid_spec=pltpu.PrefetchScalarGridSpec(
            num_scalar_prefetch=1,
            grid=(1,),
            in_specs=[
                whole(TOK, SP * CAP),
                pl.BlockSpec((TOK, 256), lambda i, t: (0, t[0])),
                whole(SP * CAP, 256),
                whole(CW, TOK),
                whole(CW, TOK),
                whole(CW, TOK),
                whole(CW, TOK),
            ],
            out_specs=[whole(TOK, 256), whole(TP, 72, TOK), whole(SP, 32, 128)],
        ),
        flops=10**9,
    )(tp, back, upstream, ret, proj, mixed, slope, slope_n)


def norm_body(got_ref, saved_ref, stat_ref, grad_ref, rim_ref):
    total = jnp.sum(got_ref[...].astype(F32), axis=0)
    mixed = total[0:64]
    first = (total[64:65] + total[66:67]) / CW
    second = (total[65:66] + total[67:68]) / CW
    mean, inv = stat_ref[0:1, :], stat_ref[1:2, :]
    normed = (saved_ref[...].astype(F32) - mean) * inv
    sig = jax.nn.sigmoid(normed)
    grad = mixed * sig * (1.0 + normed * (1.0 - sig))
    conv = inv * (grad - first - normed * second)
    grad_ref[...] = conv
    rim_ref[...] = conv[:, 0:128]


def norm(got, saved, stat):
    return call(norm_body, (shape((64, TOK), F32), shape((64, 128), F32)), flops=10**7)(
        got, saved, stat
    )


def conv_body(grad_ref, rim_ref, taps_ref, value_ref, gate_ref, dv_ref, dg_ref):
    padded = jnp.concatenate([grad_ref[...], rim_ref[...]], axis=1)
    total = jnp.zeros((64, TOK), F32)
    width = padded.shape[1]
    for j in range(taps_ref.shape[1]):
        moved = padded if j == 0 else pltpu.roll(padded, width - j, 1)
        total = total + taps_ref[:, j : j + 1] * moved[:, 0:TOK]
    sig = jax.nn.sigmoid(gate_ref[...].astype(F32))
    dv_ref[...] = (total * sig).astype(BF)
    dg_ref[...] = (total * value_ref[...].astype(F32) * sig * (1.0 - sig)).astype(BF)


def conv(grad, rim, taps, value, gate):
    return call(conv_body, (shape((64, TOK), BF), shape((64, TOK), BF)), flops=10**8)(
        grad, rim, taps, value, gate
    )


def total_body(got_ref, out_ref):
    total = jnp.sum(got_ref[...].astype(F32), axis=0)
    out_ref[0:32, :] = total[:, 0:64]
    out_ref[32:64, :] = total[:, 64:128]


def total(got):
    return call(total_body, shape((64, 64), F32), flops=10**7)(got)


def moved(x, by):
    return lax.ppermute(x, "tp", [(i, (i + by) % TP) for i in range(TP)])


def across(x):
    return lax.ppermute(x, "tp", [(i, i ^ 1) for i in range(TP)])


def across_moved(x, by):
    return lax.ppermute(x, "tp", [(i, ((i + by) % TP) ^ 1) for i in range(TP)])


def around(block):
    left, right = moved(block, 2), moved(block, -2)
    top, bottom = moved(left[:256], 2), moved(right[256:], -2)
    return block, left, right, top, bottom


def exchange(x, axis):
    return lax.all_to_all(x, axis, 0, 0, tiled=True)


def on_device(
    upstream, stream, routes, route_weights, glu_value, glu_gate, conv_taps, conv_saved,
    out_proj, expert_gate, expert_up, expert_down,
):
    tp = lax.axis_index("tp").reshape(1)
    rows_out, target = pick_rows(tp, routes.T, stream)
    rows_in = exchange(rows_out.reshape(SP, HALF, 512), "sp").reshape(ROWS, 512)

    gate_own, up_own, down_own = expert_gate[0], expert_up[0], expert_down[0]
    gate_par, up_par, down_par = across(gate_own), across(up_own), across(down_own)

    cot_out, back = pick_cot(tp, target, route_weights.T, upstream)
    cot_in = exchange(cot_out.reshape(SP, HALF, 512), "sp").reshape(ROWS, 512)

    saved = conv_saved.T
    early = jnp.concatenate(
        [
            out_proj.T.reshape(64, TP, 256).transpose(1, 0, 2),
            jnp.broadcast_to(saved[None], (TP, 64, TOK)),
        ],
        axis=1,
    )
    proj, mixed, slope, slope_n, stat = prepare(exchange(early, "tp"))

    xs = around(rows_in)
    by_quarter = [w.reshape(4, 512, 256) for w in (gate_own, gate_par, up_own, up_par)]
    by_piece = [w.reshape(8, 256, 256) for w in (gate_own, gate_par, up_own, up_par)]
    act, a1, a2 = forward(tp, xs, by_quarter)

    cs = around(cot_in)
    far_top, far_bottom, gg, gu = backward(tp, cs, (down_own, down_par), a1, a2, by_piece)
    got_top, got_bottom = moved(far_top, 2), moved(far_bottom, -2)
    parts = near(tp, gg, gu, by_piece)
    rs, rc, ls, lc = merge(tp, got_top, got_bottom, parts[:4])
    summed = settle(
        (
            parts[4],
            moved(rs, 2),
            moved(ls, -2),
            across(parts[5]),
            across_moved(rc, 2),
            across_moved(lc, -2),
        )
    )
    returned = exchange(summed, "sp").reshape(SP * CAP, 256)

    lent = lend(tp, xs, cs, gg, gu, act)
    grad_gate_w, grad_up_w, grad_down_w = keep(
        tp, xs, cs, gg, gu, act, tuple(across(w) for w in lent)
    )

    grad_stream, part, outer = tokens(tp, back, upstream, returned, proj, mixed, slope, slope_n)
    grad_conv, rim = norm(exchange(part, "tp"), saved, stat)
    rim_in = lax.ppermute(rim, "sp", [(i, i - 1) for i in range(1, SP)])
    grad_value, grad_gate = conv(grad_conv, rim_in, conv_taps.T, glu_value.T, glu_gate.T)
    own_piece = total(exchange(outer, "sp"))
    grad_out_proj = lax.ppermute(
        own_piece,
        ("sp", "tp"),
        [
            ((i * 8 + u) * TP + t, (4 * t + i) * TP + u)
            for i in range(4)
            for u in range(TP)
            for t in range(TP)
        ],
    )
    return (
        grad_stream,
        grad_value.T,
        grad_gate.T,
        grad_out_proj,
        grad_gate_w.reshape(1, 2048, 256),
        grad_up_w.reshape(1, 2048, 256),
        grad_down_w[None],
    )


def solution(mesh):
    in_specs = (
        P("sp", None),
        P("sp", None),
        P("sp", None),
        P("sp", None),
        P("sp", "tp"),
        P("sp", "tp"),
        P(None, "tp"),
        P("sp", "tp"),
        P(None, "tp"),
        P("sp", None, "tp"),
        P("sp", None, "tp"),
        P("sp", "tp", None),
    )
    out_specs = (
        P("sp", "tp"),
        P("sp", "tp"),
        P("sp", "tp"),
        P("sp", "tp"),
        P("sp", None, "tp"),
        P("sp", None, "tp"),
        P("sp", "tp", None),
    )
    return jax.shard_map(
        on_device, mesh=mesh, in_specs=in_specs, out_specs=out_specs, check_vma=False
    )
```

```python
import jax
import jax.numpy as jnp
from jax import lax
from jax.experimental import pallas as pl
from jax.experimental.pallas import tpu as pltpu
from jax.sharding import PartitionSpec as P

CLAMP = 7.0
ALPHA = 1.702
EPS = 1e-05
CW = 512
CAP = 32
HALF = 16
SP = 32
TP = 8
TOK = 256
ROWS = SP * HALF
BF = jnp.bfloat16
F32 = jnp.float32
MIB = 1 << 20


def dot(a, b, ca=1, cb=0):
    return lax.dot_general(a, b, (((ca,), (cb,)), ((), ())), preferred_element_type=F32)


def flag(mask):
    return jnp.where(mask, 1.0, 0.0)


def iota(shape, dim):
    return lax.broadcasted_iota(jnp.int32, shape, dim)


class Later:
    def __init__(self, source, buffer, sem):
        self.copy, self.buffer, self.waiting = pltpu.make_async_copy(source, buffer, sem), buffer, True
        self.copy.start()

    def now(self):
        if self.waiting:
            self.copy.wait()
            self.waiting = False
        return self.buffer


def now(x):
    return x.now() if isinstance(x, Later) else x


def call(body, outs, tp, args, staged=(), cuts=None, scratch=(), flops=0, limit=40):
    cuts = cuts or {}
    single = not isinstance(outs, tuple)
    outs = (outs,) if single else outs
    n_in, n_out, n_scr = len(args), len(outs), len(scratch)

    def kernel(t_ref, *refs):
        ins, rest = list(refs[:n_in]), refs[n_in:]
        made, scr, buffers = rest[:n_out], rest[n_out : n_out + n_scr], rest[n_out + n_scr :]
        for n, i in enumerate(staged):
            source = ins[i].at[cuts[i][1](t_ref[0])] if i in cuts else ins[i]
            ins[i] = Later(source, buffers[n], buffers[-1].at[n])
        body(t_ref[0], ins, made, scr)
        for i in staged:
            now(ins[i])

    extra = [
        pltpu.VMEM(cuts[i][0] if i in cuts else args[i].shape, args[i].dtype) for i in staged
    ]
    if staged:
        extra.append(pltpu.SemaphoreType.DMA((len(staged),)))
    args = tuple(
        pltpu.with_memory_space_constraint(x, pltpu.HBM) if i in staged else x
        for i, x in enumerate(args)
    )
    made = pl.pallas_call(
        kernel,
        out_shape=outs,
        in_specs=[SMEM] + [HBM if i in staged else VMEM for i in range(n_in)],
        out_specs=(VMEM,) * n_out,
        scratch_shapes=list(scratch) + extra,
        compiler_params=pltpu.CompilerParams(vmem_limit_bytes=limit * MIB),
        cost_estimate=pl.CostEstimate(flops=flops, bytes_accessed=MIB, transcendentals=0),
    )(tp, *args)
    return made[0] if single else made


def shape(dims, dtype):
    return jax.ShapeDtypeStruct(dims, dtype)


SMEM = pl.BlockSpec(memory_space=pltpu.SMEM)
VMEM = pl.BlockSpec(memory_space=pltpu.VMEM)
HBM = pl.BlockSpec(memory_space=pltpu.HBM)


def columns_of(width, which):
    return lambda t: (slice(None), pl.ds(pl.multiple_of(which(t) * width, width), width))


def pick_rows_body(t, ins, outs, scr):
    core = t % 2
    r = ins[0][...]
    r0, r1 = r[0:1, :], r[1:2, :]
    expert = iota((SP, TOK), 0)
    named0, named1 = expert == r0, expert == r1
    both = (flag(named0) + flag(named1)).astype(BF)
    before = flag(iota((TOK, TOK), 0) < iota((TOK, TOK), 1)).astype(BF)
    earlier = dot(both, before)
    slot0 = jnp.sum(jnp.where(named0, earlier, 0.0), axis=0, keepdims=True).astype(jnp.int32)
    slot1 = jnp.sum(jnp.where(named1, earlier, 0.0), axis=0, keepdims=True).astype(jnp.int32)
    l0 = jnp.where(slot0 // HALF == core, r0 * HALF + slot0 - HALF * core, -1)
    l1 = jnp.where(slot1 // HALF == core, r1 * HALF + slot1 - HALF * core, -1)
    b0 = r0 * CAP + (slot0 + HALF * core) % CAP
    b1 = r1 * CAP + (slot1 + HALF * core) % CAP
    outs[1][...] = jnp.concatenate([l0, l1, b0, b1, l0, l1, b0, b1], axis=0)
    place = iota((ROWS, TOK), 0)
    pick = flag((place == l0) | (place == l1)).astype(BF)
    outs[0][...] = dot(pick, now(ins[1])[...]).astype(BF)


def pick_rows(tp, routes, stream):
    return call(
        pick_rows_body,
        (pltpu.HBM((ROWS, 512), BF), shape((8, TOK), jnp.int32)),
        tp,
        (routes, stream),
        staged=(1,),
        cuts={1: ((TOK, 512), columns_of(512, lambda t: t // 2))},
        flops=10**9,
    )


def pick_cot_body(t, ins, outs, scr):
    tgt, w = ins[0][...], ins[1][...]
    table = jnp.concatenate([tgt[2:4, :].astype(F32), w, tgt[2:4, :].astype(F32), w], axis=0)
    columns = jnp.transpose(jnp.concatenate([table] * 16, axis=0))
    up = now(ins[2])[...].astype(F32)
    cot0 = (columns[:, 2:3] * up).astype(BF)
    cot1 = (columns[:, 3:4] * up).astype(BF)
    place = iota((ROWS, TOK), 0)
    cot = dot(flag(place == tgt[0:1, :]).astype(BF), cot0)
    cot = cot + dot(flag(place == tgt[1:2, :]).astype(BF), cot1)
    outs[0][...] = cot.astype(BF)
    b0 = columns[:, 0:1].astype(jnp.int32)
    b1 = columns[:, 1:2].astype(jnp.int32)
    spot = iota((TOK, SP * CAP), 1)
    outs[1][...] = flag((spot == b0) | (spot == b1)).astype(BF)


def pick_cot(tp, target, weights, upstream):
    return call(
        pick_cot_body,
        (pltpu.HBM((ROWS, 512), BF), pltpu.HBM((TOK, SP * CAP), BF)),
        tp,
        (target, weights, upstream),
        staged=(2,),
        cuts={2: ((TOK, 512), columns_of(512, lambda t: t // 2))},
        flops=10**9,
    )


def quarters(t):
    y = t // 2
    return y, (y + 3) % 4, (y + 1) % 4, (y + 2) % 4


def joined(refs):
    own, left, right, top, bottom = [now(r) for r in refs]
    return (
        own[...],
        left[...],
        right[...],
        jnp.concatenate([top[...], bottom[...]], axis=0),
    )


def forward_body(t, ins, outs, scr):
    act_ref, a1_ref, a2_ref = outs
    pg, pu = scr
    q = quarters(t)
    x = joined(ins[0:5])
    for j in range(2):
        cols = slice(256 * j, 256 * j + 256)
        g = now(ins[5 + j])
        pg[:, cols] = sum(dot(x[i], g[q[i]]) for i in range(4))
        u = now(ins[7 + j])
        pu[:, cols] = sum(dot(x[i], u[q[i]]) for i in range(4))

    @pl.loop(0, ROWS // 32)
    def _(i):
        at = pl.ds(pl.multiple_of(i * 32, 32), 32)
        gate_pre, up_pre = pg[at, :], pu[at, :]
        capped = jnp.minimum(gate_pre, CLAMP)
        clipped = jnp.clip(up_pre, -CLAMP, CLAMP)
        sig = jax.nn.sigmoid(ALPHA * capped)
        gated = capped * sig
        act_ref[at, :] = (gated * (clipped + 1.0)).astype(BF)
        slope = sig + ALPHA * gated * (1.0 - sig)
        a1_ref[at, :] = jnp.where(gate_pre < CLAMP, (clipped + 1.0) * slope, 0.0)
        a2_ref[at, :] = jnp.where(jnp.abs(up_pre) < CLAMP, gated, 0.0)


def forward(tp, blocks, weights):
    return call(
        forward_body,
        (shape((ROWS, 512), BF), shape((ROWS, 512), F32), shape((ROWS, 512), F32)),
        tp,
        (*blocks, *weights),
        staged=(5, 7, 6, 8),
        scratch=[pltpu.VMEM((ROWS, 512), F32)] * 2,
        flops=2 * 10**9,
    )


def partial_of(g, u, weights, piece):
    g0, g1, u0, u1 = weights
    return (
        dot(g[:, 0:256], g0[piece], 1, 1)
        + dot(g[:, 256:512], g1[piece], 1, 1)
        + dot(u[:, 0:256], u0[piece], 1, 1)
        + dot(u[:, 256:512], u1[piece], 1, 1)
    )


def backward_body(t, ins, outs, scr):
    top_ref, bottom_ref, gg_ref, gu_ref = outs
    ga = scr[0]
    a1, a2 = ins[7], ins[8]
    q = quarters(t)
    x = joined(ins[0:5])
    for j in range(2):
        d = now(ins[5 + j])
        ga[:, 256 * j : 256 * j + 256] = sum(
            dot(x[i], d[:, pl.ds(pl.multiple_of(q[i] * 512, 512), 512)], 1, 1) for i in range(4)
        )

    @pl.loop(0, ROWS // 32)
    def _(i):
        at = pl.ds(pl.multiple_of(i * 32, 32), 32)
        grad = ga[at, :]
        gg_ref[at, :] = (grad * a1[at, :]).astype(BF)
        gu_ref[at, :] = (grad * a2[at, :]).astype(BF)

    g, u = gg_ref[...], gu_ref[...]
    weights = [now(w) for w in ins[9:13]]
    for half in range(2):
        part = partial_of(g, u, weights, half).astype(BF)
        top_ref[half] = part[0:256]
        bottom_ref[half] = part[256:512]


def backward(tp, blocks, downs, a1, a2, weights):
    far = ((2, 256, 256), lambda t: (pl.ds(2 * ((t // 2 + 2) % 4), 2),))
    return call(
        backward_body,
        (
            shape((2, 256, 256), BF),
            shape((2, 256, 256), BF),
            shape((ROWS, 512), BF),
            shape((ROWS, 512), BF),
        ),
        tp,
        (*blocks, *downs, a1, a2, *weights),
        staged=(5, 6, 9, 10, 11, 12),
        cuts={9: far, 10: far, 11: far, 12: far},
        scratch=[pltpu.VMEM((ROWS, 512), F32)],
        flops=2 * 10**9,
    )


def near_body(t, ins, outs, scr):
    g, u = ins[0][...], ins[1][...]
    weights = [now(w) for w in ins[2:6]]
    right, left = (t + 2) % 8, (t + 6) % 8
    swap = 1 - 2 * (t % 2)
    pieces = (right, right + swap, left, left + swap, t, t + swap)
    for ref, piece in zip(outs, pieces):
        ref[...] = partial_of(g, u, weights, piece).astype(BF)


def near(tp, gg, gu, weights):
    return call(
        near_body,
        (shape((ROWS, 256), BF),) * 6,
        tp,
        (gg, gu, *weights),
        staged=(2, 3, 4, 5),
        flops=3 * 10**9,
    )


def merge_body(t, ins, outs, scr):
    core = t % 2
    top, bottom = ins[0:2]
    for src, dst, got, first in (
        (ins[2], outs[0], top[core], True),
        (ins[3], outs[1], top[1 - core], True),
        (ins[4], outs[2], bottom[core], False),
        (ins[5], outs[3], bottom[1 - core], False),
    ):
        hit, other = (slice(0, 256), slice(256, 512)) if first else (slice(256, 512), slice(0, 256))
        dst[hit, :] = (src[hit, :].astype(F32) + got.astype(F32)).astype(BF)
        dst[other, :] = src[other, :]


def merge(tp, top, bottom, parts):
    return call(
        merge_body, (shape((ROWS, 256), BF),) * 4, tp, (top, bottom, *parts), flops=10**7, limit=16
    )


def settle_body(t, ins, outs, scr):
    a0, a1, a2, b0, b1, b2 = [x[...].astype(F32) for x in ins]
    outs[0][:, 0:HALF, :] = (a0 + a1 + a2).astype(BF).reshape(SP, HALF, 256)
    outs[0][:, HALF:CAP, :] = (b0 + b1 + b2).astype(BF).reshape(SP, HALF, 256)


def settle(tp, parts):
    return call(settle_body, pltpu.HBM((SP, CAP, 256), BF), tp, parts, flops=10**7, limit=16)


def weights_of(t, ins, cols):
    q = quarters(t)
    xs, cs = joined(ins[0:5]), joined(ins[5:10])
    gg, gu, act = [now(x) for x in ins[10:13]]
    gu_cols = jnp.concatenate([gg[:, cols], gu[:, cols]], axis=1)
    act_cols = act[:, cols]
    for i in range(4):
        both = dot(xs[i], gu_cols, 0, 0)
        yield q[i], both[:, 0:256], both[:, 256:512], dot(act_cols, cs[i], 0, 0)


def lend_body(t, ins, outs, scr):
    for q, a, b, d in weights_of(t, ins, slice(256, 512)):
        outs[0][q] = a.astype(BF)
        outs[0][4 + q] = b.astype(BF)
        outs[0][8 + q, 0:256, :] = d[:, 0:256].astype(BF)
        outs[0][8 + q, 256:512, :] = d[:, 256:512].astype(BF)


def lend(tp, xs, cs, gg, gu, act):
    return call(
        lend_body,
        shape((12, 512, 256), BF),
        tp,
        (*xs, *cs, gg, gu, act),
        staged=tuple(range(13)),
        flops=2 * 10**9,
    )


def keep_body(t, ins, outs, scr):
    gate_ref, up_ref, down_ref = outs
    lent = now(ins[13])
    for q, a, b, d in weights_of(t, ins, slice(0, 256)):
        gate_ref[q] = a + lent[q].astype(F32)
        up_ref[q] = b + lent[4 + q].astype(F32)
        for half in range(2):
            cols = slice(256 * half, 256 * half + 256)
            at = pl.ds(pl.multiple_of(q * 512 + 256 * half, 256), 256)
            down_ref[:, at] = d[:, cols] + lent[8 + q, cols, :].astype(F32)


def keep(tp, xs, cs, gg, gu, act, lent):
    return call(
        keep_body,
        (shape((4, 512, 256), F32), shape((4, 512, 256), F32), shape((256, 2048), F32)),
        tp,
        (*xs, *cs, gg, gu, act, lent),
        staged=tuple(range(14)),
        flops=2 * 10**9,
    )


def hand_out_body(t, ins, outs, scr):
    proj = now(ins[0])
    for d in range(4):
        other = lax.bitwise_xor(t, 2 * d + 1)
        outs[0][d] = proj[:, pl.ds(pl.multiple_of(other * 256, 256), 256)]
    outs[0][4] = ins[1][...]


def hand_out(tp, proj, saved):
    return call(
        hand_out_body, shape((5, 64, TOK), BF), tp, (proj, saved), staged=(0,), limit=16
    )


def hand_on_body(t, ins, outs, scr):
    proj = now(ins[0])
    for d in range(1, 4):
        other = lax.bitwise_xor(t, 2 * d)
        outs[d - 1][0] = proj[:, pl.ds(pl.multiple_of(other * 256, 256), 256)]
        outs[d - 1][1] = ins[2][d]
        outs[d - 1][2] = ins[1][...]
        outs[d - 1][3] = ins[2][4]


def hand_on(tp, proj, saved, got):
    return call(
        hand_on_body,
        (shape((4, 64, TOK), BF),) * 3,
        tp,
        (proj, saved, got),
        staged=(0,),
        limit=16,
    )


def prepare_body(t, ins, outs, scr):
    proj_ref, mixed_ref, slope_ref, slope_n_ref, stat_ref = outs
    all_saved = scr[0]

    def at(d):
        return pl.ds(pl.multiple_of(lax.bitwise_xor(t, d) * 64, 64), 64)

    proj_ref[at(0), :] = now(ins[0])[...]
    all_saved[at(0), :] = ins[1][...]
    proj_ref[at(1), :] = ins[2][0]
    all_saved[at(1), :] = ins[2][4]
    for d in range(1, 4):
        for other in range(2):
            proj_ref[at(2 * d + other), :] = ins[2 + d][other]
            all_saved[at(2 * d + other), :] = ins[2 + d][2 + other]
    saved = all_saved[...].astype(F32)
    mean = jnp.sum(saved, axis=0, keepdims=True) / CW
    var = jnp.sum(saved * saved, axis=0, keepdims=True) / CW - mean * mean
    inv = lax.rsqrt(var + EPS)
    normed = (saved - mean) * inv
    sig = jax.nn.sigmoid(normed)
    mixed_ref[...] = (normed * sig).astype(BF)
    slope = sig * (1.0 + normed * (1.0 - sig))
    slope_ref[...] = slope
    slope_n_ref[...] = slope * normed
    stat_ref[...] = jnp.concatenate([mean, inv, mean, inv, mean, inv, mean, inv], axis=0)


def prepare(tp, proj, saved, got):
    return call(
        prepare_body,
        (
            pltpu.HBM((CW, TOK), BF),
            pltpu.HBM((CW, TOK), BF),
            pltpu.HBM((CW, TOK), F32),
            pltpu.HBM((CW, TOK), F32),
            shape((8, TOK), F32),
        ),
        tp,
        (proj, saved, *got),
        staged=(0,),
        cuts={0: ((64, TOK), columns_of(256, lambda t: t))},
        scratch=[pltpu.VMEM((CW, TOK), BF)],
        flops=10**8,
    )


def tokens_body(t, ins, outs, scr):
    gs_ref, outer_ref, own_ref, lent_ref = outs
    routed = dot(now(ins[0])[...], ins[2][...])
    gs = (now(ins[1])[...].astype(F32) + routed).astype(BF)
    gs_ref[...] = gs
    outer = dot(gs, now(ins[4])[...], 0, 1)
    lane = iota((64, 128), 1) < 64
    for u in range(4):
        for i in range(4):
            block = outer[64 * i : 64 * i + 64, 128 * u : 128 * u + 128]
            turned = pltpu.roll(block, 64, 1)
            even = jnp.where(lane[0:32], block[0:32], turned[32:64])
            odd = jnp.where(lane[0:32], turned[0:32], block[32:64])
            outer_ref[8 * i + 2 * u] = even.astype(BF)
            outer_ref[8 * i + 2 * u + 1] = odd.astype(BF)
    part_all = scr[0]
    part = dot(now(ins[3])[...], gs, 1, 1)
    part_all[...] = part
    first = jnp.sum(part * now(ins[5])[...], axis=0, keepdims=True)
    second = jnp.sum(part * now(ins[6])[...], axis=0, keepdims=True)
    sums = jnp.concatenate([first, second], axis=0)
    parted = split_sums(sums)

    def at(d):
        return pl.ds(pl.multiple_of(lax.bitwise_xor(t, d) * 64, 64), 64)

    for d in range(4):
        own_ref[d, 0:64, :] = part_all[at(2 * d), :]
        lent_ref[d, 0:64, :] = part_all[at(2 * d + 1), :].astype(BF)
        lent_ref[d, 64:72, :] = parted
    own_ref[0, 64:72, :] = jnp.concatenate([sums] * 4, axis=0)


def split_sums(sums):
    high = sums.astype(BF).astype(F32)
    low = sums - high
    return jnp.concatenate([high, low, high, low], axis=0).astype(BF)


def fold_body(t, ins, outs, scr):
    own, got = ins
    sums = own[0, 64:66, :] + got[0, 64:66, :].astype(F32) + got[0, 66:68, :].astype(F32)
    outs[0][0:64, :] = own[0, 0:64, :] + got[0, 0:64, :].astype(F32)
    outs[0][64:72, :] = jnp.concatenate([sums] * 4, axis=0)
    parted = split_sums(sums)
    for d in range(1, 4):
        outs[d][0:64, :] = (own[d, 0:64, :] + got[d, 0:64, :].astype(F32)).astype(BF)
        outs[d][64:72, :] = parted


def fold(tp, own, got):
    return call(
        fold_body,
        (shape((72, TOK), F32),) + (shape((72, TOK), BF),) * 3,
        tp,
        (own, got),
        flops=10**7,
        limit=16,
    )


def tokens(tp, back, upstream, ret, proj, mixed, slope, slope_n):
    return call(
        tokens_body,
        (
            shape((TOK, 256), BF),
            pltpu.HBM((SP, 32, 128), BF),
            shape((4, 72, TOK), F32),
            shape((4, 72, TOK), BF),
        ),
        tp,
        (back, upstream, ret, proj, mixed, slope, slope_n),
        staged=(0, 1, 4, 3, 5, 6),
        cuts={1: ((TOK, 256), columns_of(256, lambda t: t))},
        scratch=[pltpu.VMEM((CW, TOK), F32)],
        flops=10**9,
    )


def norm_body(t, ins, outs, scr):
    own, saved, stat = ins[0], ins[4], ins[5]
    mixed, sums = own[0:64, :], own[64:66, :]
    for got in ins[1:4]:
        mixed = mixed + got[0:64, :].astype(F32)
        sums = sums + got[64:66, :].astype(F32) + got[66:68, :].astype(F32)
    first, second = sums[0:1] / CW, sums[1:2] / CW
    mean, inv = stat[0:1, :], stat[1:2, :]
    normed = (saved[...].astype(F32) - mean) * inv
    sig = jax.nn.sigmoid(normed)
    grad = mixed * sig * (1.0 + normed * (1.0 - sig))
    conv_grad = inv * (grad - first - normed * second)
    outs[0][...] = conv_grad
    outs[1][...] = conv_grad[:, 0:128]


def norm(tp, own, got, saved, stat):
    return call(
        norm_body,
        (shape((64, TOK), F32), shape((64, 128), F32)),
        tp,
        (own, *got, saved, stat),
        flops=10**7,
        limit=16,
    )


def tap_sum(padded, taps):
    total = jnp.zeros((64, TOK), F32)
    width = padded.shape[1]
    for j in range(taps.shape[1]):
        turned = padded if j == 0 else pltpu.roll(padded, width - j, 1)
        total = total + taps[:, j : j + 1] * turned[:, 0:TOK]
    return total


def conv_own_body(t, ins, outs, scr):
    grad, taps = ins
    outs[0][...] = tap_sum(jnp.concatenate([grad[...], jnp.zeros((64, 128), F32)], axis=1), taps)


def conv_own(tp, grad, taps):
    return call(conv_own_body, shape((64, TOK), F32), tp, (grad, taps), flops=10**8, limit=16)


def conv_rim_body(t, ins, outs, scr):
    own, rim, taps, value, gate = ins
    dv_ref, dg_ref = outs
    both = jnp.concatenate([jnp.zeros((64, 128), F32), rim[...]], axis=1)
    reach = jnp.zeros((64, 128), F32)
    for j in range(1, taps.shape[1]):
        reach = reach + taps[:, j : j + 1] * pltpu.roll(both, TOK - j, 1)[:, 0:128]
    total = jnp.concatenate([own[:, 0:128], own[:, 128:256] + reach], axis=1)
    sig = jax.nn.sigmoid(gate[...].astype(F32))
    dv_ref[...] = (total * sig).astype(BF)
    dg_ref[...] = (total * value[...].astype(F32) * sig * (1.0 - sig)).astype(BF)


def conv_rim(tp, own, rim, taps, value, gate):
    return call(
        conv_rim_body,
        (shape((64, TOK), BF), shape((64, TOK), BF)),
        tp,
        (own, rim, taps, value, gate),
        flops=10**8,
        limit=16,
    )


def total_body(t, ins, outs, scr):
    whole = jnp.sum(ins[0][...].astype(F32), axis=0)
    outs[0][0:32, :] = whole[:, 0:64]
    outs[0][32:64, :] = whole[:, 64:128]


def total(tp, got):
    return call(total_body, shape((64, 64), F32), tp, (got,), flops=10**7, limit=16)


def moved(x, by):
    return lax.ppermute(x, "tp", [(i, (i + by) % TP) for i in range(TP)])


def swapped(x, by):
    return lax.ppermute(x, "tp", [(i, i ^ by) for i in range(TP)])


def across_moved(x, by):
    return lax.ppermute(x, "tp", [(i, ((i + by) % TP) ^ 1) for i in range(TP)])


def around(block, hold=None):
    left, right = moved(block, 2), moved(block, -2)
    if hold is not None:
        left, right, _ = lax.optimization_barrier((left, right, hold))
    top, bottom = moved(left[:256], 2), moved(right[256:], -2)
    return block, left, right, top, bottom


def exchange(x):
    return lax.all_to_all(x, "sp", 0, 0, tiled=True)


def after(x, *others):
    return lax.optimization_barrier((x, *others))[0]


def step(
    upstream, stream, routes, route_weights, glu_value, glu_gate, conv_taps, conv_saved,
    out_proj, expert_gate, expert_up, expert_down,
):
    tp = lax.axis_index("tp").reshape(1)
    rows_out, target = pick_rows(tp, routes.T, stream)
    rows_in = exchange(rows_out.reshape(SP, HALF, 512)).reshape(ROWS, 512)

    saved, proj = conv_saved.T, out_proj.T
    near_early = swapped(hand_out(tp, proj, saved), 1)
    far_early = hand_on(tp, proj, saved, near_early)
    early = (near_early, *(swapped(x, 2 * d + 2) for d, x in enumerate(far_early)))
    gate_own, up_own, down_own = expert_gate[0], expert_up[0], expert_down[0]
    gate_par, up_par, down_par = (swapped(w, 1) for w in (gate_own, up_own, down_own))

    cot_out, back = pick_cot(tp, target, route_weights.T, upstream)
    cot_out = after(cot_out, *early)
    cot_in = exchange(cot_out.reshape(SP, HALF, 512)).reshape(ROWS, 512)
    proj_all, mixed, slope, slope_n, stat = prepare(tp, proj, saved, early)

    xs = around(rows_in)
    by_quarter = [w.reshape(4, 512, 256) for w in (gate_own, gate_par, up_own, up_par)]
    by_piece = [w.reshape(8, 256, 256) for w in (gate_own, gate_par, up_own, up_par)]
    act, a1, a2 = forward(tp, xs, by_quarter)

    cs = around(cot_in, act)
    far_top, far_bottom, gg, gu = backward(tp, cs, (down_own, down_par), a1, a2, by_piece)
    got_top, got_bottom = moved(far_top, 2), moved(far_bottom, -2)
    parts = near(tp, gg, gu, by_piece)
    rs, rc, ls, lc = merge(tp, got_top, got_bottom, parts[:4])
    lent = lend(tp, xs, cs, gg, gu, after(act, rs))
    came = (moved(rs, 2), moved(ls, -2), across_moved(rc, 2), across_moved(lc, -2))
    own_cross = swapped(parts[5], 1)
    summed = settle(
        tp, (after(parts[4], lent), came[0], came[1], own_cross, came[2], came[3])
    )
    returned = exchange(summed).reshape(SP * CAP, 256)
    grads = keep(tp, xs, cs, gg, gu, act, swapped(lent, 1))
    grad_gate_w, grad_up_w, grad_down_w = grads
    back = after(back, grad_down_w)

    made = tokens(tp, back, upstream, returned, proj_all, mixed, slope, slope_n)
    grad_stream, outer, own_part, lent_part = made
    outer_in = exchange(outer)
    folded = fold(tp, own_part, swapped(lent_part, 1))
    own_part = folded[0]
    part_in = tuple(swapped(x, 2 * d + 2) for d, x in enumerate(folded[1:]))
    grad_conv, rim = norm(tp, own_part, part_in, saved, stat)
    rim_in = lax.ppermute(rim, "sp", [(i, i - 1) for i in range(1, SP)])
    taps = conv_taps.T
    grad_glu = conv_own(tp, grad_conv, taps)
    grad_value, grad_gate = conv_rim(tp, grad_glu, rim_in, taps, glu_value.T, glu_gate.T)
    grad_out_proj = lax.ppermute(
        total(tp, outer_in),
        ("sp", "tp"),
        [
            ((i * 8 + u) * TP + t, (4 * t + i) * TP + u)
            for i in range(4)
            for u in range(TP)
            for t in range(TP)
        ],
    )
    return (
        grad_stream,
        grad_value.T,
        grad_gate.T,
        grad_out_proj,
        grad_gate_w.reshape(1, 2048, 256),
        grad_up_w.reshape(1, 2048, 256),
        grad_down_w[None],
    )


def solution(mesh):
    in_specs = (
        P("sp", None),
        P("sp", None),
        P("sp", None),
        P("sp", None),
        P("sp", "tp"),
        P("sp", "tp"),
        P(None, "tp"),
        P("sp", "tp"),
        P(None, "tp"),
        P("sp", None, "tp"),
        P("sp", None, "tp"),
        P("sp", "tp", None),
    )
    out_specs = (
        P("sp", "tp"),
        P("sp", "tp"),
        P("sp", "tp"),
        P("sp", "tp"),
        P("sp", None, "tp"),
        P("sp", None, "tp"),
        P("sp", "tp", None),
    )
    return jax.shard_map(step, mesh=mesh, in_specs=in_specs, out_specs=out_specs, check_vma=False)
```

```python
import jax
import jax.numpy as jnp
from jax import lax
from jax.experimental import pallas as pl
from jax.experimental.pallas import tpu as pltpu
from jax.sharding import PartitionSpec as P

CLAMP = 7.0
ALPHA = 1.702
EPS = 1e-05
CW = 512
CAP = 32
HALF = 16
SP = 32
TP = 8
TOK = 256
ROWS = SP * HALF
BF = jnp.bfloat16
F32 = jnp.float32
MIB = 1 << 20


def dot(a, b, ca=1, cb=0):
    return lax.dot_general(a, b, (((ca,), (cb,)), ((), ())), preferred_element_type=F32)


def flag(mask):
    return jnp.where(mask, 1.0, 0.0)


def iota(shape, dim):
    return lax.broadcasted_iota(jnp.int32, shape, dim)


class Later:
    def __init__(self, source, buffer, sem):
        self.copy, self.buffer, self.waiting = pltpu.make_async_copy(source, buffer, sem), buffer, True
        self.copy.start()

    def now(self):
        if self.waiting:
            self.copy.wait()
            self.waiting = False
        return self.buffer


def now(x):
    return x.now() if isinstance(x, Later) else x


def call(body, outs, tp, args, staged=(), cuts=None, into=None, scratch=(), flops=0, limit=40):
    cuts, into = cuts or {}, into or {}
    own = tuple(i for i in staged if i not in into)
    single = not isinstance(outs, tuple)
    outs = (outs,) if single else outs
    n_in, n_out, n_scr = len(args), len(outs), len(scratch)

    def kernel(t_ref, *refs):
        ins, rest = list(refs[:n_in]), refs[n_in:]
        made, scr, buffers = rest[:n_out], rest[n_out : n_out + n_scr], rest[n_out + n_scr :]
        for n, i in enumerate(staged):
            source = ins[i].at[cuts[i][1](t_ref[0])] if i in cuts else ins[i]
            if i in into:
                target = scr[into[i][0]].at[into[i][1](t_ref[0])]
            else:
                target = buffers[own.index(i)]
            ins[i] = Later(source, target, buffers[-1].at[n])
        body(t_ref[0], ins, made, scr)
        for i in staged:
            now(ins[i])

    extra = [
        pltpu.VMEM(cuts[i][0] if i in cuts else args[i].shape, args[i].dtype) for i in own
    ]
    if staged:
        extra.append(pltpu.SemaphoreType.DMA((len(staged),)))
    args = tuple(
        pltpu.with_memory_space_constraint(x, pltpu.HBM) if i in staged else x
        for i, x in enumerate(args)
    )
    made = pl.pallas_call(
        kernel,
        out_shape=outs,
        in_specs=[SMEM] + [HBM if i in staged else VMEM for i in range(n_in)],
        out_specs=(VMEM,) * n_out,
        scratch_shapes=list(scratch) + extra,
        compiler_params=pltpu.CompilerParams(vmem_limit_bytes=limit * MIB),
        cost_estimate=pl.CostEstimate(flops=flops, bytes_accessed=MIB, transcendentals=0),
    )(tp, *args)
    return made[0] if single else made


def shape(dims, dtype):
    return jax.ShapeDtypeStruct(dims, dtype)


SMEM = pl.BlockSpec(memory_space=pltpu.SMEM)
VMEM = pl.BlockSpec(memory_space=pltpu.VMEM)
HBM = pl.BlockSpec(memory_space=pltpu.HBM)


def columns_of(width, which):
    return lambda t: (slice(None), pl.ds(pl.multiple_of(which(t) * width, width), width))


def pick_rows_body(t, ins, outs, scr):
    core = t % 2
    r = ins[0][...]
    r0, r1 = r[0:1, :], r[1:2, :]
    expert = iota((SP, TOK), 0)
    named0, named1 = expert == r0, expert == r1
    both = (flag(named0) + flag(named1)).astype(BF)
    before = flag(iota((TOK, TOK), 0) < iota((TOK, TOK), 1)).astype(BF)
    earlier = dot(both, before)
    slot0 = jnp.sum(jnp.where(named0, earlier, 0.0), axis=0, keepdims=True).astype(jnp.int32)
    slot1 = jnp.sum(jnp.where(named1, earlier, 0.0), axis=0, keepdims=True).astype(jnp.int32)
    l0 = jnp.where(slot0 // HALF == core, r0 * HALF + slot0 - HALF * core, -1)
    l1 = jnp.where(slot1 // HALF == core, r1 * HALF + slot1 - HALF * core, -1)
    b0 = r0 * CAP + (slot0 + HALF * core) % CAP
    b1 = r1 * CAP + (slot1 + HALF * core) % CAP
    outs[1][...] = jnp.concatenate([l0, l1, b0, b1, l0, l1, b0, b1], axis=0)
    place = iota((ROWS, TOK), 0)
    pick = flag((place == l0) | (place == l1)).astype(BF)
    outs[0][...] = dot(pick, now(ins[1])[...]).astype(BF)


def pick_rows(tp, routes, stream):
    return call(
        pick_rows_body,
        (pltpu.HBM((ROWS, 512), BF), shape((8, TOK), jnp.int32)),
        tp,
        (routes, stream),
        staged=(1,),
        cuts={1: ((TOK, 512), columns_of(512, lambda t: t // 2))},
        flops=10**9,
    )


def pick_cot_body(t, ins, outs, scr):
    tgt, w = ins[0][...], ins[1][...]
    table = jnp.concatenate([tgt[2:4, :].astype(F32), w, tgt[2:4, :].astype(F32), w], axis=0)
    columns = jnp.transpose(jnp.concatenate([table] * 16, axis=0))
    up = now(ins[2])[...].astype(F32)
    cot0 = (columns[:, 2:3] * up).astype(BF)
    cot1 = (columns[:, 3:4] * up).astype(BF)
    place = iota((ROWS, TOK), 0)
    cot = dot(flag(place == tgt[0:1, :]).astype(BF), cot0)
    cot = cot + dot(flag(place == tgt[1:2, :]).astype(BF), cot1)
    outs[0][...] = cot.astype(BF)
    b0 = columns[:, 0:1].astype(jnp.int32)
    b1 = columns[:, 1:2].astype(jnp.int32)
    spot = iota((TOK, SP * CAP), 1)
    outs[1][...] = flag((spot == b0) | (spot == b1)).astype(BF)


def pick_cot(tp, target, weights, upstream):
    return call(
        pick_cot_body,
        (pltpu.HBM((ROWS, 512), BF), pltpu.HBM((TOK, SP * CAP), BF)),
        tp,
        (target, weights, upstream),
        staged=(2,),
        cuts={2: ((TOK, 512), columns_of(512, lambda t: t // 2))},
        flops=10**9,
    )


def quarters(t):
    y = t // 2
    return y, (y + 3) % 4, (y + 1) % 4, (y + 2) % 4


def joined(refs):
    refs = [now(r)[...] for r in refs]
    own, sides, far = refs[0], refs[1:-2], jnp.concatenate(refs[-2:], axis=0)
    if len(sides) == 4:
        sides = [jnp.concatenate(sides[0:2], axis=0), jnp.concatenate(sides[2:4], axis=0)]
    return own, *sides, far


def forward_body(t, ins, outs, scr):
    act_ref, a1_ref, a2_ref = outs
    pg, pu = scr
    q = quarters(t)
    x = joined(ins[0:5])
    for j in range(2):
        cols = slice(256 * j, 256 * j + 256)
        g = now(ins[5 + j])
        pg[:, cols] = sum(dot(x[i], g[q[i]]) for i in range(4))
        u = now(ins[7 + j])
        pu[:, cols] = sum(dot(x[i], u[q[i]]) for i in range(4))

    @pl.loop(0, ROWS // 32)
    def _(i):
        at = pl.ds(pl.multiple_of(i * 32, 32), 32)
        gate_pre, up_pre = pg[at, :], pu[at, :]
        capped = jnp.minimum(gate_pre, CLAMP)
        clipped = jnp.clip(up_pre, -CLAMP, CLAMP)
        sig = jax.nn.sigmoid(ALPHA * capped)
        gated = capped * sig
        act_ref[at, :] = (gated * (clipped + 1.0)).astype(BF)
        slope = sig + ALPHA * gated * (1.0 - sig)
        a1_ref[at, :] = jnp.where(gate_pre < CLAMP, (clipped + 1.0) * slope, 0.0)
        a2_ref[at, :] = jnp.where(jnp.abs(up_pre) < CLAMP, gated, 0.0)


def forward(tp, blocks, weights):
    return call(
        forward_body,
        (shape((ROWS, 512), BF), shape((ROWS, 512), F32), shape((ROWS, 512), F32)),
        tp,
        (*blocks, *weights),
        staged=(5, 7, 6, 8),
        scratch=[pltpu.VMEM((ROWS, 512), F32)] * 2,
        flops=2 * 10**9,
    )


def partial_of(g, u, weights, piece):
    g0, g1, u0, u1 = weights
    return (
        dot(g[:, 0:256], g0[piece], 1, 1)
        + dot(g[:, 256:512], g1[piece], 1, 1)
        + dot(u[:, 0:256], u0[piece], 1, 1)
        + dot(u[:, 256:512], u1[piece], 1, 1)
    )


def backward_body(t, ins, outs, scr):
    top_ref, bottom_ref, gg_ref, gu_ref = outs
    ga = scr[0]
    a1, a2 = ins[9], ins[10]
    q = quarters(t)
    x = joined(ins[0:7])
    for j in range(2):
        d = now(ins[7 + j])
        ga[:, 256 * j : 256 * j + 256] = sum(
            dot(x[i], d[:, pl.ds(pl.multiple_of(q[i] * 512, 512), 512)], 1, 1) for i in range(4)
        )

    @pl.loop(0, ROWS // 32)
    def _(i):
        at = pl.ds(pl.multiple_of(i * 32, 32), 32)
        grad = ga[at, :]
        gg_ref[at, :] = (grad * a1[at, :]).astype(BF)
        gu_ref[at, :] = (grad * a2[at, :]).astype(BF)

    g, u = gg_ref[...], gu_ref[...]
    weights = [now(w) for w in ins[11:15]]
    for half in range(2):
        part = partial_of(g, u, weights, half).astype(BF)
        top_ref[half] = part[0:256]
        bottom_ref[half] = part[256:512]


def backward(tp, blocks, downs, a1, a2, weights):
    far = ((2, 256, 256), lambda t: (pl.ds(2 * ((t // 2 + 2) % 4), 2),))
    return call(
        backward_body,
        (
            shape((2, 256, 256), BF),
            shape((2, 256, 256), BF),
            shape((ROWS, 512), BF),
            shape((ROWS, 512), BF),
        ),
        tp,
        (*blocks, *downs, a1, a2, *weights),
        staged=(7, 8, 11, 12, 13, 14),
        cuts={11: far, 12: far, 13: far, 14: far},
        scratch=[pltpu.VMEM((ROWS, 512), F32)],
        flops=2 * 10**9,
    )


def near_body(t, ins, outs, scr):
    g, u = ins[0][...], ins[1][...]
    weights = [now(w) for w in ins[2:6]]
    right, left = (t + 2) % 8, (t + 6) % 8
    swap = 1 - 2 * (t % 2)
    pieces = (right, right + swap, left, left + swap, t, t + swap)
    for ref, piece in zip(outs, pieces):
        ref[...] = partial_of(g, u, weights, piece).astype(BF)


def near(tp, gg, gu, weights):
    return call(
        near_body,
        (shape((ROWS, 256), BF),) * 6,
        tp,
        (gg, gu, *weights),
        staged=(2, 3, 4, 5),
        flops=3 * 10**9,
    )


def merge_body(t, ins, outs, scr):
    core = t % 2
    top, bottom = ins[0:2]
    for src, dst, got, first in (
        (ins[2], outs[0], top[core], True),
        (ins[3], outs[1], top[1 - core], True),
        (ins[4], outs[2], bottom[core], False),
        (ins[5], outs[3], bottom[1 - core], False),
    ):
        hit, other = (slice(0, 256), slice(256, 512)) if first else (slice(256, 512), slice(0, 256))
        dst[hit, :] = (src[hit, :].astype(F32) + got.astype(F32)).astype(BF)
        dst[other, :] = src[other, :]


def merge(tp, top, bottom, parts):
    return call(
        merge_body, (shape((ROWS, 256), BF),) * 4, tp, (top, bottom, *parts), flops=10**7, limit=16
    )


def settle_body(t, ins, outs, scr):
    a0, a1, a2, b0, b1, b2 = [x[...].astype(F32) for x in ins]
    outs[0][:, 0:HALF, :] = (a0 + a1 + a2).astype(BF).reshape(SP, HALF, 256)
    outs[0][:, HALF:CAP, :] = (b0 + b1 + b2).astype(BF).reshape(SP, HALF, 256)


def settle(tp, parts):
    return call(settle_body, pltpu.HBM((SP, CAP, 256), BF), tp, parts, flops=10**7, limit=16)


def by_column(scr_index, first, halves):
    whole, upper, lower = slice(None), slice(0, 256), slice(256, 512)
    sides = ((3, upper), (3, lower), (1, upper), (1, lower)) if halves else ((3, whole), (1, whole))
    places = ((0, whole), *sides, (2, upper), (2, lower))
    return {
        first + n: (scr_index, lambda t, by=by, rows=rows: ((t // 2 + by) % 4, rows))
        for n, (by, rows) in enumerate(places)
    }


def weights_call(body, outs, tp, args):
    return call(
        body,
        outs,
        tp,
        args,
        staged=tuple(range(len(args))),
        into=by_column(0, 0, False) | by_column(1, 5, True),
        scratch=[pltpu.VMEM((4, ROWS, 512), BF)] * 2,
        flops=2 * 10**9,
    )


def each_quarter(ins, scr, cols, store):
    ins = [now(x) for x in ins]
    gg, gu, act = ins[12:15]
    gu_cols = jnp.concatenate([gg[:, cols], gu[:, cols]], axis=1)
    act_cols = act[:, cols]

    @pl.loop(0, 4)
    def _(q):
        store(q, dot(scr[0][q], gu_cols, 0, 0), dot(act_cols, scr[1][q], 0, 0))


def lend_body(t, ins, outs, scr):
    def store(q, both, down):
        outs[0][q] = both[:, 0:256].astype(BF)
        outs[0][4 + q] = both[:, 256:512].astype(BF)
        outs[0][8 + q, 0:256, :] = down[:, 0:256].astype(BF)
        outs[0][8 + q, 256:512, :] = down[:, 256:512].astype(BF)

    each_quarter(ins, scr, slice(256, 512), store)


def lend(tp, xs, cs, gg, gu, act):
    return weights_call(
        lend_body, shape((12, 512, 256), BF), tp, (*xs, *cs, gg, gu, act)
    )


def keep_body(t, ins, outs, scr):
    gate_ref, up_ref, down_ref = outs

    def store(q, both, down):
        lent = now(ins[15])
        gate_ref[q] = both[:, 0:256] + lent[q].astype(F32)
        up_ref[q] = both[:, 256:512] + lent[4 + q].astype(F32)
        for half in range(2):
            cols = slice(256 * half, 256 * half + 256)
            at = pl.ds(pl.multiple_of(q * 512 + 256 * half, 256), 256)
            down_ref[:, at] = down[:, cols] + lent[8 + q, cols, :].astype(F32)

    each_quarter(ins, scr, slice(0, 256), store)


def keep(tp, xs, cs, gg, gu, act, lent):
    return weights_call(
        keep_body,
        (shape((4, 512, 256), F32), shape((4, 512, 256), F32), shape((256, 2048), F32)),
        tp,
        (*xs, *cs, gg, gu, act, lent),
    )


def hand_out_body(t, ins, outs, scr):
    proj = now(ins[0])
    for d in range(4):
        other = lax.bitwise_xor(t, 2 * d + 1)
        outs[0][d] = proj[:, pl.ds(pl.multiple_of(other * 256, 256), 256)]
    outs[0][4] = ins[1][...]


def hand_out(tp, proj, saved):
    return call(
        hand_out_body, shape((5, 64, TOK), BF), tp, (proj, saved), staged=(0,), limit=16
    )


def hand_on_body(t, ins, outs, scr):
    proj = now(ins[0])
    for d in range(1, 4):
        other = lax.bitwise_xor(t, 2 * d)
        outs[d - 1][0] = proj[:, pl.ds(pl.multiple_of(other * 256, 256), 256)]
        outs[d - 1][1] = ins[2][d]
        outs[d - 1][2] = ins[1][...]
        outs[d - 1][3] = ins[2][4]


def hand_on(tp, proj, saved, got):
    return call(
        hand_on_body,
        (shape((4, 64, TOK), BF),) * 3,
        tp,
        (proj, saved, got),
        staged=(0,),
        limit=16,
    )


def prepare_body(t, ins, outs, scr):
    proj_ref, mixed_ref, slope_ref, slope_n_ref, stat_ref = outs
    all_saved = scr[0]

    def at(d):
        return pl.ds(pl.multiple_of(lax.bitwise_xor(t, d) * 64, 64), 64)

    proj_ref[at(0), :] = now(ins[0])[...]
    all_saved[at(0), :] = ins[1][...]
    proj_ref[at(1), :] = ins[2][0]
    all_saved[at(1), :] = ins[2][4]
    for d in range(1, 4):
        for other in range(2):
            proj_ref[at(2 * d + other), :] = ins[2 + d][other]
            all_saved[at(2 * d + other), :] = ins[2 + d][2 + other]
    saved = all_saved[...].astype(F32)
    mean = jnp.sum(saved, axis=0, keepdims=True) / CW
    var = jnp.sum(saved * saved, axis=0, keepdims=True) / CW - mean * mean
    inv = lax.rsqrt(var + EPS)
    normed = (saved - mean) * inv
    sig = jax.nn.sigmoid(normed)
    mixed_ref[...] = (normed * sig).astype(BF)
    slope = sig * (1.0 + normed * (1.0 - sig))
    slope_ref[...] = slope
    slope_n_ref[...] = slope * normed
    stat_ref[...] = jnp.concatenate([mean, inv, mean, inv, mean, inv, mean, inv], axis=0)


def prepare(tp, proj, saved, got):
    return call(
        prepare_body,
        (
            pltpu.HBM((CW, TOK), BF),
            pltpu.HBM((CW, TOK), BF),
            pltpu.HBM((CW, TOK), F32),
            pltpu.HBM((CW, TOK), F32),
            shape((8, TOK), F32),
        ),
        tp,
        (proj, saved, *got),
        staged=(0,),
        cuts={0: ((64, TOK), columns_of(256, lambda t: t))},
        scratch=[pltpu.VMEM((CW, TOK), BF)],
        flops=10**8,
    )


def tokens_body(t, ins, outs, scr):
    gs_ref, outer_ref, own_ref, lent_ref = outs
    routed = dot(now(ins[0])[...], ins[2][...])
    gs = (now(ins[1])[...].astype(F32) + routed).astype(BF)
    gs_ref[...] = gs
    outer = dot(gs, now(ins[4])[...], 0, 1)
    lane = iota((64, 128), 1) < 64
    for u in range(4):
        for i in range(4):
            block = outer[64 * i : 64 * i + 64, 128 * u : 128 * u + 128]
            turned = pltpu.roll(block, 64, 1)
            even = jnp.where(lane[0:32], block[0:32], turned[32:64])
            odd = jnp.where(lane[0:32], turned[0:32], block[32:64])
            outer_ref[8 * u + i] = even.astype(BF)
            outer_ref[8 * u + 4 + i] = odd.astype(BF)
    part_all = scr[0]
    part = dot(now(ins[3])[...], gs, 1, 1)
    part_all[...] = part
    first = jnp.sum(part * now(ins[5])[...], axis=0, keepdims=True)
    second = jnp.sum(part * now(ins[6])[...], axis=0, keepdims=True)
    sums = jnp.concatenate([first, second], axis=0)
    parted = split_sums(sums)

    def at(d):
        return pl.ds(pl.multiple_of(lax.bitwise_xor(t, d) * 64, 64), 64)

    for d in range(4):
        own_ref[d, 0:64, :] = part_all[at(2 * d), :]
        lent_ref[d, 0:64, :] = part_all[at(2 * d + 1), :].astype(BF)
        lent_ref[d, 64:72, :] = parted
    own_ref[0, 64:72, :] = jnp.concatenate([sums] * 4, axis=0)


def split_sums(sums):
    high = sums.astype(BF).astype(F32)
    low = sums - high
    return jnp.concatenate([high, low, high, low], axis=0).astype(BF)


def fold_body(t, ins, outs, scr):
    own, got = ins
    sums = own[0, 64:66, :] + got[0, 64:66, :].astype(F32) + got[0, 66:68, :].astype(F32)
    outs[0][0:64, :] = own[0, 0:64, :] + got[0, 0:64, :].astype(F32)
    outs[0][64:72, :] = jnp.concatenate([sums] * 4, axis=0)
    parted = split_sums(sums)
    for d in range(1, 4):
        outs[d][0:64, :] = (own[d, 0:64, :] + got[d, 0:64, :].astype(F32)).astype(BF)
        outs[d][64:72, :] = parted


def fold(tp, own, got):
    return call(
        fold_body,
        (shape((72, TOK), F32),) + (shape((72, TOK), BF),) * 3,
        tp,
        (own, got),
        flops=10**7,
        limit=16,
    )


def tokens(tp, back, upstream, ret, proj, mixed, slope, slope_n):
    return call(
        tokens_body,
        (
            shape((TOK, 256), BF),
            pltpu.HBM((SP, 32, 128), BF),
            shape((4, 72, TOK), F32),
            shape((4, 72, TOK), BF),
        ),
        tp,
        (back, upstream, ret, proj, mixed, slope, slope_n),
        staged=(0, 1, 4, 3, 5, 6),
        cuts={1: ((TOK, 256), columns_of(256, lambda t: t))},
        scratch=[pltpu.VMEM((CW, TOK), F32)],
        flops=10**9,
    )


def norm_body(t, ins, outs, scr):
    own, saved, stat = ins[0], ins[4], ins[5]
    mixed, sums = own[0:64, :], own[64:66, :]
    for got in ins[1:4]:
        mixed = mixed + got[0:64, :].astype(F32)
        sums = sums + got[64:66, :].astype(F32) + got[66:68, :].astype(F32)
    first, second = sums[0:1] / CW, sums[1:2] / CW
    mean, inv = stat[0:1, :], stat[1:2, :]
    normed = (saved[...].astype(F32) - mean) * inv
    sig = jax.nn.sigmoid(normed)
    grad = mixed * sig * (1.0 + normed * (1.0 - sig))
    conv_grad = inv * (grad - first - normed * second)
    outs[0][...] = conv_grad
    outs[1][...] = conv_grad[:, 0:128]


def norm(tp, own, got, saved, stat):
    return call(
        norm_body,
        (shape((64, TOK), F32), shape((64, 128), F32)),
        tp,
        (own, *got, saved, stat),
        flops=10**7,
        limit=16,
    )


def tap_sum(padded, taps):
    total = jnp.zeros((64, TOK), F32)
    width = padded.shape[1]
    for j in range(taps.shape[1]):
        turned = padded if j == 0 else pltpu.roll(padded, width - j, 1)
        total = total + taps[:, j : j + 1] * turned[:, 0:TOK]
    return total


def conv_own_body(t, ins, outs, scr):
    grad, taps = ins
    outs[0][...] = tap_sum(jnp.concatenate([grad[...], jnp.zeros((64, 128), F32)], axis=1), taps)


def conv_own(tp, grad, taps):
    return call(conv_own_body, shape((64, TOK), F32), tp, (grad, taps), flops=10**8, limit=16)


def conv_rim_body(t, ins, outs, scr):
    own, rim, taps, value, gate = ins
    dv_ref, dg_ref = outs
    both = jnp.concatenate([jnp.zeros((64, 128), F32), rim[...]], axis=1)
    reach = jnp.zeros((64, 128), F32)
    for j in range(1, taps.shape[1]):
        reach = reach + taps[:, j : j + 1] * pltpu.roll(both, TOK - j, 1)[:, 0:128]
    total = jnp.concatenate([own[:, 0:128], own[:, 128:256] + reach], axis=1)
    sig = jax.nn.sigmoid(gate[...].astype(F32))
    dv_ref[...] = (total * sig).astype(BF)
    dg_ref[...] = (total * value[...].astype(F32) * sig * (1.0 - sig)).astype(BF)


def conv_rim(tp, own, rim, taps, value, gate):
    return call(
        conv_rim_body,
        (shape((64, TOK), BF), shape((64, TOK), BF)),
        tp,
        (own, rim, taps, value, gate),
        flops=10**8,
        limit=16,
    )


def total_body(t, ins, outs, scr):
    whole = jnp.sum(ins[0][...].astype(F32), axis=0)
    outs[0][0:32, :] = whole[:, 0:64]
    outs[0][32:64, :] = whole[:, 64:128]


def total(tp, got):
    return call(total_body, shape((64, 64), F32), tp, (got,), flops=10**7, limit=16)


def moved(x, by):
    return lax.ppermute(x, "tp", [(i, (i + by) % TP) for i in range(TP)])


def swapped(x, by):
    return lax.ppermute(x, "tp", [(i, i ^ by) for i in range(TP)])


def across_moved(x, by):
    return lax.ppermute(x, "tp", [(i, ((i + by) % TP) ^ 1) for i in range(TP)])


def around(block):
    left, right = moved(block, 2), moved(block, -2)
    top, bottom = moved(left[:256], 2), moved(right[256:], -2)
    return block, left, right, top, bottom


def around_in_halves(block):
    upper, lower = block[:256], block[256:]
    left_upper, right_lower = moved(upper, 2), moved(lower, -2)
    left_lower, right_upper = moved(lower, 2), moved(upper, -2)
    top, bottom = moved(left_upper, 2), moved(right_lower, -2)
    return block, left_upper, left_lower, right_upper, right_lower, top, bottom


def exchange(x):
    return lax.all_to_all(x, "sp", 0, 0, tiled=True)


def after(x, *others):
    return lax.optimization_barrier((x, *others))[0]


def step(
    upstream, stream, routes, route_weights, glu_value, glu_gate, conv_taps, conv_saved,
    out_proj, expert_gate, expert_up, expert_down,
):
    tp = lax.axis_index("tp").reshape(1)
    rows_out, target = pick_rows(tp, routes.T, stream)
    rows_in = exchange(rows_out.reshape(SP, HALF, 512)).reshape(ROWS, 512)

    saved, proj = conv_saved.T, out_proj.T
    near_early = swapped(hand_out(tp, proj, saved), 1)
    far_early = hand_on(tp, proj, saved, near_early)
    early = (near_early, *(swapped(x, 2 * d + 2) for d, x in enumerate(far_early)))
    gate_own, up_own, down_own = expert_gate[0], expert_up[0], expert_down[0]
    gate_par, up_par, down_par = (swapped(w, 1) for w in (gate_own, up_own, down_own))

    cot_out, back = pick_cot(tp, target, route_weights.T, upstream)
    cot_out = after(cot_out, *early)
    cot_in = exchange(cot_out.reshape(SP, HALF, 512))
    cot_in = cot_in.reshape(ROWS, 512)
    proj_all, mixed, slope, slope_n, stat = prepare(tp, proj, saved, early)

    xs = around(rows_in)
    by_quarter = [w.reshape(4, 512, 256) for w in (gate_own, gate_par, up_own, up_par)]
    by_piece = [w.reshape(8, 256, 256) for w in (gate_own, gate_par, up_own, up_par)]
    act, a1, a2 = forward(tp, xs, by_quarter)

    cs = around_in_halves(cot_in)
    far_top, far_bottom, gg, gu = backward(tp, cs, (down_own, down_par), a1, a2, by_piece)
    got_top, got_bottom = moved(far_top, 2), moved(far_bottom, -2)
    parts = near(tp, gg, gu, by_piece)
    rs, rc, ls, lc = merge(tp, got_top, got_bottom, parts[:4])
    lent = lend(tp, xs, cs, gg, gu, after(act, rs))
    came = (moved(rs, 2), moved(ls, -2), across_moved(rc, 2), across_moved(lc, -2))
    own_cross = swapped(parts[5], 1)
    summed = settle(
        tp, (after(parts[4], lent), came[0], came[1], own_cross, came[2], came[3])
    )
    returned = exchange(summed).reshape(SP * CAP, 256)
    grads = keep(tp, xs, cs, gg, gu, act, swapped(lent, 1))
    grad_gate_w, grad_up_w, grad_down_w = grads
    back = after(back, grad_down_w)

    made = tokens(tp, back, upstream, returned, proj_all, mixed, slope, slope_n)
    grad_stream, outer, own_part, lent_part = made
    outer_in = exchange(outer)
    lent_in = swapped(lent_part, 1)
    folded = fold(tp, own_part, lent_in)
    own_part = folded[0]
    part_in = tuple(swapped(x, 2 * d + 2) for d, x in enumerate(folded[1:]))
    grad_conv, rim = norm(tp, own_part, part_in, saved, stat)
    rim_in = lax.ppermute(rim, "sp", [(i, i - 1) for i in range(1, SP)])
    taps = conv_taps.T
    grad_glu = conv_own(tp, grad_conv, taps)
    grad_value, grad_gate = conv_rim(tp, grad_glu, rim_in, taps, glu_value.T, glu_gate.T)
    grad_out_proj = lax.ppermute(
        total(tp, outer_in),
        ("sp", "tp"),
        [
            ((4 * u + i) * TP + t, (4 * t + i) * TP + u)
            for i in range(4)
            for u in range(TP)
            for t in range(TP)
        ],
    )
    return (
        grad_stream,
        grad_value.T,
        grad_gate.T,
        grad_out_proj,
        grad_gate_w.reshape(1, 2048, 256),
        grad_up_w.reshape(1, 2048, 256),
        grad_down_w[None],
    )


def solution(mesh):
    in_specs = (
        P("sp", None),
        P("sp", None),
        P("sp", None),
        P("sp", None),
        P("sp", "tp"),
        P("sp", "tp"),
        P(None, "tp"),
        P("sp", "tp"),
        P(None, "tp"),
        P("sp", None, "tp"),
        P("sp", None, "tp"),
        P("sp", "tp", None),
    )
    out_specs = (
        P("sp", "tp"),
        P("sp", "tp"),
        P("sp", "tp"),
        P("sp", "tp"),
        P("sp", None, "tp"),
        P("sp", None, "tp"),
        P("sp", "tp", None),
    )
    return jax.shard_map(step, mesh=mesh, in_specs=in_specs, out_specs=out_specs, check_vma=False)
```

```python
import jax
import jax.numpy as jnp
from jax import lax
from jax.experimental import pallas as pl
from jax.experimental.pallas import tpu as pltpu
from jax.sharding import PartitionSpec as P

CLAMP = 7.0
ALPHA = 1.702
EPS = 1e-05
CW = 512
CAP = 32
HALF = 16
SP = 32
TP = 8
TOK = 256
ROWS = SP * HALF
BF = jnp.bfloat16
F32 = jnp.float32
MIB = 1 << 20


def dot(a, b, ca=1, cb=0):
    return lax.dot_general(a, b, (((ca,), (cb,)), ((), ())), preferred_element_type=F32)


def flag(mask):
    return jnp.where(mask, 1.0, 0.0)


def iota(shape, dim):
    return lax.broadcasted_iota(jnp.int32, shape, dim)


class Later:
    def __init__(self, source, buffer, sem):
        self.copy, self.buffer, self.waiting = pltpu.make_async_copy(source, buffer, sem), buffer, True
        self.copy.start()

    def now(self):
        if self.waiting:
            self.copy.wait()
            self.waiting = False
        return self.buffer


def now(x):
    return x.now() if isinstance(x, Later) else x


def call(body, outs, tp, args, staged=(), cuts=None, into=None, scratch=(), flops=0, limit=40):
    cuts, into = cuts or {}, into or {}
    own = tuple(i for i in staged if i not in into)
    single = not isinstance(outs, tuple)
    outs = (outs,) if single else outs
    n_in, n_out, n_scr = len(args), len(outs), len(scratch)

    def kernel(t_ref, *refs):
        ins, rest = list(refs[:n_in]), refs[n_in:]
        made, scr, buffers = rest[:n_out], rest[n_out : n_out + n_scr], rest[n_out + n_scr :]
        for n, i in enumerate(staged):
            source = ins[i].at[cuts[i][1](t_ref[0])] if i in cuts else ins[i]
            if i in into:
                target = scr[into[i][0]].at[into[i][1](t_ref[0])]
            else:
                target = buffers[own.index(i)]
            ins[i] = Later(source, target, buffers[-1].at[n])
        body(t_ref[0], ins, made, scr)
        for i in staged:
            now(ins[i])

    extra = [
        pltpu.VMEM(cuts[i][0] if i in cuts else args[i].shape, args[i].dtype) for i in own
    ]
    if staged:
        extra.append(pltpu.SemaphoreType.DMA((len(staged),)))
    args = tuple(
        pltpu.with_memory_space_constraint(x, pltpu.HBM) if i in staged else x
        for i, x in enumerate(args)
    )
    made = pl.pallas_call(
        kernel,
        out_shape=outs,
        in_specs=[SMEM] + [HBM if i in staged else VMEM for i in range(n_in)],
        out_specs=(VMEM,) * n_out,
        scratch_shapes=list(scratch) + extra,
        compiler_params=pltpu.CompilerParams(vmem_limit_bytes=limit * MIB),
        cost_estimate=pl.CostEstimate(flops=flops, bytes_accessed=MIB, transcendentals=0),
    )(tp, *args)
    return made[0] if single else made


def shape(dims, dtype):
    return jax.ShapeDtypeStruct(dims, dtype)


SMEM = pl.BlockSpec(memory_space=pltpu.SMEM)
VMEM = pl.BlockSpec(memory_space=pltpu.VMEM)
HBM = pl.BlockSpec(memory_space=pltpu.HBM)


def columns_of(width, which):
    return lambda t: (slice(None), pl.ds(pl.multiple_of(which(t) * width, width), width))


def pick_rows_body(t, ins, outs, scr):
    core = t % 2
    r = ins[0][...]
    r0, r1 = r[0:1, :], r[1:2, :]
    expert = iota((SP, TOK), 0)
    named0, named1 = expert == r0, expert == r1
    both = (flag(named0) + flag(named1)).astype(BF)
    before = flag(iota((TOK, TOK), 0) < iota((TOK, TOK), 1)).astype(BF)
    earlier = dot(both, before)
    slot0 = jnp.sum(jnp.where(named0, earlier, 0.0), axis=0, keepdims=True).astype(jnp.int32)
    slot1 = jnp.sum(jnp.where(named1, earlier, 0.0), axis=0, keepdims=True).astype(jnp.int32)
    l0 = jnp.where(slot0 // HALF == core, r0 * HALF + slot0 - HALF * core, -1)
    l1 = jnp.where(slot1 // HALF == core, r1 * HALF + slot1 - HALF * core, -1)
    b0 = r0 * CAP + (slot0 + HALF * core) % CAP
    b1 = r1 * CAP + (slot1 + HALF * core) % CAP
    outs[1][...] = jnp.concatenate([l0, l1, b0, b1, l0, l1, b0, b1], axis=0)
    place = iota((ROWS, TOK), 0)
    pick = flag((place == l0) | (place == l1)).astype(BF)
    outs[0][...] = dot(pick, now(ins[1])[...]).astype(BF)


def pick_rows(tp, routes, stream):
    return call(
        pick_rows_body,
        (pltpu.HBM((ROWS, 512), BF), shape((8, TOK), jnp.int32)),
        tp,
        (routes, stream),
        staged=(1,),
        cuts={1: ((TOK, 512), columns_of(512, lambda t: t // 2))},
        flops=10**9,
    )


def pick_cot_body(t, ins, outs, scr):
    tgt, w = ins[0][...], ins[1][...]
    table = jnp.concatenate([tgt[2:4, :].astype(F32), w, tgt[2:4, :].astype(F32), w], axis=0)
    columns = jnp.transpose(jnp.concatenate([table] * 16, axis=0))
    up = now(ins[2])[...].astype(F32)
    cot0 = (columns[:, 2:3] * up).astype(BF)
    cot1 = (columns[:, 3:4] * up).astype(BF)
    place = iota((ROWS, TOK), 0)
    cot = dot(flag(place == tgt[0:1, :]).astype(BF), cot0)
    cot = cot + dot(flag(place == tgt[1:2, :]).astype(BF), cot1)
    outs[0][...] = cot.astype(BF)
    b0 = columns[:, 0:1].astype(jnp.int32)
    b1 = columns[:, 1:2].astype(jnp.int32)
    spot = iota((TOK, SP * CAP), 1)
    outs[1][...] = flag((spot == b0) | (spot == b1)).astype(BF)


def pick_cot(tp, target, weights, upstream):
    return call(
        pick_cot_body,
        (pltpu.HBM((ROWS, 512), BF), pltpu.HBM((TOK, SP * CAP), BF)),
        tp,
        (target, weights, upstream),
        staged=(2,),
        cuts={2: ((TOK, 512), columns_of(512, lambda t: t // 2))},
        flops=10**9,
    )


def quarters(t):
    y = t // 2
    return y, (y + 3) % 4, (y + 1) % 4, (y + 2) % 4


def joined(refs):
    refs = [now(r)[...] for r in refs]
    own, sides, far = refs[0], refs[1:-2], jnp.concatenate(refs[-2:], axis=0)
    if len(sides) == 4:
        sides = [jnp.concatenate(sides[0:2], axis=0), jnp.concatenate(sides[2:4], axis=0)]
    return own, *sides, far


def forward_body(t, ins, outs, scr):
    act_ref, a1_ref, a2_ref = outs
    pg, pu = scr
    q = quarters(t)
    x = joined(ins[0:5])
    for j in range(2):
        cols = slice(256 * j, 256 * j + 256)
        g = now(ins[5 + j])
        pg[:, cols] = sum(dot(x[i], g[q[i]]) for i in range(4))
        u = now(ins[7 + j])
        pu[:, cols] = sum(dot(x[i], u[q[i]]) for i in range(4))

    @pl.loop(0, ROWS // 32)
    def _(i):
        at = pl.ds(pl.multiple_of(i * 32, 32), 32)
        gate_pre, up_pre = pg[at, :], pu[at, :]
        capped = jnp.minimum(gate_pre, CLAMP)
        clipped = jnp.clip(up_pre, -CLAMP, CLAMP)
        sig = jax.nn.sigmoid(ALPHA * capped)
        gated = capped * sig
        act_ref[at, :] = (gated * (clipped + 1.0)).astype(BF)
        slope = sig + ALPHA * gated * (1.0 - sig)
        a1_ref[at, :] = jnp.where(gate_pre < CLAMP, (clipped + 1.0) * slope, 0.0)
        a2_ref[at, :] = jnp.where(jnp.abs(up_pre) < CLAMP, gated, 0.0)


def forward(tp, blocks, weights):
    return call(
        forward_body,
        (shape((ROWS, 512), BF), shape((ROWS, 512), F32), shape((ROWS, 512), F32)),
        tp,
        (*blocks, *weights),
        staged=(5, 3, 4, 7, 6, 8),
        scratch=[pltpu.VMEM((ROWS, 512), F32)] * 2,
        flops=2 * 10**9,
    )


def partial_of(g, u, weights, piece):
    g0, g1, u0, u1 = weights
    return (
        dot(g[:, 0:256], g0[piece], 1, 1)
        + dot(g[:, 256:512], g1[piece], 1, 1)
        + dot(u[:, 0:256], u0[piece], 1, 1)
        + dot(u[:, 256:512], u1[piece], 1, 1)
    )


def down_columns(d, quarter):
    return d[:, pl.ds(pl.multiple_of(quarter * 512, 512), 512)]


def three_body(t, ins, outs, scr):
    q = quarters(t)
    own = ins[0][...]
    sides = [(q[1], ins[1], ins[2]), (q[2], ins[3], ins[4])]
    for j in range(2):
        d = now(ins[5 + j])
        cols = slice(256 * j, 256 * j + 256)
        outs[0][:, cols] = dot(own, down_columns(d, q[0]), 1, 1)
        for at, upper, lower in sides:
            part = down_columns(d, at)
            outs[0][0:256, cols] += dot(upper[...], part, 1, 1)
            outs[0][256:512, cols] += dot(lower[...], part, 1, 1)


def three(tp, blocks, downs):
    return call(
        three_body,
        shape((ROWS, 512), F32),
        tp,
        (*blocks, *downs),
        staged=(5, 6),
        flops=10**9,
        limit=32,
    )


def backward_body(t, ins, outs, scr):
    top_ref, bottom_ref, gg_ref, gu_ref = outs
    top, bottom, ga, a1, a2 = ins[0:5]
    far = scr[0]
    for j in range(2):
        d = now(ins[5 + j])[...]
        cols = slice(256 * j, 256 * j + 256)
        far[0:256, cols] = dot(top[...], d, 1, 1)
        far[256:512, cols] = dot(bottom[...], d, 1, 1)

    @pl.loop(0, ROWS // 32)
    def _(i):
        at = pl.ds(pl.multiple_of(i * 32, 32), 32)
        grad = ga[at, :] + far[at, :]
        gg_ref[at, :] = (grad * a1[at, :]).astype(BF)
        gu_ref[at, :] = (grad * a2[at, :]).astype(BF)

    g, u = gg_ref[...], gu_ref[...]
    weights = [now(w) for w in ins[7:11]]
    for half in range(2):
        part = partial_of(g, u, weights, half).astype(BF)
        top_ref[half] = part[0:256]
        bottom_ref[half] = part[256:512]


def backward(tp, far, ga, downs, a1, a2, weights):
    pieces = ((2, 256, 256), lambda t: (pl.ds(2 * ((t // 2 + 2) % 4), 2),))
    columns = ((256, 512), columns_of(512, lambda t: (t // 2 + 2) % 4))
    return call(
        backward_body,
        (
            shape((2, 256, 256), BF),
            shape((2, 256, 256), BF),
            shape((ROWS, 512), BF),
            shape((ROWS, 512), BF),
        ),
        tp,
        (*far, ga, a1, a2, *downs, *weights),
        staged=(5, 6, 7, 8, 9, 10),
        cuts={5: columns, 6: columns} | {i: pieces for i in range(7, 11)},
        scratch=[pltpu.VMEM((ROWS, 512), F32)],
        flops=2 * 10**9,
        limit=32,
    )


def near_body(t, ins, outs, scr):
    g, u = ins[0][...], ins[1][...]
    weights = [now(w) for w in ins[2:6]]
    right, left = (t + 2) % 8, (t + 6) % 8
    swap = 1 - 2 * (t % 2)
    pieces = (right, right + swap, left, left + swap, t, t + swap)
    for ref, piece in zip(outs, pieces):
        ref[...] = partial_of(g, u, weights, piece).astype(BF)


def near(tp, gg, gu, weights):
    return call(
        near_body,
        (shape((ROWS, 256), BF),) * 6,
        tp,
        (gg, gu, *weights),
        staged=(2, 3, 4, 5),
        flops=3 * 10**9,
    )


def merge_body(t, ins, outs, scr):
    core = t % 2
    top, bottom = ins[0:2]
    for src, dst, got, first in (
        (ins[2], outs[0], top[core], True),
        (ins[3], outs[1], top[1 - core], True),
        (ins[4], outs[2], bottom[core], False),
        (ins[5], outs[3], bottom[1 - core], False),
    ):
        hit, other = (slice(0, 256), slice(256, 512)) if first else (slice(256, 512), slice(0, 256))
        dst[hit, :] = (src[hit, :].astype(F32) + got.astype(F32)).astype(BF)
        dst[other, :] = src[other, :]


def merge(tp, top, bottom, parts):
    return call(
        merge_body, (shape((ROWS, 256), BF),) * 4, tp, (top, bottom, *parts), flops=10**7, limit=16
    )


def settle_body(t, ins, outs, scr):
    a0, a1, a2, b0, b1, b2 = [x[...].astype(F32) for x in ins]
    outs[0][:, 0:HALF, :] = (a0 + a1 + a2).astype(BF).reshape(SP, HALF, 256)
    outs[0][:, HALF:CAP, :] = (b0 + b1 + b2).astype(BF).reshape(SP, HALF, 256)


def settle(tp, parts):
    return call(settle_body, pltpu.HBM((SP, CAP, 256), BF), tp, parts, flops=10**7, limit=16)


def by_column(scr_index, first, halves):
    whole, upper, lower = slice(None), slice(0, 256), slice(256, 512)
    sides = ((3, upper), (3, lower), (1, upper), (1, lower)) if halves else ((3, whole), (1, whole))
    places = ((0, whole), *sides, (2, upper), (2, lower))
    return {
        first + n: (scr_index, lambda t, by=by, rows=rows: ((t // 2 + by) % 4, rows))
        for n, (by, rows) in enumerate(places)
    }


def weights_call(body, outs, tp, args):
    return call(
        body,
        outs,
        tp,
        args,
        staged=tuple(range(len(args))),
        into=by_column(0, 0, False) | by_column(1, 5, True),
        scratch=[pltpu.VMEM((4, ROWS, 512), BF)] * 2,
        flops=2 * 10**9,
    )


def each_quarter(ins, scr, cols, store):
    ins = [now(x) for x in ins]
    gg, gu, act = ins[12:15]
    gu_cols = jnp.concatenate([gg[:, cols], gu[:, cols]], axis=1)
    act_cols = act[:, cols]

    @pl.loop(0, 4)
    def _(q):
        store(q, dot(scr[0][q], gu_cols, 0, 0), dot(act_cols, scr[1][q], 0, 0))


def lend_body(t, ins, outs, scr):
    def store(q, both, down):
        outs[0][q] = both[:, 0:256].astype(BF)
        outs[0][4 + q] = both[:, 256:512].astype(BF)
        outs[0][8 + q, 0:256, :] = down[:, 0:256].astype(BF)
        outs[0][8 + q, 256:512, :] = down[:, 256:512].astype(BF)

    each_quarter(ins, scr, slice(256, 512), store)


def lend(tp, xs, cs, gg, gu, act):
    return weights_call(
        lend_body, shape((12, 512, 256), BF), tp, (*xs, *cs, gg, gu, act)
    )


def keep_body(t, ins, outs, scr):
    gate_ref, up_ref, down_ref = outs

    def store(q, both, down):
        lent = now(ins[15])
        gate_ref[q] = both[:, 0:256] + lent[q].astype(F32)
        up_ref[q] = both[:, 256:512] + lent[4 + q].astype(F32)
        for half in range(2):
            cols = slice(256 * half, 256 * half + 256)
            at = pl.ds(pl.multiple_of(q * 512 + 256 * half, 256), 256)
            down_ref[:, at] = down[:, cols] + lent[8 + q, cols, :].astype(F32)

    each_quarter(ins, scr, slice(0, 256), store)


def keep(tp, xs, cs, gg, gu, act, lent):
    return weights_call(
        keep_body,
        (shape((4, 512, 256), F32), shape((4, 512, 256), F32), shape((256, 2048), F32)),
        tp,
        (*xs, *cs, gg, gu, act, lent),
    )


def hand_out_body(t, ins, outs, scr):
    proj = now(ins[0])
    for d in range(4):
        other = lax.bitwise_xor(t, 2 * d + 1)
        outs[0][d] = proj[:, pl.ds(pl.multiple_of(other * 256, 256), 256)]
    outs[0][4] = ins[1][...]


def hand_out(tp, proj, saved):
    return call(
        hand_out_body, shape((5, 64, TOK), BF), tp, (proj, saved), staged=(0,), limit=16
    )


def hand_on_body(t, ins, outs, scr):
    proj = now(ins[0])
    for d in range(1, 4):
        other = lax.bitwise_xor(t, 2 * d)
        outs[d - 1][0] = proj[:, pl.ds(pl.multiple_of(other * 256, 256), 256)]
        outs[d - 1][1] = ins[2][d]
        outs[d - 1][2] = ins[1][...]
        outs[d - 1][3] = ins[2][4]


def hand_on(tp, proj, saved, got):
    return call(
        hand_on_body,
        (shape((4, 64, TOK), BF),) * 3,
        tp,
        (proj, saved, got),
        staged=(0,),
        limit=16,
    )


def prepare_body(t, ins, outs, scr):
    proj_ref, mixed_ref, slope_ref, slope_n_ref, stat_ref = outs
    all_saved = scr[0]

    def at(d):
        return pl.ds(pl.multiple_of(lax.bitwise_xor(t, d) * 64, 64), 64)

    proj_ref[at(0), :] = now(ins[0])[...]
    all_saved[at(0), :] = ins[1][...]
    proj_ref[at(1), :] = ins[2][0]
    all_saved[at(1), :] = ins[2][4]
    for d in range(1, 4):
        for other in range(2):
            proj_ref[at(2 * d + other), :] = ins[2 + d][other]
            all_saved[at(2 * d + other), :] = ins[2 + d][2 + other]
    saved = all_saved[...].astype(F32)
    mean = jnp.sum(saved, axis=0, keepdims=True) / CW
    var = jnp.sum(saved * saved, axis=0, keepdims=True) / CW - mean * mean
    inv = lax.rsqrt(var + EPS)
    normed = (saved - mean) * inv
    sig = jax.nn.sigmoid(normed)
    mixed_ref[...] = (normed * sig).astype(BF)
    slope = sig * (1.0 + normed * (1.0 - sig))
    slope_ref[...] = slope
    slope_n_ref[...] = slope * normed
    stat_ref[...] = jnp.concatenate([mean, inv, mean, inv, mean, inv, mean, inv], axis=0)


def prepare(tp, proj, saved, got):
    return call(
        prepare_body,
        (
            pltpu.HBM((CW, TOK), BF),
            pltpu.HBM((CW, TOK), BF),
            pltpu.HBM((CW, TOK), F32),
            pltpu.HBM((CW, TOK), F32),
            shape((8, TOK), F32),
        ),
        tp,
        (proj, saved, *got),
        staged=(0,),
        cuts={0: ((64, TOK), columns_of(256, lambda t: t))},
        scratch=[pltpu.VMEM((CW, TOK), BF)],
        flops=10**8,
    )


def tokens_body(t, ins, outs, scr):
    gs_ref, outer_ref, own_ref, lent_ref = outs
    routed = dot(now(ins[0])[...], now(ins[2])[...])
    gs = (now(ins[1])[...].astype(F32) + routed).astype(BF)
    gs_ref[...] = gs
    outer = dot(gs, now(ins[4])[...], 0, 1)
    lane = iota((64, 128), 1) < 64
    for u in range(4):
        for i in range(4):
            block = outer[64 * i : 64 * i + 64, 128 * u : 128 * u + 128]
            turned = pltpu.roll(block, 64, 1)
            even = jnp.where(lane[0:32], block[0:32], turned[32:64])
            odd = jnp.where(lane[0:32], turned[0:32], block[32:64])
            outer_ref[8 * u + i] = even.astype(BF)
            outer_ref[8 * u + 4 + i] = odd.astype(BF)
    part_all = scr[0]
    part = dot(now(ins[3])[...], gs, 1, 1)
    part_all[...] = part
    first = jnp.sum(part * now(ins[5])[...], axis=0, keepdims=True)
    second = jnp.sum(part * now(ins[6])[...], axis=0, keepdims=True)
    sums = jnp.concatenate([first, second], axis=0)
    parted = split_sums(sums)

    def at(d):
        return pl.ds(pl.multiple_of(lax.bitwise_xor(t, d) * 64, 64), 64)

    for d in range(4):
        own_ref[d, 0:64, :] = part_all[at(2 * d), :]
        lent_ref[d, 0:64, :] = part_all[at(2 * d + 1), :].astype(BF)
        lent_ref[d, 64:72, :] = parted
    own_ref[0, 64:72, :] = jnp.concatenate([sums] * 4, axis=0)


def split_sums(sums):
    high = sums.astype(BF).astype(F32)
    low = sums - high
    return jnp.concatenate([high, low, high, low], axis=0).astype(BF)


def fold_body(t, ins, outs, scr):
    own, got = ins
    sums = own[0, 64:66, :] + got[0, 64:66, :].astype(F32) + got[0, 66:68, :].astype(F32)
    outs[0][0:64, :] = own[0, 0:64, :] + got[0, 0:64, :].astype(F32)
    outs[0][64:72, :] = jnp.concatenate([sums] * 4, axis=0)
    parted = split_sums(sums)
    for d in range(1, 4):
        outs[d][0:64, :] = (own[d, 0:64, :] + got[d, 0:64, :].astype(F32)).astype(BF)
        outs[d][64:72, :] = parted


def fold(tp, own, got):
    return call(
        fold_body,
        (shape((72, TOK), F32),) + (shape((72, TOK), BF),) * 3,
        tp,
        (own, got),
        flops=10**7,
        limit=16,
    )


def tokens(tp, back, upstream, ret, proj, mixed, slope, slope_n):
    return call(
        tokens_body,
        (
            shape((TOK, 256), BF),
            pltpu.HBM((SP, 32, 128), BF),
            shape((4, 72, TOK), F32),
            shape((4, 72, TOK), BF),
        ),
        tp,
        (back, upstream, ret, proj, mixed, slope, slope_n),
        staged=(0, 2, 1, 4, 3, 5, 6),
        cuts={1: ((TOK, 256), columns_of(256, lambda t: t))},
        scratch=[pltpu.VMEM((CW, TOK), F32)],
        flops=10**9,
    )


def norm_body(t, ins, outs, scr):
    own, saved, stat = ins[0], ins[4], ins[5]
    mixed, sums = own[0:64, :], own[64:66, :]
    for got in ins[1:4]:
        mixed = mixed + got[0:64, :].astype(F32)
        sums = sums + got[64:66, :].astype(F32) + got[66:68, :].astype(F32)
    first, second = sums[0:1] / CW, sums[1:2] / CW
    mean, inv = stat[0:1, :], stat[1:2, :]
    normed = (saved[...].astype(F32) - mean) * inv
    sig = jax.nn.sigmoid(normed)
    grad = mixed * sig * (1.0 + normed * (1.0 - sig))
    conv_grad = inv * (grad - first - normed * second)
    outs[0][...] = conv_grad
    outs[1][...] = conv_grad[:, 0:128]


def norm(tp, own, got, saved, stat):
    return call(
        norm_body,
        (shape((64, TOK), F32), shape((64, 128), F32)),
        tp,
        (own, *got, saved, stat),
        flops=10**7,
        limit=16,
    )


def tap_sum(padded, taps):
    total = jnp.zeros((64, TOK), F32)
    width = padded.shape[1]
    for j in range(taps.shape[1]):
        turned = padded if j == 0 else pltpu.roll(padded, width - j, 1)
        total = total + taps[:, j : j + 1] * turned[:, 0:TOK]
    return total


def conv_own_body(t, ins, outs, scr):
    grad, taps = ins
    outs[0][...] = tap_sum(jnp.concatenate([grad[...], jnp.zeros((64, 128), F32)], axis=1), taps)


def conv_own(tp, grad, taps):
    return call(conv_own_body, shape((64, TOK), F32), tp, (grad, taps), flops=10**8, limit=16)


def conv_rim_body(t, ins, outs, scr):
    own, rim, taps, value, gate = ins
    dv_ref, dg_ref = outs
    both = jnp.concatenate([jnp.zeros((64, 128), F32), rim[...]], axis=1)
    reach = jnp.zeros((64, 128), F32)
    for j in range(1, taps.shape[1]):
        reach = reach + taps[:, j : j + 1] * pltpu.roll(both, TOK - j, 1)[:, 0:128]
    total = jnp.concatenate([own[:, 0:128], own[:, 128:256] + reach], axis=1)
    sig = jax.nn.sigmoid(gate[...].astype(F32))
    dv_ref[...] = (total * sig).astype(BF)
    dg_ref[...] = (total * value[...].astype(F32) * sig * (1.0 - sig)).astype(BF)


def conv_rim(tp, own, rim, taps, value, gate):
    return call(
        conv_rim_body,
        (shape((64, TOK), BF), shape((64, TOK), BF)),
        tp,
        (own, rim, taps, value, gate),
        flops=10**8,
        limit=16,
    )


def total_body(t, ins, outs, scr):
    whole = jnp.sum(ins[0][...].astype(F32), axis=0)
    outs[0][0:32, :] = whole[:, 0:64]
    outs[0][32:64, :] = whole[:, 64:128]


def total(tp, got):
    return call(total_body, shape((64, 64), F32), tp, (got,), flops=10**7, limit=16)


def moved(x, by):
    return lax.ppermute(x, "tp", [(i, (i + by) % TP) for i in range(TP)])


def swapped(x, by):
    return lax.ppermute(x, "tp", [(i, i ^ by) for i in range(TP)])


def across_moved(x, by):
    return lax.ppermute(x, "tp", [(i, ((i + by) % TP) ^ 1) for i in range(TP)])


def around(block):
    left, right = moved(block, 2), moved(block, -2)
    top, bottom = moved(left[:256], 2), moved(right[256:], -2)
    return block, left, right, top, bottom


def around_in_halves(block):
    upper, lower = block[:256], block[256:]
    left_upper, right_lower = moved(upper, 2), moved(lower, -2)
    left_lower, right_upper = moved(lower, 2), moved(upper, -2)
    top, bottom = moved(left_upper, 2), moved(right_lower, -2)
    return block, left_upper, left_lower, right_upper, right_lower, top, bottom


def exchange(x):
    return lax.all_to_all(x, "sp", 0, 0, tiled=True)


def after(x, *others):
    return lax.optimization_barrier((x, *others))[0]


def step(
    upstream, stream, routes, route_weights, glu_value, glu_gate, conv_taps, conv_saved,
    out_proj, expert_gate, expert_up, expert_down,
):
    tp = lax.axis_index("tp").reshape(1)
    rows_out, target = pick_rows(tp, routes.T, stream)
    rows_in = exchange(rows_out.reshape(SP, HALF, 512)).reshape(ROWS, 512)

    saved, proj = conv_saved.T, out_proj.T
    near_early = swapped(hand_out(tp, proj, saved), 1)
    far_early = hand_on(tp, proj, saved, near_early)
    early = (near_early, *(swapped(x, 2 * d + 2) for d, x in enumerate(far_early)))
    gate_own, up_own, down_own = expert_gate[0], expert_up[0], expert_down[0]
    gate_par, up_par, down_par = (swapped(w, 1) for w in (gate_own, up_own, down_own))

    cot_out, back = pick_cot(tp, target, route_weights.T, upstream)
    cot_out = after(cot_out, *early)
    cot_in = exchange(cot_out.reshape(SP, HALF, 512))
    cot_in = cot_in.reshape(ROWS, 512)
    proj_all, mixed, slope, slope_n, stat = prepare(tp, proj, saved, early)

    xs = around(rows_in)
    by_quarter = [w.reshape(4, 512, 256) for w in (gate_own, gate_par, up_own, up_par)]
    by_piece = [w.reshape(8, 256, 256) for w in (gate_own, gate_par, up_own, up_par)]
    act, a1, a2 = forward(tp, xs, by_quarter)

    cs = around_in_halves(cot_in)
    downs = (down_own, down_par)
    ga = three(tp, cs[:5], downs)
    far_top, far_bottom, gg, gu = backward(tp, cs[5:], ga, downs, a1, a2, by_piece)
    got_top, got_bottom = moved(far_top, 2), moved(far_bottom, -2)
    parts = near(tp, gg, gu, by_piece)
    rs, rc, ls, lc = merge(tp, got_top, got_bottom, parts[:4])
    lent = lend(tp, xs, cs, gg, gu, after(act, rs))
    came = (moved(rs, 2), moved(ls, -2), across_moved(rc, 2), across_moved(lc, -2))
    own_cross = swapped(parts[5], 1)
    summed = settle(
        tp, (after(parts[4], lent), came[0], came[1], own_cross, came[2], came[3])
    )
    returned = exchange(summed).reshape(SP * CAP, 256)
    grads = keep(tp, xs, cs, gg, gu, act, swapped(lent, 1))
    grad_gate_w, grad_up_w, grad_down_w = grads
    back = after(back, grad_down_w)

    made = tokens(tp, back, upstream, returned, proj_all, mixed, slope, slope_n)
    grad_stream, outer, own_part, lent_part = made
    outer_in = exchange(outer)
    lent_in = swapped(lent_part, 1)
    folded = fold(tp, own_part, lent_in)
    own_part = folded[0]
    part_in = tuple(swapped(x, 2 * d + 2) for d, x in enumerate(folded[1:]))
    grad_conv, rim = norm(tp, own_part, part_in, saved, stat)
    rim_in = lax.ppermute(rim, "sp", [(i, i - 1) for i in range(1, SP)])
    taps = conv_taps.T
    grad_glu = conv_own(tp, grad_conv, taps)
    grad_value, grad_gate = conv_rim(tp, grad_glu, rim_in, taps, glu_value.T, glu_gate.T)
    grad_out_proj = lax.ppermute(
        total(tp, outer_in),
        ("sp", "tp"),
        [
            ((4 * u + i) * TP + t, (4 * t + i) * TP + u)
            for i in range(4)
            for u in range(TP)
            for t in range(TP)
        ],
    )
    return (
        grad_stream,
        grad_value.T,
        grad_gate.T,
        grad_out_proj,
        grad_gate_w.reshape(1, 2048, 256),
        grad_up_w.reshape(1, 2048, 256),
        grad_down_w[None],
    )


def solution(mesh):
    in_specs = (
        P("sp", None),
        P("sp", None),
        P("sp", None),
        P("sp", None),
        P("sp", "tp"),
        P("sp", "tp"),
        P(None, "tp"),
        P("sp", "tp"),
        P(None, "tp"),
        P("sp", None, "tp"),
        P("sp", None, "tp"),
        P("sp", "tp", None),
    )
    out_specs = (
        P("sp", "tp"),
        P("sp", "tp"),
        P("sp", "tp"),
        P("sp", "tp"),
        P("sp", None, "tp"),
        P("sp", None, "tp"),
        P("sp", "tp", None),
    )
    return jax.shard_map(step, mesh=mesh, in_specs=in_specs, out_specs=out_specs, check_vma=False)
```

```python
import jax
import jax.numpy as jnp
from jax import lax
from jax.experimental import pallas as pl
from jax.experimental.pallas import tpu as pltpu
from jax.sharding import PartitionSpec as P

CLAMP = 7.0
ALPHA = 1.702
EPS = 1e-05
CW = 512
CAP = 32
HALF = 16
SP = 32
TP = 8
TOK = 256
ROWS = SP * HALF
EARLY = 128
LATE = 512 - EARLY
FIRST = 512 + EARLY
BF = jnp.bfloat16
F32 = jnp.float32
MIB = 1 << 20


def dot(a, b, ca=1, cb=0):
    return lax.dot_general(a, b, (((ca,), (cb,)), ((), ())), preferred_element_type=F32)


def flag(mask):
    return jnp.where(mask, 1.0, 0.0)


def iota(shape, dim):
    return lax.broadcasted_iota(jnp.int32, shape, dim)


class Later:
    def __init__(self, copies, buffer):
        self.copies, self.buffer = copies, buffer
        for copy in copies:
            copy.start()

    def now(self):
        for copy in self.copies:
            copy.wait()
        self.copies = []
        return self.buffer


def now(x):
    return x.now() if isinstance(x, Later) else x


def call(body, outs, tp, args, staged=(), cuts=None, into=None, scratch=(), flops=0, limit=40):
    cuts, into = cuts or {}, into or {}
    own = tuple(i for i in staged if i not in into)
    n_copies = sum(len(into[i]) if i in into else 1 for i in staged)
    single = not isinstance(outs, tuple)
    outs = (outs,) if single else outs
    n_in, n_out, n_scr = len(args), len(outs), len(scratch)

    def kernel(t_ref, *refs):
        ins, rest = list(refs[:n_in]), refs[n_in:]
        made, scr, buffers = rest[:n_out], rest[n_out : n_out + n_scr], rest[n_out + n_scr :]
        t, sems = t_ref[0], iter(range(n_copies))
        for i in staged:
            if i in into:
                pairs = [(ins[i].at[cut], scr[k].at[to(t)]) for cut, k, to in into[i]]
            else:
                source = ins[i].at[cuts[i][1](t)] if i in cuts else ins[i]
                pairs = [(source, buffers[own.index(i)])]
            copies = [
                pltpu.make_async_copy(source, target, buffers[-1].at[next(sems)])
                for source, target in pairs
            ]
            ins[i] = Later(copies, pairs[0][1])
        body(t_ref[0], ins, made, scr)
        for i in staged:
            now(ins[i])

    extra = [
        pltpu.VMEM(cuts[i][0] if i in cuts else args[i].shape, args[i].dtype) for i in own
    ]
    if staged:
        extra.append(pltpu.SemaphoreType.DMA((n_copies,)))
    args = tuple(
        pltpu.with_memory_space_constraint(x, pltpu.HBM) if i in staged else x
        for i, x in enumerate(args)
    )
    made = pl.pallas_call(
        kernel,
        out_shape=outs,
        in_specs=[SMEM] + [HBM if i in staged else VMEM for i in range(n_in)],
        out_specs=(VMEM,) * n_out,
        scratch_shapes=list(scratch) + extra,
        compiler_params=pltpu.CompilerParams(vmem_limit_bytes=limit * MIB),
        cost_estimate=pl.CostEstimate(flops=flops, bytes_accessed=MIB, transcendentals=0),
    )(tp, *args)
    return made[0] if single else made


def shape(dims, dtype):
    return jax.ShapeDtypeStruct(dims, dtype)


SMEM = pl.BlockSpec(memory_space=pltpu.SMEM)
VMEM = pl.BlockSpec(memory_space=pltpu.VMEM)
HBM = pl.BlockSpec(memory_space=pltpu.HBM)


def columns_of(width, which):
    return lambda t: (slice(None), pl.ds(pl.multiple_of(which(t) * width, width), width))


def pick_rows_body(t, ins, outs, scr):
    core = t % 2
    r = ins[0][...]
    r0, r1 = r[0:1, :], r[1:2, :]
    expert = iota((SP, TOK), 0)
    named0, named1 = expert == r0, expert == r1
    both = (flag(named0) + flag(named1)).astype(BF)
    before = flag(iota((TOK, TOK), 0) < iota((TOK, TOK), 1)).astype(BF)
    earlier = dot(both, before)
    slot0 = jnp.sum(jnp.where(named0, earlier, 0.0), axis=0, keepdims=True).astype(jnp.int32)
    slot1 = jnp.sum(jnp.where(named1, earlier, 0.0), axis=0, keepdims=True).astype(jnp.int32)
    l0 = jnp.where(slot0 // HALF == core, r0 * HALF + slot0 - HALF * core, -1)
    l1 = jnp.where(slot1 // HALF == core, r1 * HALF + slot1 - HALF * core, -1)
    b0 = r0 * CAP + (slot0 + HALF * core) % CAP
    b1 = r1 * CAP + (slot1 + HALF * core) % CAP
    outs[1][...] = jnp.concatenate([l0, l1, b0, b1, l0, l1, b0, b1], axis=0)
    place = iota((ROWS, TOK), 0)
    at0, at1 = place == l0, place == l1
    pick = flag(at0 | at1).astype(BF)
    w = ins[2][...]
    scale = jnp.where(at0, w[0:1, :], 0.0) + jnp.where(at1, w[1:2, :], 0.0)
    scale = jnp.sum(scale, axis=1, keepdims=True)
    outs[0][:, 0:512] = dot(pick, now(ins[1])[...]).astype(BF)
    outs[0][:, 512:FIRST] = (scale * dot(pick, now(ins[3])[...])).astype(BF)


def pick_rows(tp, routes, stream, weights, upstream):
    return call(
        pick_rows_body,
        (pltpu.HBM((ROWS, FIRST), BF), shape((8, TOK), jnp.int32)),
        tp,
        (routes, stream, weights, upstream),
        staged=(1, 3),
        cuts={
            1: ((TOK, 512), columns_of(512, lambda t: t // 2)),
            3: ((TOK, EARLY), columns_of(EARLY, lambda t: t // 2 * (512 // EARLY))),
        },
        flops=10**9,
    )


def pick_cot_body(t, ins, outs, scr):
    tgt, w = ins[0][...], ins[1][...]
    table = jnp.concatenate([tgt[2:4, :].astype(F32), w, tgt[2:4, :].astype(F32), w], axis=0)
    columns = jnp.transpose(jnp.concatenate([table] * 16, axis=0))
    up = now(ins[2])[...].astype(F32)
    cot0 = (columns[:, 2:3] * up).astype(BF)
    cot1 = (columns[:, 3:4] * up).astype(BF)
    place = iota((ROWS, TOK), 0)
    cot = dot(flag(place == tgt[0:1, :]).astype(BF), cot0)
    cot = cot + dot(flag(place == tgt[1:2, :]).astype(BF), cot1)
    outs[0][...] = cot.astype(BF)
    b0 = columns[:, 0:1].astype(jnp.int32)
    b1 = columns[:, 1:2].astype(jnp.int32)
    spot = iota((TOK, SP * CAP), 1)
    outs[1][...] = flag((spot == b0) | (spot == b1)).astype(BF)


def pick_cot(tp, target, weights, upstream):
    return call(
        pick_cot_body,
        (pltpu.HBM((ROWS, LATE), BF), pltpu.HBM((TOK, SP * CAP), BF)),
        tp,
        (target, weights, upstream),
        staged=(2,),
        cuts={
            2: (
                (TOK, LATE),
                lambda t: (slice(None), pl.ds(pl.multiple_of(t // 2 * 512 + EARLY, 128), LATE)),
            )
        },
        flops=10**9,
    )


def quarters(t):
    y = t // 2
    return y, (y + 3) % 4, (y + 1) % 4, (y + 2) % 4


def joined(refs):
    own, left, right, top, bottom = [now(r)[:, 0:512] for r in refs]
    return own, left, right, jnp.concatenate([top, bottom], axis=0)


def forward_body(t, ins, outs, scr):
    act_ref, a1_ref, a2_ref = outs
    pg, pu = scr
    q = quarters(t)
    x = joined(ins[0:5])
    for j in range(2):
        cols = slice(256 * j, 256 * j + 256)
        g = now(ins[5 + j])
        pg[:, cols] = sum(dot(x[i], g[q[i]]) for i in range(4))
        u = now(ins[7 + j])
        pu[:, cols] = sum(dot(x[i], u[q[i]]) for i in range(4))

    @pl.loop(0, ROWS // 32)
    def _(i):
        at = pl.ds(pl.multiple_of(i * 32, 32), 32)
        gate_pre, up_pre = pg[at, :], pu[at, :]
        capped = jnp.minimum(gate_pre, CLAMP)
        clipped = jnp.clip(up_pre, -CLAMP, CLAMP)
        sig = jax.nn.sigmoid(ALPHA * capped)
        gated = capped * sig
        act_ref[at, :] = (gated * (clipped + 1.0)).astype(BF)
        slope = sig + ALPHA * gated * (1.0 - sig)
        a1_ref[at, :] = jnp.where(gate_pre < CLAMP, (clipped + 1.0) * slope, 0.0)
        a2_ref[at, :] = jnp.where(jnp.abs(up_pre) < CLAMP, gated, 0.0)


def forward(tp, blocks, weights):
    return call(
        forward_body,
        (shape((ROWS, 512), BF), shape((ROWS, 512), F32), shape((ROWS, 512), F32)),
        tp,
        (*blocks, *weights),
        staged=(5, 3, 4, 7, 6, 8),
        cuts={
            3: ((256, 512), lambda t: (slice(None), pl.ds(0, 512))),
            4: ((256, 512), lambda t: (slice(None), pl.ds(0, 512))),
        },
        scratch=[pltpu.VMEM((ROWS, 512), F32)] * 2,
        flops=2 * 10**9,
    )


def partial_of(g, u, weights, piece):
    g0, g1, u0, u1 = weights
    return (
        dot(g[:, 0:256], g0[piece], 1, 1)
        + dot(g[:, 256:512], g1[piece], 1, 1)
        + dot(u[:, 0:256], u0[piece], 1, 1)
        + dot(u[:, 256:512], u1[piece], 1, 1)
    )


def down_columns(d, quarter):
    return d[:, pl.ds(pl.multiple_of(quarter * 512, 512), 512)]


def three_body(t, ins, outs, scr):
    q = quarters(t)
    early = [now(x) for x in ins[0:3]]
    upper, lower = slice(0, 256), slice(256, 512)

    def beside(block, rows, late):
        return jnp.concatenate([early[block][rows, :], late[...]], axis=1)

    own = beside(0, slice(None), ins[3])
    parts = [
        (q[1], upper, beside(1, upper, ins[4])),
        (q[1], lower, beside(1, lower, ins[5])),
        (q[2], upper, beside(2, upper, ins[6])),
        (q[2], lower, beside(2, lower, ins[7])),
    ]
    for j in range(2):
        d = now(ins[8 + j])
        cols = slice(256 * j, 256 * j + 256)
        outs[0][:, cols] = dot(own, down_columns(d, q[0]), 1, 1)
        for at, rows, part in parts:
            outs[0][rows, cols] += dot(part, down_columns(d, at), 1, 1)


def three(tp, first, late, downs):
    early = ((ROWS, EARLY), lambda t: (slice(None), pl.ds(512, EARLY)))
    return call(
        three_body,
        shape((ROWS, 512), F32),
        tp,
        (*first, *late, *downs),
        staged=(0, 1, 2, 8, 9),
        cuts={0: early, 1: early, 2: early},
        flops=10**9,
        limit=32,
    )


def backward_body(t, ins, outs, scr):
    top_ref, bottom_ref, gg_ref, gu_ref = outs
    ga, a1, a2 = ins[4:7]
    top = jnp.concatenate([now(ins[0])[...], ins[2][...]], axis=1)
    bottom = jnp.concatenate([now(ins[1])[...], ins[3][...]], axis=1)
    far = scr[0]
    for j in range(2):
        d = now(ins[7 + j])[...]
        cols = slice(256 * j, 256 * j + 256)
        far[0:256, cols] = dot(top, d, 1, 1)
        far[256:512, cols] = dot(bottom, d, 1, 1)

    @pl.loop(0, ROWS // 32)
    def _(i):
        at = pl.ds(pl.multiple_of(i * 32, 32), 32)
        grad = ga[at, :] + far[at, :]
        gg_ref[at, :] = (grad * a1[at, :]).astype(BF)
        gu_ref[at, :] = (grad * a2[at, :]).astype(BF)

    g, u = gg_ref[...], gu_ref[...]
    weights = [now(w) for w in ins[9:13]]
    for half in range(2):
        part = partial_of(g, u, weights, half).astype(BF)
        top_ref[half] = part[0:256]
        bottom_ref[half] = part[256:512]


def backward(tp, far, ga, downs, a1, a2, weights):
    pieces = ((2, 256, 256), lambda t: (pl.ds(2 * ((t // 2 + 2) % 4), 2),))
    columns = ((256, 512), columns_of(512, lambda t: (t // 2 + 2) % 4))
    early = ((256, EARLY), lambda t: (slice(None), pl.ds(512, EARLY)))
    return call(
        backward_body,
        (
            shape((2, 256, 256), BF),
            shape((2, 256, 256), BF),
            shape((ROWS, 512), BF),
            shape((ROWS, 512), BF),
        ),
        tp,
        (*far, ga, a1, a2, *downs, *weights),
        staged=(0, 1, 7, 8, 9, 10, 11, 12),
        cuts={0: early, 1: early, 7: columns, 8: columns} | {i: pieces for i in range(9, 13)},
        scratch=[pltpu.VMEM((ROWS, 512), F32)],
        flops=2 * 10**9,
        limit=32,
    )


def near_body(t, ins, outs, scr):
    g, u = ins[0][...], ins[1][...]
    weights = [now(w) for w in ins[2:6]]
    right, left = (t + 2) % 8, (t + 6) % 8
    swap = 1 - 2 * (t % 2)
    pieces = (right, right + swap, left, left + swap, t, t + swap)
    for ref, piece in zip(outs, pieces):
        ref[...] = partial_of(g, u, weights, piece).astype(BF)


def near(tp, gg, gu, weights):
    return call(
        near_body,
        (shape((ROWS, 256), BF),) * 6,
        tp,
        (gg, gu, *weights),
        staged=(2, 3, 4, 5),
        flops=3 * 10**9,
    )


def merge_body(t, ins, outs, scr):
    core = t % 2
    top, bottom = ins[0:2]
    for src, dst, got, first in (
        (ins[2], outs[0], top[core], True),
        (ins[3], outs[1], top[1 - core], True),
        (ins[4], outs[2], bottom[core], False),
        (ins[5], outs[3], bottom[1 - core], False),
    ):
        hit, other = (slice(0, 256), slice(256, 512)) if first else (slice(256, 512), slice(0, 256))
        dst[hit, :] = (src[hit, :].astype(F32) + got.astype(F32)).astype(BF)
        dst[other, :] = src[other, :]


def merge(tp, top, bottom, parts):
    return call(
        merge_body, (shape((ROWS, 256), BF),) * 4, tp, (top, bottom, *parts), flops=10**7, limit=16
    )


def settle_body(t, ins, outs, scr):
    a0, a1, a2, b0, b1, b2 = [x[...].astype(F32) for x in ins]
    outs[0][:, 0:HALF, :] = (a0 + a1 + a2).astype(BF).reshape(SP, HALF, 256)
    outs[0][:, HALF:CAP, :] = (b0 + b1 + b2).astype(BF).reshape(SP, HALF, 256)


def settle(tp, parts):
    return call(settle_body, pltpu.HBM((SP, CAP, 256), BF), tp, parts, flops=10**7, limit=16)


def by_column():
    whole, upper, lower = slice(0, 512), slice(0, 256), slice(256, 512)
    every = slice(None)

    def place(by, rows, cols):
        return lambda t: ((t // 2 + by) % 4, rows, cols)

    into = {}
    for n, (by, rows) in enumerate(((0, whole), (3, whole), (1, whole), (2, upper), (2, lower))):
        into[n] = [
            ((every, pl.ds(0, 512)), 0, place(by, rows, every)),
            ((every, pl.ds(512, EARLY)), 1, place(by, rows, slice(0, EARLY))),
        ]
    places = ((0, whole), (3, upper), (3, lower), (1, upper), (1, lower), (2, upper), (2, lower))
    for n, (by, rows) in enumerate(places):
        into[5 + n] = [((every, every), 1, place(by, rows, slice(EARLY, 512)))]
    return into


def weights_call(body, outs, tp, args):
    return call(
        body,
        outs,
        tp,
        args,
        staged=tuple(range(len(args))),
        into=by_column(),
        scratch=[pltpu.VMEM((4, ROWS, 512), BF)] * 2,
        flops=2 * 10**9,
    )


def each_quarter(ins, scr, cols, store):
    ins = [now(x) for x in ins]
    gg, gu, act = ins[12:15]
    gu_cols = jnp.concatenate([gg[:, cols], gu[:, cols]], axis=1)
    act_cols = act[:, cols]

    @pl.loop(0, 4)
    def _(q):
        store(q, dot(scr[0][q], gu_cols, 0, 0), dot(act_cols, scr[1][q], 0, 0))


def lend_body(t, ins, outs, scr):
    def store(q, both, down):
        outs[0][q] = both[:, 0:256].astype(BF)
        outs[0][4 + q] = both[:, 256:512].astype(BF)
        outs[0][8 + q, 0:256, :] = down[:, 0:256].astype(BF)
        outs[0][8 + q, 256:512, :] = down[:, 256:512].astype(BF)

    each_quarter(ins, scr, slice(256, 512), store)


def lend(tp, xs, cs, gg, gu, act):
    return weights_call(
        lend_body, shape((12, 512, 256), BF), tp, (*xs, *cs, gg, gu, act)
    )


def keep_body(t, ins, outs, scr):
    gate_ref, up_ref, down_ref = outs

    def store(q, both, down):
        lent = now(ins[15])
        gate_ref[q] = both[:, 0:256] + lent[q].astype(F32)
        up_ref[q] = both[:, 256:512] + lent[4 + q].astype(F32)
        for half in range(2):
            cols = slice(256 * half, 256 * half + 256)
            at = pl.ds(pl.multiple_of(q * 512 + 256 * half, 256), 256)
            down_ref[:, at] = down[:, cols] + lent[8 + q, cols, :].astype(F32)

    each_quarter(ins, scr, slice(0, 256), store)


def keep(tp, xs, cs, gg, gu, act, lent):
    return weights_call(
        keep_body,
        (shape((4, 512, 256), F32), shape((4, 512, 256), F32), shape((256, 2048), F32)),
        tp,
        (*xs, *cs, gg, gu, act, lent),
    )


def hand_out_body(t, ins, outs, scr):
    proj = now(ins[0])
    for d in range(4):
        other = lax.bitwise_xor(t, 2 * d + 1)
        outs[0][d] = proj[:, pl.ds(pl.multiple_of(other * 256, 256), 256)]
    outs[0][4] = ins[1][...]


def hand_out(tp, proj, saved):
    return call(
        hand_out_body, shape((5, 64, TOK), BF), tp, (proj, saved), staged=(0,), limit=16
    )


def hand_on_body(t, ins, outs, scr):
    proj = now(ins[0])
    for d in range(1, 4):
        other = lax.bitwise_xor(t, 2 * d)
        outs[d - 1][0] = proj[:, pl.ds(pl.multiple_of(other * 256, 256), 256)]
        outs[d - 1][1] = ins[2][d]
        outs[d - 1][2] = ins[1][...]
        outs[d - 1][3] = ins[2][4]


def hand_on(tp, proj, saved, got):
    return call(
        hand_on_body,
        (shape((4, 64, TOK), BF),) * 3,
        tp,
        (proj, saved, got),
        staged=(0,),
        limit=16,
    )


def prepare_body(t, ins, outs, scr):
    proj_ref, mixed_ref, slope_ref, slope_n_ref, stat_ref = outs
    all_saved = scr[0]

    def at(d):
        return pl.ds(pl.multiple_of(lax.bitwise_xor(t, d) * 64, 64), 64)

    proj_ref[at(0), :] = now(ins[0])[...]
    all_saved[at(0), :] = ins[1][...]
    proj_ref[at(1), :] = ins[2][0]
    all_saved[at(1), :] = ins[2][4]
    for d in range(1, 4):
        for other in range(2):
            proj_ref[at(2 * d + other), :] = ins[2 + d][other]
            all_saved[at(2 * d + other), :] = ins[2 + d][2 + other]
    saved = all_saved[...].astype(F32)
    mean = jnp.sum(saved, axis=0, keepdims=True) / CW
    var = jnp.sum(saved * saved, axis=0, keepdims=True) / CW - mean * mean
    inv = lax.rsqrt(var + EPS)
    normed = (saved - mean) * inv
    sig = jax.nn.sigmoid(normed)
    mixed_ref[...] = (normed * sig).astype(BF)
    slope = sig * (1.0 + normed * (1.0 - sig))
    slope_ref[...] = slope
    slope_n_ref[...] = slope * normed
    stat_ref[...] = jnp.concatenate([mean, inv, mean, inv, mean, inv, mean, inv], axis=0)


def prepare(tp, proj, saved, got):
    return call(
        prepare_body,
        (
            pltpu.HBM((CW, TOK), BF),
            pltpu.HBM((CW, TOK), BF),
            pltpu.HBM((CW, TOK), F32),
            pltpu.HBM((CW, TOK), F32),
            shape((8, TOK), F32),
        ),
        tp,
        (proj, saved, *got),
        staged=(0,),
        cuts={0: ((64, TOK), columns_of(256, lambda t: t))},
        scratch=[pltpu.VMEM((CW, TOK), BF)],
        flops=10**8,
    )


def tokens_body(t, ins, outs, scr):
    gs_ref, outer_ref, own_ref, lent_ref = outs
    routed = dot(now(ins[0])[...], now(ins[2])[...])
    gs = (now(ins[1])[...].astype(F32) + routed).astype(BF)
    gs_ref[...] = gs
    outer = dot(gs, now(ins[4])[...], 0, 1)
    lane = iota((64, 128), 1) < 64
    for u in range(4):
        for i in range(4):
            block = outer[64 * i : 64 * i + 64, 128 * u : 128 * u + 128]
            turned = pltpu.roll(block, 64, 1)
            even = jnp.where(lane[0:32], block[0:32], turned[32:64])
            odd = jnp.where(lane[0:32], turned[0:32], block[32:64])
            outer_ref[8 * u + i] = even.astype(BF)
            outer_ref[8 * u + 4 + i] = odd.astype(BF)
    part_all = scr[0]
    part = dot(now(ins[3])[...], gs, 1, 1)
    part_all[...] = part
    first = jnp.sum(part * now(ins[5])[...], axis=0, keepdims=True)
    second = jnp.sum(part * now(ins[6])[...], axis=0, keepdims=True)
    sums = jnp.concatenate([first, second], axis=0)
    parted = split_sums(sums)

    def at(d):
        return pl.ds(pl.multiple_of(lax.bitwise_xor(t, d) * 64, 64), 64)

    for d in range(4):
        own_ref[d, 0:64, :] = part_all[at(2 * d), :]
        lent_ref[d, 0:64, :] = part_all[at(2 * d + 1), :].astype(BF)
        lent_ref[d, 64:72, :] = parted
    own_ref[0, 64:72, :] = jnp.concatenate([sums] * 4, axis=0)


def split_sums(sums):
    high = sums.astype(BF).astype(F32)
    low = sums - high
    return jnp.concatenate([high, low, high, low], axis=0).astype(BF)


def fold_body(t, ins, outs, scr):
    own, got = ins
    sums = own[0, 64:66, :] + got[0, 64:66, :].astype(F32) + got[0, 66:68, :].astype(F32)
    outs[0][0:64, :] = own[0, 0:64, :] + got[0, 0:64, :].astype(F32)
    outs[0][64:72, :] = jnp.concatenate([sums] * 4, axis=0)
    parted = split_sums(sums)
    for d in range(1, 4):
        outs[d][0:64, :] = (own[d, 0:64, :] + got[d, 0:64, :].astype(F32)).astype(BF)
        outs[d][64:72, :] = parted


def fold(tp, own, got):
    return call(
        fold_body,
        (shape((72, TOK), F32),) + (shape((72, TOK), BF),) * 3,
        tp,
        (own, got),
        flops=10**7,
        limit=16,
    )


def tokens(tp, back, upstream, ret, proj, mixed, slope, slope_n):
    return call(
        tokens_body,
        (
            shape((TOK, 256), BF),
            pltpu.HBM((SP, 32, 128), BF),
            shape((4, 72, TOK), F32),
            shape((4, 72, TOK), BF),
        ),
        tp,
        (back, upstream, ret, proj, mixed, slope, slope_n),
        staged=(0, 2, 1, 4, 3, 5, 6),
        cuts={1: ((TOK, 256), columns_of(256, lambda t: t))},
        scratch=[pltpu.VMEM((CW, TOK), F32)],
        flops=10**9,
    )


def norm_body(t, ins, outs, scr):
    own, saved, stat = ins[0], ins[4], ins[5]
    mixed, sums = own[0:64, :], own[64:66, :]
    for got in ins[1:4]:
        mixed = mixed + got[0:64, :].astype(F32)
        sums = sums + got[64:66, :].astype(F32) + got[66:68, :].astype(F32)
    first, second = sums[0:1] / CW, sums[1:2] / CW
    mean, inv = stat[0:1, :], stat[1:2, :]
    normed = (saved[...].astype(F32) - mean) * inv
    sig = jax.nn.sigmoid(normed)
    grad = mixed * sig * (1.0 + normed * (1.0 - sig))
    conv_grad = inv * (grad - first - normed * second)
    outs[0][...] = conv_grad
    outs[1][...] = conv_grad[:, 0:128]


def norm(tp, own, got, saved, stat):
    return call(
        norm_body,
        (shape((64, TOK), F32), shape((64, 128), F32)),
        tp,
        (own, *got, saved, stat),
        flops=10**7,
        limit=16,
    )


def tap_sum(padded, taps):
    total = jnp.zeros((64, TOK), F32)
    width = padded.shape[1]
    for j in range(taps.shape[1]):
        turned = padded if j == 0 else pltpu.roll(padded, width - j, 1)
        total = total + taps[:, j : j + 1] * turned[:, 0:TOK]
    return total


def conv_own_body(t, ins, outs, scr):
    grad, taps = ins
    outs[0][...] = tap_sum(jnp.concatenate([grad[...], jnp.zeros((64, 128), F32)], axis=1), taps)


def conv_own(tp, grad, taps):
    return call(conv_own_body, shape((64, TOK), F32), tp, (grad, taps), flops=10**8, limit=16)


def conv_rim_body(t, ins, outs, scr):
    own, rim, taps, value, gate = ins
    dv_ref, dg_ref = outs
    both = jnp.concatenate([jnp.zeros((64, 128), F32), rim[...]], axis=1)
    reach = jnp.zeros((64, 128), F32)
    for j in range(1, taps.shape[1]):
        reach = reach + taps[:, j : j + 1] * pltpu.roll(both, TOK - j, 1)[:, 0:128]
    total = jnp.concatenate([own[:, 0:128], own[:, 128:256] + reach], axis=1)
    sig = jax.nn.sigmoid(gate[...].astype(F32))
    dv_ref[...] = (total * sig).astype(BF)
    dg_ref[...] = (total * value[...].astype(F32) * sig * (1.0 - sig)).astype(BF)


def conv_rim(tp, own, rim, taps, value, gate):
    return call(
        conv_rim_body,
        (shape((64, TOK), BF), shape((64, TOK), BF)),
        tp,
        (own, rim, taps, value, gate),
        flops=10**8,
        limit=16,
    )


def total_body(t, ins, outs, scr):
    whole = jnp.sum(ins[0][...].astype(F32), axis=0)
    outs[0][0:32, :] = whole[:, 0:64]
    outs[0][32:64, :] = whole[:, 64:128]


def total(tp, got):
    return call(total_body, shape((64, 64), F32), tp, (got,), flops=10**7, limit=16)


def moved(x, by):
    return lax.ppermute(x, "tp", [(i, (i + by) % TP) for i in range(TP)])


def swapped(x, by):
    return lax.ppermute(x, "tp", [(i, i ^ by) for i in range(TP)])


def across_moved(x, by):
    return lax.ppermute(x, "tp", [(i, ((i + by) % TP) ^ 1) for i in range(TP)])


def around(block):
    left, right = moved(block, 2), moved(block, -2)
    top, bottom = moved(left[:256], 2), moved(right[256:], -2)
    return block, left, right, top, bottom


def around_in_halves(block):
    upper, lower = block[:256], block[256:]
    left_upper, right_lower = moved(upper, 2), moved(lower, -2)
    left_lower, right_upper = moved(lower, 2), moved(upper, -2)
    top, bottom = moved(left_upper, 2), moved(right_lower, -2)
    return block, left_upper, left_lower, right_upper, right_lower, top, bottom


def exchange(x):
    return lax.all_to_all(x, "sp", 0, 0, tiled=True)


def after(x, *others):
    return lax.optimization_barrier((x, *others))[0]


def step(
    upstream, stream, routes, route_weights, glu_value, glu_gate, conv_taps, conv_saved,
    out_proj, expert_gate, expert_up, expert_down,
):
    tp = lax.axis_index("tp").reshape(1)
    weights = route_weights.T
    rows_out, target = pick_rows(tp, routes.T, stream, weights, upstream)
    rows_in = exchange(rows_out.reshape(SP, HALF, FIRST)).reshape(ROWS, FIRST)

    saved, proj = conv_saved.T, out_proj.T
    near_early = swapped(hand_out(tp, proj, saved), 1)
    far_early = hand_on(tp, proj, saved, near_early)
    early = (near_early, *(swapped(x, 2 * d + 2) for d, x in enumerate(far_early)))
    gate_own, up_own, down_own = expert_gate[0], expert_up[0], expert_down[0]
    gate_par, up_par, down_par = (swapped(w, 1) for w in (gate_own, up_own, down_own))

    cot_out, back = pick_cot(tp, target, weights, upstream)
    cot_out = after(cot_out, *early)
    cot_in = exchange(cot_out.reshape(SP, HALF, LATE))
    cot_in = cot_in.reshape(ROWS, LATE)
    proj_all, mixed, slope, slope_n, stat = prepare(tp, proj, saved, early)

    xs = around(rows_in)
    by_quarter = [w.reshape(4, 512, 256) for w in (gate_own, gate_par, up_own, up_par)]
    by_piece = [w.reshape(8, 256, 256) for w in (gate_own, gate_par, up_own, up_par)]
    act, a1, a2 = forward(tp, xs, by_quarter)

    cs = around_in_halves(cot_in)
    downs = (down_own, down_par)
    ga = three(tp, xs[:3], cs[:5], downs)
    far_top, far_bottom, gg, gu = backward(tp, (*xs[3:], *cs[5:]), ga, downs, a1, a2, by_piece)
    got_top, got_bottom = moved(far_top, 2), moved(far_bottom, -2)
    parts = near(tp, gg, gu, by_piece)
    rs, rc, ls, lc = merge(tp, got_top, got_bottom, parts[:4])
    lent = lend(tp, xs, cs, gg, gu, after(act, rs))
    came = (moved(rs, 2), moved(ls, -2), across_moved(rc, 2), across_moved(lc, -2))
    own_cross = swapped(parts[5], 1)
    summed = settle(
        tp, (after(parts[4], lent), came[0], came[1], own_cross, came[2], came[3])
    )
    returned = exchange(summed).reshape(SP * CAP, 256)
    grads = keep(tp, xs, cs, gg, gu, act, swapped(lent, 1))
    grad_gate_w, grad_up_w, grad_down_w = grads
    back = after(back, grad_down_w)

    made = tokens(tp, back, upstream, returned, proj_all, mixed, slope, slope_n)
    grad_stream, outer, own_part, lent_part = made
    outer_in = exchange(outer)
    lent_in = swapped(lent_part, 1)
    folded = fold(tp, own_part, lent_in)
    own_part = folded[0]
    part_in = tuple(swapped(x, 2 * d + 2) for d, x in enumerate(folded[1:]))
    grad_conv, rim = norm(tp, own_part, part_in, saved, stat)
    rim_in = lax.ppermute(rim, "sp", [(i, i - 1) for i in range(1, SP)])
    taps = conv_taps.T
    grad_glu = conv_own(tp, grad_conv, taps)
    grad_value, grad_gate = conv_rim(tp, grad_glu, rim_in, taps, glu_value.T, glu_gate.T)
    grad_out_proj = lax.ppermute(
        total(tp, outer_in),
        ("sp", "tp"),
        [
            ((4 * u + i) * TP + t, (4 * t + i) * TP + u)
            for i in range(4)
            for u in range(TP)
            for t in range(TP)
        ],
    )
    return (
        grad_stream,
        grad_value.T,
        grad_gate.T,
        grad_out_proj,
        grad_gate_w.reshape(1, 2048, 256),
        grad_up_w.reshape(1, 2048, 256),
        grad_down_w[None],
    )


def solution(mesh):
    in_specs = (
        P("sp", None),
        P("sp", None),
        P("sp", None),
        P("sp", None),
        P("sp", "tp"),
        P("sp", "tp"),
        P(None, "tp"),
        P("sp", "tp"),
        P(None, "tp"),
        P("sp", None, "tp"),
        P("sp", None, "tp"),
        P("sp", "tp", None),
    )
    out_specs = (
        P("sp", "tp"),
        P("sp", "tp"),
        P("sp", "tp"),
        P("sp", "tp"),
        P("sp", None, "tp"),
        P("sp", None, "tp"),
        P("sp", "tp", None),
    )
    return jax.shard_map(step, mesh=mesh, in_specs=in_specs, out_specs=out_specs, check_vma=False)
```

```python
import jax
import jax.numpy as jnp
from jax import lax
from jax.experimental import pallas as pl
from jax.experimental.pallas import tpu as pltpu
from jax.sharding import PartitionSpec as P

CLAMP = 7.0
ALPHA = 1.702
EPS = 1e-05
CW = 512
CAP = 32
HALF = 16
SP = 32
TP = 8
TOK = 256
ROWS = SP * HALF
EARLY = 128
LATE = 512 - EARLY
FIRST = 512 + EARLY
BF = jnp.bfloat16
F32 = jnp.float32
MIB = 1 << 20


def dot(a, b, ca=1, cb=0):
    return lax.dot_general(a, b, (((ca,), (cb,)), ((), ())), preferred_element_type=F32)


def flag(mask):
    return jnp.where(mask, 1.0, 0.0)


def iota(shape, dim):
    return lax.broadcasted_iota(jnp.int32, shape, dim)


class Later:
    def __init__(self, copies, buffer):
        self.copies, self.buffer = copies, buffer
        for copy in copies:
            copy.start()

    def now(self):
        for copy in self.copies:
            copy.wait()
        self.copies = []
        return self.buffer


def now(x):
    return x.now() if isinstance(x, Later) else x


def call(body, outs, tp, args, staged=(), cuts=None, into=None, scratch=(), flops=0, limit=40):
    cuts, into = cuts or {}, into or {}
    own = tuple(i for i in staged if i not in into)
    n_copies = sum(len(into[i]) if i in into else 1 for i in staged)
    single = not isinstance(outs, tuple)
    outs = (outs,) if single else outs
    n_in, n_out, n_scr = len(args), len(outs), len(scratch)

    def kernel(t_ref, *refs):
        ins, rest = list(refs[:n_in]), refs[n_in:]
        made, scr, buffers = rest[:n_out], rest[n_out : n_out + n_scr], rest[n_out + n_scr :]
        t, sems = t_ref[0], iter(range(n_copies))
        for i in staged:
            if i in into:
                pairs = [(ins[i].at[cut], scr[k].at[to(t)]) for cut, k, to in into[i]]
            else:
                source = ins[i].at[cuts[i][1](t)] if i in cuts else ins[i]
                pairs = [(source, buffers[own.index(i)])]
            copies = [
                pltpu.make_async_copy(source, target, buffers[-1].at[next(sems)])
                for source, target in pairs
            ]
            ins[i] = Later(copies, pairs[0][1])
        body(t_ref[0], ins, made, scr)
        for i in staged:
            now(ins[i])

    extra = [
        pltpu.VMEM(cuts[i][0] if i in cuts else args[i].shape, args[i].dtype) for i in own
    ]
    if staged:
        extra.append(pltpu.SemaphoreType.DMA((n_copies,)))
    args = tuple(
        pltpu.with_memory_space_constraint(x, pltpu.HBM) if i in staged else x
        for i, x in enumerate(args)
    )
    made = pl.pallas_call(
        kernel,
        out_shape=outs,
        in_specs=[SMEM] + [HBM if i in staged else VMEM for i in range(n_in)],
        out_specs=(VMEM,) * n_out,
        scratch_shapes=list(scratch) + extra,
        compiler_params=pltpu.CompilerParams(vmem_limit_bytes=limit * MIB),
        cost_estimate=pl.CostEstimate(flops=flops, bytes_accessed=MIB, transcendentals=0),
    )(tp, *args)
    return made[0] if single else made


def shape(dims, dtype):
    return jax.ShapeDtypeStruct(dims, dtype)


SMEM = pl.BlockSpec(memory_space=pltpu.SMEM)
VMEM = pl.BlockSpec(memory_space=pltpu.VMEM)
HBM = pl.BlockSpec(memory_space=pltpu.HBM)


def columns_of(width, which):
    return lambda t: (slice(None), pl.ds(pl.multiple_of(which(t) * width, width), width))


def pick_rows_body(t, ins, outs, scr):
    core = t % 2
    r = ins[0][...]
    r0, r1 = r[0:1, :], r[1:2, :]
    expert = iota((SP, TOK), 0)
    named0, named1 = expert == r0, expert == r1
    both = (flag(named0) + flag(named1)).astype(BF)
    before = flag(iota((TOK, TOK), 0) < iota((TOK, TOK), 1)).astype(BF)
    earlier = dot(both, before)
    slot0 = jnp.sum(jnp.where(named0, earlier, 0.0), axis=0, keepdims=True).astype(jnp.int32)
    slot1 = jnp.sum(jnp.where(named1, earlier, 0.0), axis=0, keepdims=True).astype(jnp.int32)
    l0 = jnp.where(slot0 // HALF == core, r0 * HALF + slot0 - HALF * core, -1)
    l1 = jnp.where(slot1 // HALF == core, r1 * HALF + slot1 - HALF * core, -1)
    b0 = r0 * CAP + (slot0 + HALF * core) % CAP
    b1 = r1 * CAP + (slot1 + HALF * core) % CAP
    outs[1][...] = jnp.concatenate([l0, l1, b0, b1, l0, l1, b0, b1], axis=0)
    place = iota((ROWS, TOK), 0)
    at0, at1 = place == l0, place == l1
    pick = flag(at0 | at1).astype(BF)
    w = ins[2][...]
    scale = jnp.where(at0, w[0:1, :], 0.0) + jnp.where(at1, w[1:2, :], 0.0)
    scale = jnp.sum(scale, axis=1, keepdims=True)
    outs[0][:, 0:512] = dot(pick, now(ins[1])[...]).astype(BF)
    outs[0][:, 512:FIRST] = (scale * dot(pick, now(ins[3])[...])).astype(BF)


def pick_rows(tp, routes, stream, weights, upstream):
    return call(
        pick_rows_body,
        (pltpu.HBM((ROWS, FIRST), BF), shape((8, TOK), jnp.int32)),
        tp,
        (routes, stream, weights, upstream),
        staged=(1, 3),
        cuts={
            1: ((TOK, 512), columns_of(512, lambda t: t // 2)),
            3: ((TOK, EARLY), columns_of(EARLY, lambda t: t // 2 * (512 // EARLY))),
        },
        flops=10**9,
    )


def pick_cot_body(t, ins, outs, scr):
    tgt, w = ins[0][...], ins[1][...]
    table = jnp.concatenate([tgt[2:4, :].astype(F32), w, tgt[2:4, :].astype(F32), w], axis=0)
    columns = jnp.transpose(jnp.concatenate([table] * 16, axis=0))
    up = now(ins[2])[...].astype(F32)
    cot0 = (columns[:, 2:3] * up).astype(BF)
    cot1 = (columns[:, 3:4] * up).astype(BF)
    place = iota((ROWS, TOK), 0)
    cot = dot(flag(place == tgt[0:1, :]).astype(BF), cot0)
    cot = cot + dot(flag(place == tgt[1:2, :]).astype(BF), cot1)
    outs[0][...] = cot.astype(BF)
    b0 = columns[:, 0:1].astype(jnp.int32)
    b1 = columns[:, 1:2].astype(jnp.int32)
    spot = iota((TOK, SP * CAP), 1)
    outs[1][...] = flag((spot == b0) | (spot == b1)).astype(BF)


def pick_cot(tp, target, weights, upstream):
    return call(
        pick_cot_body,
        (pltpu.HBM((ROWS, LATE), BF), pltpu.HBM((TOK, SP * CAP), BF)),
        tp,
        (target, weights, upstream),
        staged=(2,),
        cuts={
            2: (
                (TOK, LATE),
                lambda t: (slice(None), pl.ds(pl.multiple_of(t // 2 * 512 + EARLY, 128), LATE)),
            )
        },
        flops=10**9,
    )


def quarters(t):
    y = t // 2
    return y, (y + 3) % 4, (y + 1) % 4, (y + 2) % 4


def first_body(t, ins, outs, scr):
    q = quarters(t)
    x = [ref[:, 0:512] for ref in ins[0:3]]
    for j in range(2):
        cols = slice(256 * j, 256 * j + 256)
        for out, at in ((outs[0], 3), (outs[1], 5)):
            w = now(ins[at + j])
            out[:, cols] = sum(dot(x[i], w[q[i]]) for i in range(3))


def first(tp, near_blocks, weights):
    return call(
        first_body,
        (shape((ROWS, 512), F32),) * 2,
        tp,
        (*near_blocks, *weights),
        staged=(3, 5, 4, 6),
        flops=10**9,
        limit=32,
    )


def forward_body(t, ins, outs, scr):
    act_ref, a1_ref, a2_ref = outs
    pg, pu = scr
    top, bottom = now(ins[2])[...], now(ins[3])[...]
    for j in range(2):
        cols = slice(256 * j, 256 * j + 256)
        for near_sum, into, at in ((ins[0], pg, 4), (ins[1], pu, 6)):
            w = now(ins[at + j])[0]
            into[0:256, cols] = near_sum[0:256, cols] + dot(top, w)
            into[256:512, cols] = near_sum[256:512, cols] + dot(bottom, w)

    @pl.loop(0, ROWS // 32)
    def _(i):
        at = pl.ds(pl.multiple_of(i * 32, 32), 32)
        gate_pre, up_pre = pg[at, :], pu[at, :]
        capped = jnp.minimum(gate_pre, CLAMP)
        clipped = jnp.clip(up_pre, -CLAMP, CLAMP)
        sig = jax.nn.sigmoid(ALPHA * capped)
        gated = capped * sig
        act_ref[at, :] = (gated * (clipped + 1.0)).astype(BF)
        slope = sig + ALPHA * gated * (1.0 - sig)
        a1_ref[at, :] = jnp.where(gate_pre < CLAMP, (clipped + 1.0) * slope, 0.0)
        a2_ref[at, :] = jnp.where(jnp.abs(up_pre) < CLAMP, gated, 0.0)


def forward(tp, sums, far_blocks, weights):
    rows = ((256, 512), lambda t: (slice(None), pl.ds(0, 512)))
    quarter = ((1, 512, 256), lambda t: (pl.ds((t // 2 + 2) % 4, 1),))
    return call(
        forward_body,
        (shape((ROWS, 512), BF), shape((ROWS, 512), F32), shape((ROWS, 512), F32)),
        tp,
        (*sums, *far_blocks, *weights),
        staged=(2, 3, 4, 6, 5, 7),
        cuts={2: rows, 3: rows} | {i: quarter for i in range(4, 8)},
        scratch=[pltpu.VMEM((ROWS, 512), F32)] * 2,
        flops=2 * 10**9,
        limit=32,
    )


def partial_of(g, u, weights, piece):
    g0, g1, u0, u1 = weights
    return (
        dot(g[:, 0:256], g0[piece], 1, 1)
        + dot(g[:, 256:512], g1[piece], 1, 1)
        + dot(u[:, 0:256], u0[piece], 1, 1)
        + dot(u[:, 256:512], u1[piece], 1, 1)
    )


def down_columns(d, quarter):
    return d[:, pl.ds(pl.multiple_of(quarter * 512, 512), 512)]


def three_body(t, ins, outs, scr):
    q = quarters(t)
    early = [now(x) for x in ins[0:3]]
    upper, lower = slice(0, 256), slice(256, 512)

    def beside(block, rows, late):
        return jnp.concatenate([early[block][rows, :], late[...]], axis=1)

    own = beside(0, slice(None), ins[3])
    parts = [
        (q[1], upper, beside(1, upper, ins[4])),
        (q[1], lower, beside(1, lower, ins[5])),
        (q[2], upper, beside(2, upper, ins[6])),
        (q[2], lower, beside(2, lower, ins[7])),
    ]
    for j in range(2):
        d = now(ins[8 + j])
        cols = slice(256 * j, 256 * j + 256)
        outs[0][:, cols] = dot(own, down_columns(d, q[0]), 1, 1)
        for at, rows, part in parts:
            outs[0][rows, cols] += dot(part, down_columns(d, at), 1, 1)


def three(tp, first, late, downs):
    early = ((ROWS, EARLY), lambda t: (slice(None), pl.ds(512, EARLY)))
    return call(
        three_body,
        shape((ROWS, 512), F32),
        tp,
        (*first, *late, *downs),
        staged=(0, 1, 2, 8, 9),
        cuts={0: early, 1: early, 2: early},
        flops=10**9,
        limit=32,
    )


def backward_body(t, ins, outs, scr):
    top_ref, bottom_ref, gg_ref, gu_ref = outs
    ga, a1, a2 = ins[4:7]
    top = jnp.concatenate([now(ins[0])[...], ins[2][...]], axis=1)
    bottom = jnp.concatenate([now(ins[1])[...], ins[3][...]], axis=1)
    far = scr[0]
    for j in range(2):
        d = now(ins[7 + j])[...]
        cols = slice(256 * j, 256 * j + 256)
        far[0:256, cols] = dot(top, d, 1, 1)
        far[256:512, cols] = dot(bottom, d, 1, 1)

    @pl.loop(0, ROWS // 32)
    def _(i):
        at = pl.ds(pl.multiple_of(i * 32, 32), 32)
        grad = ga[at, :] + far[at, :]
        gg_ref[at, :] = (grad * a1[at, :]).astype(BF)
        gu_ref[at, :] = (grad * a2[at, :]).astype(BF)

    g, u = gg_ref[...], gu_ref[...]
    weights = [now(w) for w in ins[9:13]]
    for half in range(2):
        part = partial_of(g, u, weights, half).astype(BF)
        top_ref[half] = part[0:256]
        bottom_ref[half] = part[256:512]


def backward(tp, far, ga, downs, a1, a2, weights):
    pieces = ((2, 256, 256), lambda t: (pl.ds(2 * ((t // 2 + 2) % 4), 2),))
    columns = ((256, 512), columns_of(512, lambda t: (t // 2 + 2) % 4))
    early = ((256, EARLY), lambda t: (slice(None), pl.ds(512, EARLY)))
    return call(
        backward_body,
        (
            shape((2, 256, 256), BF),
            shape((2, 256, 256), BF),
            shape((ROWS, 512), BF),
            shape((ROWS, 512), BF),
        ),
        tp,
        (*far, ga, a1, a2, *downs, *weights),
        staged=(0, 1, 7, 8, 9, 10, 11, 12),
        cuts={0: early, 1: early, 7: columns, 8: columns} | {i: pieces for i in range(9, 13)},
        scratch=[pltpu.VMEM((ROWS, 512), F32)],
        flops=2 * 10**9,
        limit=32,
    )


def near_body(t, ins, outs, scr):
    g, u = ins[0][...], ins[1][...]
    weights = [now(w) for w in ins[2:6]]
    right, left = (t + 2) % 8, (t + 6) % 8
    swap = 1 - 2 * (t % 2)
    pieces = (right, right + swap, left, left + swap, t, t + swap)
    for ref, piece in zip(outs, pieces):
        ref[...] = partial_of(g, u, weights, piece).astype(BF)


def near(tp, gg, gu, weights):
    return call(
        near_body,
        (shape((ROWS, 256), BF),) * 6,
        tp,
        (gg, gu, *weights),
        staged=(2, 3, 4, 5),
        flops=3 * 10**9,
    )


def merge_body(t, ins, outs, scr):
    core = t % 2
    top, bottom = ins[0:2]
    for src, dst, got, first in (
        (ins[2], outs[0], top[core], True),
        (ins[3], outs[1], top[1 - core], True),
        (ins[4], outs[2], bottom[core], False),
        (ins[5], outs[3], bottom[1 - core], False),
    ):
        hit, other = (slice(0, 256), slice(256, 512)) if first else (slice(256, 512), slice(0, 256))
        dst[hit, :] = (src[hit, :].astype(F32) + got.astype(F32)).astype(BF)
        dst[other, :] = src[other, :]


def merge(tp, top, bottom, parts):
    return call(
        merge_body, (shape((ROWS, 256), BF),) * 4, tp, (top, bottom, *parts), flops=10**7, limit=16
    )


def settle_body(t, ins, outs, scr):
    a0, a1, a2, b0, b1, b2 = [x[...].astype(F32) for x in ins]
    outs[0][:, 0:HALF, :] = (a0 + a1 + a2).astype(BF).reshape(SP, HALF, 256)
    outs[0][:, HALF:CAP, :] = (b0 + b1 + b2).astype(BF).reshape(SP, HALF, 256)


def settle(tp, parts):
    return call(settle_body, pltpu.HBM((SP, CAP, 256), BF), tp, parts, flops=10**7, limit=16)


def by_column():
    whole, upper, lower = slice(0, 512), slice(0, 256), slice(256, 512)
    every = slice(None)

    def place(by, rows, cols):
        return lambda t: ((t // 2 + by) % 4, rows, cols)

    into = {}
    for n, (by, rows) in enumerate(((0, whole), (3, whole), (1, whole), (2, upper), (2, lower))):
        into[n] = [
            ((every, pl.ds(0, 512)), 0, place(by, rows, every)),
            ((every, pl.ds(512, EARLY)), 1, place(by, rows, slice(0, EARLY))),
        ]
    places = ((0, whole), (3, upper), (3, lower), (1, upper), (1, lower), (2, upper), (2, lower))
    for n, (by, rows) in enumerate(places):
        into[5 + n] = [((every, every), 1, place(by, rows, slice(EARLY, 512)))]
    return into


def weights_call(body, outs, tp, args):
    return call(
        body,
        outs,
        tp,
        args,
        staged=tuple(range(len(args))),
        into=by_column(),
        scratch=[pltpu.VMEM((4, ROWS, 512), BF)] * 2,
        flops=2 * 10**9,
    )


def each_quarter(ins, scr, cols, store):
    ins = [now(x) for x in ins]
    gg, gu, act = ins[12:15]
    gu_cols = jnp.concatenate([gg[:, cols], gu[:, cols]], axis=1)
    act_cols = act[:, cols]

    @pl.loop(0, 4)
    def _(q):
        store(q, dot(scr[0][q], gu_cols, 0, 0), dot(act_cols, scr[1][q], 0, 0))


def lend_body(t, ins, outs, scr):
    def store(q, both, down):
        outs[0][q] = both[:, 0:256].astype(BF)
        outs[0][4 + q] = both[:, 256:512].astype(BF)
        outs[0][8 + q, 0:256, :] = down[:, 0:256].astype(BF)
        outs[0][8 + q, 256:512, :] = down[:, 256:512].astype(BF)

    each_quarter(ins, scr, slice(256, 512), store)


def lend(tp, xs, cs, gg, gu, act):
    return weights_call(
        lend_body, shape((12, 512, 256), BF), tp, (*xs, *cs, gg, gu, act)
    )


def keep_body(t, ins, outs, scr):
    gate_ref, up_ref, down_ref = outs

    def store(q, both, down):
        lent = now(ins[15])
        gate_ref[q] = both[:, 0:256] + lent[q].astype(F32)
        up_ref[q] = both[:, 256:512] + lent[4 + q].astype(F32)
        for half in range(2):
            cols = slice(256 * half, 256 * half + 256)
            at = pl.ds(pl.multiple_of(q * 512 + 256 * half, 256), 256)
            down_ref[:, at] = down[:, cols] + lent[8 + q, cols, :].astype(F32)

    each_quarter(ins, scr, slice(0, 256), store)


def keep(tp, xs, cs, gg, gu, act, lent):
    return weights_call(
        keep_body,
        (shape((4, 512, 256), F32), shape((4, 512, 256), F32), shape((256, 2048), F32)),
        tp,
        (*xs, *cs, gg, gu, act, lent),
    )


def hand_out_body(t, ins, outs, scr):
    proj = now(ins[0])
    for d in range(4):
        other = lax.bitwise_xor(t, 2 * d + 1)
        outs[0][d] = proj[:, pl.ds(pl.multiple_of(other * 256, 256), 256)]
    outs[0][4] = ins[1][...]


def hand_out(tp, proj, saved):
    return call(
        hand_out_body, shape((5, 64, TOK), BF), tp, (proj, saved), staged=(0,), limit=16
    )


def hand_on_body(t, ins, outs, scr):
    proj = now(ins[0])
    for d in range(1, 4):
        other = lax.bitwise_xor(t, 2 * d)
        outs[d - 1][0] = proj[:, pl.ds(pl.multiple_of(other * 256, 256), 256)]
        outs[d - 1][1] = ins[2][d]
        outs[d - 1][2] = ins[1][...]
        outs[d - 1][3] = ins[2][4]


def hand_on(tp, proj, saved, got):
    return call(
        hand_on_body,
        (shape((4, 64, TOK), BF),) * 3,
        tp,
        (proj, saved, got),
        staged=(0,),
        limit=16,
    )


def prepare_body(t, ins, outs, scr):
    proj_ref, mixed_ref, slope_ref, slope_n_ref, stat_ref = outs
    all_saved = scr[0]

    def at(d):
        return pl.ds(pl.multiple_of(lax.bitwise_xor(t, d) * 64, 64), 64)

    proj_ref[at(0), :] = now(ins[0])[...]
    all_saved[at(0), :] = ins[1][...]
    proj_ref[at(1), :] = ins[2][0]
    all_saved[at(1), :] = ins[2][4]
    for d in range(1, 4):
        for other in range(2):
            proj_ref[at(2 * d + other), :] = ins[2 + d][other]
            all_saved[at(2 * d + other), :] = ins[2 + d][2 + other]
    saved = all_saved[...].astype(F32)
    mean = jnp.sum(saved, axis=0, keepdims=True) / CW
    var = jnp.sum(saved * saved, axis=0, keepdims=True) / CW - mean * mean
    inv = lax.rsqrt(var + EPS)
    normed = (saved - mean) * inv
    sig = jax.nn.sigmoid(normed)
    mixed_ref[...] = (normed * sig).astype(BF)
    slope = sig * (1.0 + normed * (1.0 - sig))
    slope_ref[...] = slope
    slope_n_ref[...] = slope * normed
    stat_ref[...] = jnp.concatenate([mean, inv, mean, inv, mean, inv, mean, inv], axis=0)


def prepare(tp, proj, saved, got):
    return call(
        prepare_body,
        (
            pltpu.HBM((CW, TOK), BF),
            pltpu.HBM((CW, TOK), BF),
            pltpu.HBM((CW, TOK), F32),
            pltpu.HBM((CW, TOK), F32),
            shape((8, TOK), F32),
        ),
        tp,
        (proj, saved, *got),
        staged=(0,),
        cuts={0: ((64, TOK), columns_of(256, lambda t: t))},
        scratch=[pltpu.VMEM((CW, TOK), BF)],
        flops=10**8,
    )


def tokens_body(t, ins, outs, scr):
    gs_ref, outer_ref, own_ref, lent_ref = outs
    routed = dot(now(ins[0])[...], now(ins[2])[...])
    gs = (now(ins[1])[...].astype(F32) + routed).astype(BF)
    gs_ref[...] = gs
    outer = dot(gs, now(ins[4])[...], 0, 1)
    lane = iota((64, 128), 1) < 64
    for u in range(4):
        for i in range(4):
            block = outer[64 * i : 64 * i + 64, 128 * u : 128 * u + 128]
            turned = pltpu.roll(block, 64, 1)
            even = jnp.where(lane[0:32], block[0:32], turned[32:64])
            odd = jnp.where(lane[0:32], turned[0:32], block[32:64])
            outer_ref[8 * u + i] = even.astype(BF)
            outer_ref[8 * u + 4 + i] = odd.astype(BF)
    part_all = scr[0]
    part = dot(now(ins[3])[...], gs, 1, 1)
    part_all[...] = part
    first = jnp.sum(part * now(ins[5])[...], axis=0, keepdims=True)
    second = jnp.sum(part * now(ins[6])[...], axis=0, keepdims=True)
    sums = jnp.concatenate([first, second], axis=0)
    parted = split_sums(sums)

    def at(d):
        return pl.ds(pl.multiple_of(lax.bitwise_xor(t, d) * 64, 64), 64)

    for d in range(4):
        own_ref[d, 0:64, :] = part_all[at(2 * d), :]
        lent_ref[d, 0:64, :] = part_all[at(2 * d + 1), :].astype(BF)
        lent_ref[d, 64:72, :] = parted
    own_ref[0, 64:72, :] = jnp.concatenate([sums] * 4, axis=0)


def split_sums(sums):
    high = sums.astype(BF).astype(F32)
    low = sums - high
    return jnp.concatenate([high, low, high, low], axis=0).astype(BF)


def fold_body(t, ins, outs, scr):
    own, got = ins
    sums = own[0, 64:66, :] + got[0, 64:66, :].astype(F32) + got[0, 66:68, :].astype(F32)
    outs[0][0:64, :] = own[0, 0:64, :] + got[0, 0:64, :].astype(F32)
    outs[0][64:72, :] = jnp.concatenate([sums] * 4, axis=0)
    parted = split_sums(sums)
    for d in range(1, 4):
        outs[d][0:64, :] = (own[d, 0:64, :] + got[d, 0:64, :].astype(F32)).astype(BF)
        outs[d][64:72, :] = parted


def fold(tp, own, got):
    return call(
        fold_body,
        (shape((72, TOK), F32),) + (shape((72, TOK), BF),) * 3,
        tp,
        (own, got),
        flops=10**7,
        limit=16,
    )


def tokens(tp, back, upstream, ret, proj, mixed, slope, slope_n):
    return call(
        tokens_body,
        (
            shape((TOK, 256), BF),
            pltpu.HBM((SP, 32, 128), BF),
            shape((4, 72, TOK), F32),
            shape((4, 72, TOK), BF),
        ),
        tp,
        (back, upstream, ret, proj, mixed, slope, slope_n),
        staged=(0, 2, 1, 4, 3, 5, 6),
        cuts={1: ((TOK, 256), columns_of(256, lambda t: t))},
        scratch=[pltpu.VMEM((CW, TOK), F32)],
        flops=10**9,
    )


def norm_body(t, ins, outs, scr):
    own, saved, stat = ins[0], ins[4], ins[5]
    mixed, sums = own[0:64, :], own[64:66, :]
    for got in ins[1:4]:
        mixed = mixed + got[0:64, :].astype(F32)
        sums = sums + got[64:66, :].astype(F32) + got[66:68, :].astype(F32)
    first, second = sums[0:1] / CW, sums[1:2] / CW
    mean, inv = stat[0:1, :], stat[1:2, :]
    normed = (saved[...].astype(F32) - mean) * inv
    sig = jax.nn.sigmoid(normed)
    grad = mixed * sig * (1.0 + normed * (1.0 - sig))
    conv_grad = inv * (grad - first - normed * second)
    outs[0][...] = conv_grad
    outs[1][...] = conv_grad[:, 0:128]


def norm(tp, own, got, saved, stat):
    return call(
        norm_body,
        (shape((64, TOK), F32), shape((64, 128), F32)),
        tp,
        (own, *got, saved, stat),
        flops=10**7,
        limit=16,
    )


def tap_sum(padded, taps):
    total = jnp.zeros((64, TOK), F32)
    width = padded.shape[1]
    for j in range(taps.shape[1]):
        turned = padded if j == 0 else pltpu.roll(padded, width - j, 1)
        total = total + taps[:, j : j + 1] * turned[:, 0:TOK]
    return total


def conv_own_body(t, ins, outs, scr):
    grad, taps = ins
    outs[0][...] = tap_sum(jnp.concatenate([grad[...], jnp.zeros((64, 128), F32)], axis=1), taps)


def conv_own(tp, grad, taps):
    return call(conv_own_body, shape((64, TOK), F32), tp, (grad, taps), flops=10**8, limit=16)


def conv_rim_body(t, ins, outs, scr):
    own, rim, taps, value, gate = ins
    dv_ref, dg_ref = outs
    both = jnp.concatenate([jnp.zeros((64, 128), F32), rim[...]], axis=1)
    reach = jnp.zeros((64, 128), F32)
    for j in range(1, taps.shape[1]):
        reach = reach + taps[:, j : j + 1] * pltpu.roll(both, TOK - j, 1)[:, 0:128]
    total = jnp.concatenate([own[:, 0:128], own[:, 128:256] + reach], axis=1)
    sig = jax.nn.sigmoid(gate[...].astype(F32))
    dv_ref[...] = (total * sig).astype(BF)
    dg_ref[...] = (total * value[...].astype(F32) * sig * (1.0 - sig)).astype(BF)


def conv_rim(tp, own, rim, taps, value, gate):
    return call(
        conv_rim_body,
        (shape((64, TOK), BF), shape((64, TOK), BF)),
        tp,
        (own, rim, taps, value, gate),
        flops=10**8,
        limit=16,
    )


def total_body(t, ins, outs, scr):
    whole = jnp.sum(ins[0][...].astype(F32), axis=0)
    outs[0][0:32, :] = whole[:, 0:64]
    outs[0][32:64, :] = whole[:, 64:128]


def total(tp, got):
    return call(total_body, shape((64, 64), F32), tp, (got,), flops=10**7, limit=16)


def moved(x, by):
    return lax.ppermute(x, "tp", [(i, (i + by) % TP) for i in range(TP)])


def swapped(x, by):
    return lax.ppermute(x, "tp", [(i, i ^ by) for i in range(TP)])


def across_moved(x, by):
    return lax.ppermute(x, "tp", [(i, ((i + by) % TP) ^ 1) for i in range(TP)])


def around(block):
    left, right = moved(block, 2), moved(block, -2)
    top, bottom = moved(left[:256], 2), moved(right[256:], -2)
    return block, left, right, top, bottom


def around_in_halves(block):
    upper, lower = block[:256], block[256:]
    left_upper, right_lower = moved(upper, 2), moved(lower, -2)
    left_lower, right_upper = moved(lower, 2), moved(upper, -2)
    top, bottom = moved(left_upper, 2), moved(right_lower, -2)
    return block, left_upper, left_lower, right_upper, right_lower, top, bottom


def exchange(x):
    return lax.all_to_all(x, "sp", 0, 0, tiled=True)


def after(x, *others):
    return lax.optimization_barrier((x, *others))[0]


def step(
    upstream, stream, routes, route_weights, glu_value, glu_gate, conv_taps, conv_saved,
    out_proj, expert_gate, expert_up, expert_down,
):
    tp = lax.axis_index("tp").reshape(1)
    weights = route_weights.T
    rows_out, target = pick_rows(tp, routes.T, stream, weights, upstream)
    rows_in = exchange(rows_out.reshape(SP, HALF, FIRST)).reshape(ROWS, FIRST)

    saved, proj = conv_saved.T, out_proj.T
    near_early = swapped(hand_out(tp, proj, saved), 1)
    far_early = hand_on(tp, proj, saved, near_early)
    early = (near_early, *(swapped(x, 2 * d + 2) for d, x in enumerate(far_early)))
    gate_own, up_own, down_own = expert_gate[0], expert_up[0], expert_down[0]
    gate_par, up_par, down_par = (swapped(w, 1) for w in (gate_own, up_own, down_own))

    cot_out, back = pick_cot(tp, target, weights, upstream)
    cot_out = after(cot_out, *early)
    cot_in = exchange(cot_out.reshape(SP, HALF, LATE))
    cot_in = cot_in.reshape(ROWS, LATE)
    proj_all, mixed, slope, slope_n, stat = prepare(tp, proj, saved, early)

    xs = around(rows_in)
    by_quarter = [w.reshape(4, 512, 256) for w in (gate_own, gate_par, up_own, up_par)]
    by_piece = [w.reshape(8, 256, 256) for w in (gate_own, gate_par, up_own, up_par)]
    sums = first(tp, xs[:3], by_quarter)
    act, a1, a2 = forward(tp, sums, xs[3:], by_quarter)

    cs = around_in_halves(cot_in)
    downs = (down_own, down_par)
    ga = three(tp, xs[:3], cs[:5], downs)
    far_top, far_bottom, gg, gu = backward(tp, (*xs[3:], *cs[5:]), ga, downs, a1, a2, by_piece)
    got_top, got_bottom = moved(far_top, 2), moved(far_bottom, -2)
    parts = near(tp, gg, gu, by_piece)
    rs, rc, ls, lc = merge(tp, got_top, got_bottom, parts[:4])
    lent = lend(tp, xs, cs, gg, gu, after(act, rs))
    came = (moved(rs, 2), moved(ls, -2), across_moved(rc, 2), across_moved(lc, -2))
    own_cross = swapped(parts[5], 1)
    summed = settle(
        tp, (after(parts[4], lent), came[0], came[1], own_cross, came[2], came[3])
    )
    returned = exchange(summed).reshape(SP * CAP, 256)
    grads = keep(tp, xs, cs, gg, gu, act, swapped(lent, 1))
    grad_gate_w, grad_up_w, grad_down_w = grads
    back = after(back, grad_down_w)

    made = tokens(tp, back, upstream, returned, proj_all, mixed, slope, slope_n)
    grad_stream, outer, own_part, lent_part = made
    outer_in = exchange(outer)
    lent_in = swapped(lent_part, 1)
    folded = fold(tp, own_part, lent_in)
    own_part = folded[0]
    part_in = tuple(swapped(x, 2 * d + 2) for d, x in enumerate(folded[1:]))
    grad_conv, rim = norm(tp, own_part, part_in, saved, stat)
    rim_in = lax.ppermute(rim, "sp", [(i, i - 1) for i in range(1, SP)])
    taps = conv_taps.T
    grad_glu = conv_own(tp, grad_conv, taps)
    grad_value, grad_gate = conv_rim(tp, grad_glu, rim_in, taps, glu_value.T, glu_gate.T)
    grad_out_proj = lax.ppermute(
        total(tp, outer_in),
        ("sp", "tp"),
        [
            ((4 * u + i) * TP + t, (4 * t + i) * TP + u)
            for i in range(4)
            for u in range(TP)
            for t in range(TP)
        ],
    )
    return (
        grad_stream,
        grad_value.T,
        grad_gate.T,
        grad_out_proj,
        grad_gate_w.reshape(1, 2048, 256),
        grad_up_w.reshape(1, 2048, 256),
        grad_down_w[None],
    )


def solution(mesh):
    in_specs = (
        P("sp", None),
        P("sp", None),
        P("sp", None),
        P("sp", None),
        P("sp", "tp"),
        P("sp", "tp"),
        P(None, "tp"),
        P("sp", "tp"),
        P(None, "tp"),
        P("sp", None, "tp"),
        P("sp", None, "tp"),
        P("sp", "tp", None),
    )
    out_specs = (
        P("sp", "tp"),
        P("sp", "tp"),
        P("sp", "tp"),
        P("sp", "tp"),
        P("sp", None, "tp"),
        P("sp", None, "tp"),
        P("sp", "tp", None),
    )
    return jax.shard_map(step, mesh=mesh, in_specs=in_specs, out_specs=out_specs, check_vma=False)
```

```python
import jax
import jax.numpy as jnp
from jax import lax
from jax.experimental import pallas as pl
from jax.experimental.pallas import tpu as pltpu
from jax.sharding import PartitionSpec as P

CLAMP = 7.0
ALPHA = 1.702
EPS = 1e-05
CW = 512
CAP = 32
HALF = 16
SP = 32
TP = 8
TOK = 256
ROWS = SP * HALF
EARLY = 128
LATE = 512 - EARLY
FIRST = 512 + EARLY
BF = jnp.bfloat16
F32 = jnp.float32
MIB = 1 << 20


def dot(a, b, ca=1, cb=0):
    return lax.dot_general(a, b, (((ca,), (cb,)), ((), ())), preferred_element_type=F32)


def flag(mask):
    return jnp.where(mask, 1.0, 0.0)


def iota(shape, dim):
    return lax.broadcasted_iota(jnp.int32, shape, dim)


class Later:
    def __init__(self, copies, buffer):
        self.copies, self.buffer = copies, buffer
        for copy in copies:
            copy.start()

    def now(self):
        for copy in self.copies:
            copy.wait()
        self.copies = []
        return self.buffer


def now(x):
    return x.now() if isinstance(x, Later) else x


def call(body, outs, tp, args, staged=(), cuts=None, into=None, scratch=(), flops=0, limit=40):
    cuts, into = cuts or {}, into or {}
    own = tuple(i for i in staged if i not in into)
    n_copies = sum(len(into[i]) if i in into else 1 for i in staged)
    single = not isinstance(outs, tuple)
    outs = (outs,) if single else outs
    n_in, n_out, n_scr = len(args), len(outs), len(scratch)

    def kernel(t_ref, *refs):
        ins, rest = list(refs[:n_in]), refs[n_in:]
        made, scr, buffers = rest[:n_out], rest[n_out : n_out + n_scr], rest[n_out + n_scr :]
        t, sems = t_ref[0], iter(range(n_copies))
        for i in staged:
            if i in into:
                pairs = [(ins[i].at[cut], scr[k].at[to(t)]) for cut, k, to in into[i]]
            else:
                source = ins[i].at[cuts[i][1](t)] if i in cuts else ins[i]
                pairs = [(source, buffers[own.index(i)])]
            copies = [
                pltpu.make_async_copy(source, target, buffers[-1].at[next(sems)])
                for source, target in pairs
            ]
            ins[i] = Later(copies, pairs[0][1])
        body(t_ref[0], ins, made, scr)
        for i in staged:
            now(ins[i])

    extra = [
        pltpu.VMEM(cuts[i][0] if i in cuts else args[i].shape, args[i].dtype) for i in own
    ]
    if staged:
        extra.append(pltpu.SemaphoreType.DMA((n_copies,)))
    args = tuple(
        pltpu.with_memory_space_constraint(x, pltpu.HBM) if i in staged else x
        for i, x in enumerate(args)
    )
    made = pl.pallas_call(
        kernel,
        out_shape=outs,
        in_specs=[SMEM] + [HBM if i in staged else VMEM for i in range(n_in)],
        out_specs=(VMEM,) * n_out,
        scratch_shapes=list(scratch) + extra,
        compiler_params=pltpu.CompilerParams(vmem_limit_bytes=limit * MIB),
        cost_estimate=pl.CostEstimate(flops=flops, bytes_accessed=MIB, transcendentals=0),
    )(tp, *args)
    return made[0] if single else made


def shape(dims, dtype):
    return jax.ShapeDtypeStruct(dims, dtype)


SMEM = pl.BlockSpec(memory_space=pltpu.SMEM)
VMEM = pl.BlockSpec(memory_space=pltpu.VMEM)
HBM = pl.BlockSpec(memory_space=pltpu.HBM)


def columns_of(width, which):
    return lambda t: (slice(None), pl.ds(pl.multiple_of(which(t) * width, width), width))


def pick_rows_body(t, ins, outs, scr):
    core = t % 2
    r = ins[0][...]
    r0, r1 = r[0:1, :], r[1:2, :]
    expert = iota((SP, TOK), 0)
    named0, named1 = expert == r0, expert == r1
    both = (flag(named0) + flag(named1)).astype(BF)
    before = flag(iota((TOK, TOK), 0) < iota((TOK, TOK), 1)).astype(BF)
    earlier = dot(both, before)
    slot0 = jnp.sum(jnp.where(named0, earlier, 0.0), axis=0, keepdims=True).astype(jnp.int32)
    slot1 = jnp.sum(jnp.where(named1, earlier, 0.0), axis=0, keepdims=True).astype(jnp.int32)
    l0 = jnp.where(slot0 // HALF == core, r0 * HALF + slot0 - HALF * core, -1)
    l1 = jnp.where(slot1 // HALF == core, r1 * HALF + slot1 - HALF * core, -1)
    b0 = r0 * CAP + (slot0 + HALF * core) % CAP
    b1 = r1 * CAP + (slot1 + HALF * core) % CAP
    outs[1][...] = jnp.concatenate([l0, l1, b0, b1, l0, l1, b0, b1], axis=0)
    place = iota((ROWS, TOK), 0)
    at0, at1 = place == l0, place == l1
    pick = flag(at0 | at1).astype(BF)
    w = ins[2][...]
    scale = jnp.where(at0, w[0:1, :], 0.0) + jnp.where(at1, w[1:2, :], 0.0)
    scale = jnp.sum(scale, axis=1, keepdims=True)
    outs[0][:, 0:512] = dot(pick, now(ins[1])[...]).astype(BF)
    outs[0][:, 512:FIRST] = (scale * dot(pick, now(ins[3])[...])).astype(BF)


def pick_rows(tp, routes, stream, weights, upstream):
    return call(
        pick_rows_body,
        (pltpu.HBM((ROWS, FIRST), BF), shape((8, TOK), jnp.int32)),
        tp,
        (routes, stream, weights, upstream),
        staged=(1, 3),
        cuts={
            1: ((TOK, 512), columns_of(512, lambda t: t // 2)),
            3: ((TOK, EARLY), columns_of(EARLY, lambda t: t // 2 * (512 // EARLY))),
        },
        flops=10**9,
    )


def pick_cot_body(t, ins, outs, scr):
    tgt, w = ins[0][...], ins[1][...]
    table = jnp.concatenate([tgt[2:4, :].astype(F32), w, tgt[2:4, :].astype(F32), w], axis=0)
    columns = jnp.transpose(jnp.concatenate([table] * 16, axis=0))
    up = now(ins[2])[...].astype(F32)
    cot0 = (columns[:, 2:3] * up).astype(BF)
    cot1 = (columns[:, 3:4] * up).astype(BF)
    place = iota((ROWS, TOK), 0)
    cot = dot(flag(place == tgt[0:1, :]).astype(BF), cot0)
    cot = cot + dot(flag(place == tgt[1:2, :]).astype(BF), cot1)
    outs[0][...] = cot.astype(BF)
    b0 = columns[:, 0:1].astype(jnp.int32)
    b1 = columns[:, 1:2].astype(jnp.int32)
    spot = iota((TOK, SP * CAP), 1)
    outs[1][...] = flag((spot == b0) | (spot == b1)).astype(BF)


def pick_cot(tp, target, weights, upstream):
    return call(
        pick_cot_body,
        (pltpu.HBM((ROWS, LATE), BF), pltpu.HBM((TOK, SP * CAP), BF)),
        tp,
        (target, weights, upstream),
        staged=(2,),
        cuts={
            2: (
                (TOK, LATE),
                lambda t: (slice(None), pl.ds(pl.multiple_of(t // 2 * 512 + EARLY, 128), LATE)),
            )
        },
        flops=10**9,
    )


def quarters(t):
    y = t // 2
    return y, (y + 3) % 4, (y + 1) % 4, (y + 2) % 4


def first_body(t, ins, outs, scr):
    q = quarters(t)
    x = [ref[:, 0:512] for ref in ins[0:3]]
    for j in range(2):
        cols = slice(256 * j, 256 * j + 256)
        for out, at in ((outs[0], 3), (outs[1], 5)):
            w = now(ins[at + j])
            out[:, cols] = sum(dot(x[i], w[q[i]]) for i in range(3))


def first(tp, near_blocks, weights):
    return call(
        first_body,
        (pltpu.HBM((ROWS, 512), F32),) * 2,
        tp,
        (*near_blocks, *weights),
        staged=(3, 5, 4, 6),
        flops=10**9,
        limit=32,
    )


def forward_body(t, ins, outs, scr):
    act_ref, a1_ref, a2_ref = outs
    pg, pu = scr
    top, bottom = now(ins[2])[...], now(ins[3])[...]
    for j in range(2):
        cols = slice(256 * j, 256 * j + 256)
        for into, at in ((pg, 4), (pu, 6)):
            w = now(ins[at + j])[0]
            into[0:256, cols] = dot(top, w)
            into[256:512, cols] = dot(bottom, w)
    gate_near, up_near = now(ins[0]), now(ins[1])

    @pl.loop(0, ROWS // 32)
    def _(i):
        at = pl.ds(pl.multiple_of(i * 32, 32), 32)
        gate_pre, up_pre = gate_near[at, :] + pg[at, :], up_near[at, :] + pu[at, :]
        capped = jnp.minimum(gate_pre, CLAMP)
        clipped = jnp.clip(up_pre, -CLAMP, CLAMP)
        sig = jax.nn.sigmoid(ALPHA * capped)
        gated = capped * sig
        act_ref[at, :] = (gated * (clipped + 1.0)).astype(BF)
        slope = sig + ALPHA * gated * (1.0 - sig)
        a1_ref[at, :] = jnp.where(gate_pre < CLAMP, (clipped + 1.0) * slope, 0.0)
        a2_ref[at, :] = jnp.where(jnp.abs(up_pre) < CLAMP, gated, 0.0)


def forward(tp, sums, far_blocks, weights):
    rows = ((256, 512), lambda t: (slice(None), pl.ds(0, 512)))
    quarter = ((1, 512, 256), lambda t: (pl.ds((t // 2 + 2) % 4, 1),))
    return call(
        forward_body,
        (pltpu.HBM((ROWS, 512), BF), shape((ROWS, 512), F32), shape((ROWS, 512), F32)),
        tp,
        (*sums, *far_blocks, *weights),
        staged=(2, 3, 4, 6, 5, 7, 0, 1),
        cuts={2: rows, 3: rows} | {i: quarter for i in range(4, 8)},
        scratch=[pltpu.VMEM((ROWS, 512), F32)] * 2,
        flops=2 * 10**9,
        limit=32,
    )


def partial_of(g, u, weights, piece):
    g0, g1, u0, u1 = weights
    return (
        dot(g[:, 0:256], g0[piece], 1, 1)
        + dot(g[:, 256:512], g1[piece], 1, 1)
        + dot(u[:, 0:256], u0[piece], 1, 1)
        + dot(u[:, 256:512], u1[piece], 1, 1)
    )


def down_columns(d, quarter):
    return d[:, pl.ds(pl.multiple_of(quarter * 512, 512), 512)]


def three_body(t, ins, outs, scr):
    q = quarters(t)
    early = [now(x) for x in ins[0:3]]
    upper, lower = slice(0, 256), slice(256, 512)

    def beside(block, rows, late):
        return jnp.concatenate([early[block][rows, :], late[...]], axis=1)

    own = beside(0, slice(None), ins[3])
    parts = [
        (q[1], upper, beside(1, upper, ins[4])),
        (q[1], lower, beside(1, lower, ins[5])),
        (q[2], upper, beside(2, upper, ins[6])),
        (q[2], lower, beside(2, lower, ins[7])),
    ]
    for j in range(2):
        d = now(ins[8 + j])
        cols = slice(256 * j, 256 * j + 256)
        outs[0][:, cols] = dot(own, down_columns(d, q[0]), 1, 1)
        for at, rows, part in parts:
            outs[0][rows, cols] += dot(part, down_columns(d, at), 1, 1)


def three(tp, first, late, downs):
    early = ((ROWS, EARLY), lambda t: (slice(None), pl.ds(512, EARLY)))
    return call(
        three_body,
        shape((ROWS, 512), F32),
        tp,
        (*first, *late, *downs),
        staged=(0, 1, 2, 8, 9),
        cuts={0: early, 1: early, 2: early},
        flops=10**9,
        limit=32,
    )


def backward_body(t, ins, outs, scr):
    top_ref, bottom_ref, gg_ref, gu_ref = outs
    ga, a1, a2 = ins[4:7]
    top = jnp.concatenate([now(ins[0])[...], ins[2][...]], axis=1)
    bottom = jnp.concatenate([now(ins[1])[...], ins[3][...]], axis=1)
    far = scr[0]
    for j in range(2):
        d = now(ins[7 + j])[...]
        cols = slice(256 * j, 256 * j + 256)
        far[0:256, cols] = dot(top, d, 1, 1)
        far[256:512, cols] = dot(bottom, d, 1, 1)

    @pl.loop(0, ROWS // 32)
    def _(i):
        at = pl.ds(pl.multiple_of(i * 32, 32), 32)
        grad = ga[at, :] + far[at, :]
        gg_ref[at, :] = (grad * a1[at, :]).astype(BF)
        gu_ref[at, :] = (grad * a2[at, :]).astype(BF)

    g, u = gg_ref[...], gu_ref[...]
    weights = [now(w) for w in ins[9:13]]
    for half in range(2):
        part = partial_of(g, u, weights, half).astype(BF)
        top_ref[half] = part[0:256]
        bottom_ref[half] = part[256:512]


def backward(tp, far, ga, downs, a1, a2, weights):
    pieces = ((2, 256, 256), lambda t: (pl.ds(2 * ((t // 2 + 2) % 4), 2),))
    columns = ((256, 512), columns_of(512, lambda t: (t // 2 + 2) % 4))
    early = ((256, EARLY), lambda t: (slice(None), pl.ds(512, EARLY)))
    return call(
        backward_body,
        (
            shape((2, 256, 256), BF),
            shape((2, 256, 256), BF),
            shape((ROWS, 512), BF),
            shape((ROWS, 512), BF),
        ),
        tp,
        (*far, ga, a1, a2, *downs, *weights),
        staged=(0, 1, 7, 8, 9, 10, 11, 12),
        cuts={0: early, 1: early, 7: columns, 8: columns} | {i: pieces for i in range(9, 13)},
        scratch=[pltpu.VMEM((ROWS, 512), F32)],
        flops=2 * 10**9,
        limit=32,
    )


def near_body(t, ins, outs, scr):
    g, u = ins[0][...], ins[1][...]
    weights = [now(w) for w in ins[2:6]]
    right, left = (t + 2) % 8, (t + 6) % 8
    swap = 1 - 2 * (t % 2)
    pieces = (right, right + swap, left, left + swap, t, t + swap)
    for ref, piece in zip(outs, pieces):
        ref[...] = partial_of(g, u, weights, piece).astype(BF)


def near(tp, gg, gu, weights):
    return call(
        near_body,
        (shape((ROWS, 256), BF),) * 6,
        tp,
        (gg, gu, *weights),
        staged=(2, 3, 4, 5),
        flops=3 * 10**9,
    )


def merge_body(t, ins, outs, scr):
    core = t % 2
    top, bottom = ins[0:2]
    for src, dst, got, first in (
        (ins[2], outs[0], top[core], True),
        (ins[3], outs[1], top[1 - core], True),
        (ins[4], outs[2], bottom[core], False),
        (ins[5], outs[3], bottom[1 - core], False),
    ):
        hit, other = (slice(0, 256), slice(256, 512)) if first else (slice(256, 512), slice(0, 256))
        dst[hit, :] = (src[hit, :].astype(F32) + got.astype(F32)).astype(BF)
        dst[other, :] = src[other, :]


def merge(tp, top, bottom, parts):
    return call(
        merge_body, (shape((ROWS, 256), BF),) * 4, tp, (top, bottom, *parts), flops=10**7, limit=16
    )


def settle_body(t, ins, outs, scr):
    a0, a1, a2, b0, b1, b2 = [x[...].astype(F32) for x in ins]
    outs[0][:, 0:HALF, :] = (a0 + a1 + a2).astype(BF).reshape(SP, HALF, 256)
    outs[0][:, HALF:CAP, :] = (b0 + b1 + b2).astype(BF).reshape(SP, HALF, 256)


def settle(tp, parts):
    return call(settle_body, pltpu.HBM((SP, CAP, 256), BF), tp, parts, flops=10**7, limit=16)


def by_column():
    whole, upper, lower = slice(0, 512), slice(0, 256), slice(256, 512)
    every = slice(None)

    def place(by, rows, cols):
        return lambda t: ((t // 2 + by) % 4, rows, cols)

    into = {}
    for n, (by, rows) in enumerate(((0, whole), (3, whole), (1, whole), (2, upper), (2, lower))):
        into[n] = [
            ((every, pl.ds(0, 512)), 0, place(by, rows, every)),
            ((every, pl.ds(512, EARLY)), 1, place(by, rows, slice(0, EARLY))),
        ]
    places = ((0, whole), (3, upper), (3, lower), (1, upper), (1, lower), (2, upper), (2, lower))
    for n, (by, rows) in enumerate(places):
        into[5 + n] = [((every, every), 1, place(by, rows, slice(EARLY, 512)))]
    return into


def weights_call(body, outs, tp, args):
    return call(
        body,
        outs,
        tp,
        args,
        staged=tuple(range(len(args))),
        into=by_column(),
        scratch=[pltpu.VMEM((4, ROWS, 512), BF)] * 2,
        flops=2 * 10**9,
    )


def each_quarter(ins, scr, cols, store):
    ins = [now(x) for x in ins]
    gg, gu, act = ins[12:15]
    gu_cols = jnp.concatenate([gg[:, cols], gu[:, cols]], axis=1)
    act_cols = act[:, cols]

    @pl.loop(0, 4)
    def _(q):
        store(q, dot(scr[0][q], gu_cols, 0, 0), dot(act_cols, scr[1][q], 0, 0))


def lend_body(t, ins, outs, scr):
    def store(q, both, down):
        outs[0][q] = both[:, 0:256].astype(BF)
        outs[0][4 + q] = both[:, 256:512].astype(BF)
        outs[0][8 + q, 0:256, :] = down[:, 0:256].astype(BF)
        outs[0][8 + q, 256:512, :] = down[:, 256:512].astype(BF)

    each_quarter(ins, scr, slice(256, 512), store)


def lend(tp, xs, cs, gg, gu, act):
    return weights_call(
        lend_body, shape((12, 512, 256), BF), tp, (*xs, *cs, gg, gu, act)
    )


def keep_body(t, ins, outs, scr):
    gate_ref, up_ref, down_ref = outs

    def store(q, both, down):
        lent = now(ins[15])
        gate_ref[q] = both[:, 0:256] + lent[q].astype(F32)
        up_ref[q] = both[:, 256:512] + lent[4 + q].astype(F32)
        for half in range(2):
            cols = slice(256 * half, 256 * half + 256)
            at = pl.ds(pl.multiple_of(q * 512 + 256 * half, 256), 256)
            down_ref[:, at] = down[:, cols] + lent[8 + q, cols, :].astype(F32)

    each_quarter(ins, scr, slice(0, 256), store)


def keep(tp, xs, cs, gg, gu, act, lent):
    return weights_call(
        keep_body,
        (shape((4, 512, 256), F32), shape((4, 512, 256), F32), shape((256, 2048), F32)),
        tp,
        (*xs, *cs, gg, gu, act, lent),
    )


def hand_out_body(t, ins, outs, scr):
    proj = now(ins[0])
    for d in range(4):
        other = lax.bitwise_xor(t, 2 * d + 1)
        outs[0][d] = proj[:, pl.ds(pl.multiple_of(other * 256, 256), 256)]
    outs[0][4] = ins[1][...]


def hand_out(tp, proj, saved):
    return call(
        hand_out_body, shape((5, 64, TOK), BF), tp, (proj, saved), staged=(0,), limit=16
    )


def hand_on_body(t, ins, outs, scr):
    proj = now(ins[0])
    for d in range(1, 4):
        other = lax.bitwise_xor(t, 2 * d)
        outs[d - 1][0] = proj[:, pl.ds(pl.multiple_of(other * 256, 256), 256)]
        outs[d - 1][1] = ins[2][d]
        outs[d - 1][2] = ins[1][...]
        outs[d - 1][3] = ins[2][4]


def hand_on(tp, proj, saved, got):
    return call(
        hand_on_body,
        (shape((4, 64, TOK), BF),) * 3,
        tp,
        (proj, saved, got),
        staged=(0,),
        limit=16,
    )


def prepare_body(t, ins, outs, scr):
    proj_ref, mixed_ref, slope_ref, slope_n_ref, stat_ref = outs
    all_saved = scr[0]

    def at(d):
        return pl.ds(pl.multiple_of(lax.bitwise_xor(t, d) * 64, 64), 64)

    proj_ref[at(0), :] = now(ins[0])[...]
    all_saved[at(0), :] = ins[1][...]
    proj_ref[at(1), :] = ins[2][0]
    all_saved[at(1), :] = ins[2][4]
    for d in range(1, 4):
        for other in range(2):
            proj_ref[at(2 * d + other), :] = ins[2 + d][other]
            all_saved[at(2 * d + other), :] = ins[2 + d][2 + other]
    saved = all_saved[...].astype(F32)
    mean = jnp.sum(saved, axis=0, keepdims=True) / CW
    var = jnp.sum(saved * saved, axis=0, keepdims=True) / CW - mean * mean
    inv = lax.rsqrt(var + EPS)
    normed = (saved - mean) * inv
    sig = jax.nn.sigmoid(normed)
    mixed_ref[...] = (normed * sig).astype(BF)
    slope = sig * (1.0 + normed * (1.0 - sig))
    slope_ref[...] = slope
    slope_n_ref[...] = slope * normed
    stat_ref[...] = jnp.concatenate([mean, inv, mean, inv, mean, inv, mean, inv], axis=0)


def prepare(tp, proj, saved, got):
    return call(
        prepare_body,
        (
            pltpu.HBM((CW, TOK), BF),
            pltpu.HBM((CW, TOK), BF),
            pltpu.HBM((CW, TOK), F32),
            pltpu.HBM((CW, TOK), F32),
            shape((8, TOK), F32),
        ),
        tp,
        (proj, saved, *got),
        staged=(0,),
        cuts={0: ((64, TOK), columns_of(256, lambda t: t))},
        scratch=[pltpu.VMEM((CW, TOK), BF)],
        flops=10**8,
    )


def tokens_body(t, ins, outs, scr):
    gs_ref, outer_ref, own_ref, lent_ref = outs
    routed = dot(now(ins[0])[...], now(ins[2])[...])
    gs = (now(ins[1])[...].astype(F32) + routed).astype(BF)
    gs_ref[...] = gs
    outer = dot(gs, now(ins[4])[...], 0, 1)
    lane = iota((64, 128), 1) < 64
    for u in range(4):
        for i in range(4):
            block = outer[64 * i : 64 * i + 64, 128 * u : 128 * u + 128]
            turned = pltpu.roll(block, 64, 1)
            even = jnp.where(lane[0:32], block[0:32], turned[32:64])
            odd = jnp.where(lane[0:32], turned[0:32], block[32:64])
            outer_ref[8 * u + i] = even.astype(BF)
            outer_ref[8 * u + 4 + i] = odd.astype(BF)
    part_all = scr[0]
    part = dot(now(ins[3])[...], gs, 1, 1)
    part_all[...] = part
    first = jnp.sum(part * now(ins[5])[...], axis=0, keepdims=True)
    second = jnp.sum(part * now(ins[6])[...], axis=0, keepdims=True)
    sums = jnp.concatenate([first, second], axis=0)
    parted = split_sums(sums)

    def at(d):
        return pl.ds(pl.multiple_of(lax.bitwise_xor(t, d) * 64, 64), 64)

    for d in range(4):
        own_ref[d, 0:64, :] = part_all[at(2 * d), :]
        lent_ref[d, 0:64, :] = part_all[at(2 * d + 1), :].astype(BF)
        lent_ref[d, 64:72, :] = parted
    own_ref[0, 64:72, :] = jnp.concatenate([sums] * 4, axis=0)


def split_sums(sums):
    high = sums.astype(BF).astype(F32)
    low = sums - high
    return jnp.concatenate([high, low, high, low], axis=0).astype(BF)


def fold_body(t, ins, outs, scr):
    own, got = ins
    sums = own[0, 64:66, :] + got[0, 64:66, :].astype(F32) + got[0, 66:68, :].astype(F32)
    outs[0][0:64, :] = own[0, 0:64, :] + got[0, 0:64, :].astype(F32)
    outs[0][64:72, :] = jnp.concatenate([sums] * 4, axis=0)
    parted = split_sums(sums)
    for d in range(1, 4):
        outs[d][0:64, :] = (own[d, 0:64, :] + got[d, 0:64, :].astype(F32)).astype(BF)
        outs[d][64:72, :] = parted


def fold(tp, own, got):
    return call(
        fold_body,
        (shape((72, TOK), F32),) + (shape((72, TOK), BF),) * 3,
        tp,
        (own, got),
        flops=10**7,
        limit=16,
    )


def tokens(tp, back, upstream, ret, proj, mixed, slope, slope_n):
    return call(
        tokens_body,
        (
            shape((TOK, 256), BF),
            pltpu.HBM((SP, 32, 128), BF),
            shape((4, 72, TOK), F32),
            shape((4, 72, TOK), BF),
        ),
        tp,
        (back, upstream, ret, proj, mixed, slope, slope_n),
        staged=(0, 2, 1, 4, 3, 5, 6),
        cuts={1: ((TOK, 256), columns_of(256, lambda t: t))},
        scratch=[pltpu.VMEM((CW, TOK), F32)],
        flops=10**9,
    )


def norm_body(t, ins, outs, scr):
    own, saved, stat = ins[0], ins[4], ins[5]
    mixed, sums = own[0:64, :], own[64:66, :]
    for got in ins[1:4]:
        mixed = mixed + got[0:64, :].astype(F32)
        sums = sums + got[64:66, :].astype(F32) + got[66:68, :].astype(F32)
    first, second = sums[0:1] / CW, sums[1:2] / CW
    mean, inv = stat[0:1, :], stat[1:2, :]
    normed = (saved[...].astype(F32) - mean) * inv
    sig = jax.nn.sigmoid(normed)
    grad = mixed * sig * (1.0 + normed * (1.0 - sig))
    conv_grad = inv * (grad - first - normed * second)
    outs[0][...] = conv_grad
    outs[1][...] = conv_grad[:, 0:128]


def norm(tp, own, got, saved, stat):
    return call(
        norm_body,
        (shape((64, TOK), F32), shape((64, 128), F32)),
        tp,
        (own, *got, saved, stat),
        flops=10**7,
        limit=16,
    )


def tap_sum(padded, taps):
    total = jnp.zeros((64, TOK), F32)
    width = padded.shape[1]
    for j in range(taps.shape[1]):
        turned = padded if j == 0 else pltpu.roll(padded, width - j, 1)
        total = total + taps[:, j : j + 1] * turned[:, 0:TOK]
    return total


def conv_own_body(t, ins, outs, scr):
    grad, taps = ins
    outs[0][...] = tap_sum(jnp.concatenate([grad[...], jnp.zeros((64, 128), F32)], axis=1), taps)


def conv_own(tp, grad, taps):
    return call(conv_own_body, shape((64, TOK), F32), tp, (grad, taps), flops=10**8, limit=16)


def conv_rim_body(t, ins, outs, scr):
    own, rim, taps, value, gate = ins
    dv_ref, dg_ref = outs
    both = jnp.concatenate([jnp.zeros((64, 128), F32), rim[...]], axis=1)
    reach = jnp.zeros((64, 128), F32)
    for j in range(1, taps.shape[1]):
        reach = reach + taps[:, j : j + 1] * pltpu.roll(both, TOK - j, 1)[:, 0:128]
    total = jnp.concatenate([own[:, 0:128], own[:, 128:256] + reach], axis=1)
    sig = jax.nn.sigmoid(gate[...].astype(F32))
    dv_ref[...] = (total * sig).astype(BF)
    dg_ref[...] = (total * value[...].astype(F32) * sig * (1.0 - sig)).astype(BF)


def conv_rim(tp, own, rim, taps, value, gate):
    return call(
        conv_rim_body,
        (shape((64, TOK), BF), shape((64, TOK), BF)),
        tp,
        (own, rim, taps, value, gate),
        flops=10**8,
        limit=16,
    )


def total_body(t, ins, outs, scr):
    whole = jnp.sum(ins[0][...].astype(F32), axis=0)
    outs[0][0:32, :] = whole[:, 0:64]
    outs[0][32:64, :] = whole[:, 64:128]


def total(tp, got):
    return call(total_body, shape((64, 64), F32), tp, (got,), flops=10**7, limit=16)


def moved(x, by):
    return lax.ppermute(x, "tp", [(i, (i + by) % TP) for i in range(TP)])


def swapped(x, by):
    return lax.ppermute(x, "tp", [(i, i ^ by) for i in range(TP)])


def across_moved(x, by):
    return lax.ppermute(x, "tp", [(i, ((i + by) % TP) ^ 1) for i in range(TP)])


def around(block):
    left, right = moved(block, 2), moved(block, -2)
    top, bottom = moved(left[:256], 2), moved(right[256:], -2)
    return block, left, right, top, bottom


def around_in_halves(block):
    upper, lower = block[:256], block[256:]
    left_upper, right_lower = moved(upper, 2), moved(lower, -2)
    left_lower, right_upper = moved(lower, 2), moved(upper, -2)
    top, bottom = moved(left_upper, 2), moved(right_lower, -2)
    return block, left_upper, left_lower, right_upper, right_lower, top, bottom


def exchange(x):
    return lax.all_to_all(x, "sp", 0, 0, tiled=True)


def after(x, *others):
    return lax.optimization_barrier((x, *others))[0]


def step(
    upstream, stream, routes, route_weights, glu_value, glu_gate, conv_taps, conv_saved,
    out_proj, expert_gate, expert_up, expert_down,
):
    tp = lax.axis_index("tp").reshape(1)
    weights = route_weights.T
    rows_out, target = pick_rows(tp, routes.T, stream, weights, upstream)
    rows_in = exchange(rows_out.reshape(SP, HALF, FIRST)).reshape(ROWS, FIRST)

    saved, proj = conv_saved.T, out_proj.T
    near_early = swapped(hand_out(tp, proj, saved), 1)
    far_early = hand_on(tp, proj, saved, near_early)
    early = (near_early, *(swapped(x, 2 * d + 2) for d, x in enumerate(far_early)))
    gate_own, up_own, down_own = expert_gate[0], expert_up[0], expert_down[0]
    gate_par, up_par, down_par = (swapped(w, 1) for w in (gate_own, up_own, down_own))

    cot_out, back = pick_cot(tp, target, weights, upstream)
    cot_out = after(cot_out, *early)
    cot_in = exchange(cot_out.reshape(SP, HALF, LATE))
    cot_in = cot_in.reshape(ROWS, LATE)
    proj_all, mixed, slope, slope_n, stat = prepare(tp, proj, saved, early)

    xs = around(rows_in)
    by_quarter = [w.reshape(4, 512, 256) for w in (gate_own, gate_par, up_own, up_par)]
    by_piece = [w.reshape(8, 256, 256) for w in (gate_own, gate_par, up_own, up_par)]
    sums = first(tp, xs[:3], by_quarter)
    act, a1, a2 = forward(tp, sums, xs[3:], by_quarter)

    cs = around_in_halves(cot_in)
    downs = (down_own, down_par)
    ga = three(tp, xs[:3], cs[:5], downs)
    far_top, far_bottom, gg, gu = backward(tp, (*xs[3:], *cs[5:]), ga, downs, a1, a2, by_piece)
    got_top, got_bottom = moved(far_top, 2), moved(far_bottom, -2)
    parts = near(tp, gg, gu, by_piece)
    rs, rc, ls, lc = merge(tp, got_top, got_bottom, parts[:4])
    lent = lend(tp, xs, cs, gg, gu, after(act, rs))
    came = (moved(rs, 2), moved(ls, -2), across_moved(rc, 2), across_moved(lc, -2))
    own_cross = swapped(parts[5], 1)
    summed = settle(
        tp, (after(parts[4], lent), came[0], came[1], own_cross, came[2], came[3])
    )
    returned = exchange(summed).reshape(SP * CAP, 256)
    grads = keep(tp, xs, cs, gg, gu, act, swapped(lent, 1))
    grad_gate_w, grad_up_w, grad_down_w = grads
    back = after(back, grad_down_w)

    made = tokens(tp, back, upstream, returned, proj_all, mixed, slope, slope_n)
    grad_stream, outer, own_part, lent_part = made
    outer_in = exchange(outer)
    lent_in = swapped(lent_part, 1)
    folded = fold(tp, own_part, lent_in)
    own_part = folded[0]
    part_in = tuple(swapped(x, 2 * d + 2) for d, x in enumerate(folded[1:]))
    grad_conv, rim = norm(tp, own_part, part_in, saved, stat)
    rim_in = lax.ppermute(rim, "sp", [(i, i - 1) for i in range(1, SP)])
    taps = conv_taps.T
    grad_glu = conv_own(tp, grad_conv, taps)
    grad_value, grad_gate = conv_rim(tp, grad_glu, rim_in, taps, glu_value.T, glu_gate.T)
    grad_out_proj = lax.ppermute(
        total(tp, outer_in),
        ("sp", "tp"),
        [
            ((4 * u + i) * TP + t, (4 * t + i) * TP + u)
            for i in range(4)
            for u in range(TP)
            for t in range(TP)
        ],
    )
    return (
        grad_stream,
        grad_value.T,
        grad_gate.T,
        grad_out_proj,
        grad_gate_w.reshape(1, 2048, 256),
        grad_up_w.reshape(1, 2048, 256),
        grad_down_w[None],
    )


def solution(mesh):
    in_specs = (
        P("sp", None),
        P("sp", None),
        P("sp", None),
        P("sp", None),
        P("sp", "tp"),
        P("sp", "tp"),
        P(None, "tp"),
        P("sp", "tp"),
        P(None, "tp"),
        P("sp", None, "tp"),
        P("sp", None, "tp"),
        P("sp", "tp", None),
    )
    out_specs = (
        P("sp", "tp"),
        P("sp", "tp"),
        P("sp", "tp"),
        P("sp", "tp"),
        P("sp", None, "tp"),
        P("sp", None, "tp"),
        P("sp", "tp", None),
    )
    return jax.shard_map(step, mesh=mesh, in_specs=in_specs, out_specs=out_specs, check_vma=False)
```

```python
import jax
import jax.numpy as jnp
from jax import lax
from jax.experimental import pallas as pl
from jax.experimental.pallas import tpu as pltpu
from jax.sharding import PartitionSpec as P

CLAMP = 7.0
ALPHA = 1.702
EPS = 1e-05
CW = 512
CAP = 32
HALF = 16
SP = 32
TP = 8
TOK = 256
ROWS = SP * HALF
BF = jnp.bfloat16
F32 = jnp.float32
MIB = 1 << 20


def dot(a, b, ca=1, cb=0):
    return lax.dot_general(a, b, (((ca,), (cb,)), ((), ())), preferred_element_type=F32)


def flag(mask):
    return jnp.where(mask, 1.0, 0.0)


def iota(shape, dim):
    return lax.broadcasted_iota(jnp.int32, shape, dim)


class Later:
    def __init__(self, source, buffer, sem):
        self.copy, self.buffer, self.waiting = pltpu.make_async_copy(source, buffer, sem), buffer, True
        self.copy.start()

    def now(self):
        if self.waiting:
            self.copy.wait()
            self.waiting = False
        return self.buffer


def now(x):
    return x.now() if isinstance(x, Later) else x


def call(body, outs, tp, args, staged=(), cuts=None, into=None, scratch=(), flops=0, limit=40):
    cuts, into = cuts or {}, into or {}
    own = tuple(i for i in staged if i not in into)
    single = not isinstance(outs, tuple)
    outs = (outs,) if single else outs
    n_in, n_out, n_scr = len(args), len(outs), len(scratch)

    def kernel(t_ref, *refs):
        ins, rest = list(refs[:n_in]), refs[n_in:]
        made, scr, buffers = rest[:n_out], rest[n_out : n_out + n_scr], rest[n_out + n_scr :]
        for n, i in enumerate(staged):
            source = ins[i].at[cuts[i][1](t_ref[0])] if i in cuts else ins[i]
            if i in into:
                target = scr[into[i][0]].at[into[i][1](t_ref[0])]
            else:
                target = buffers[own.index(i)]
            ins[i] = Later(source, target, buffers[-1].at[n])
        body(t_ref[0], ins, made, scr)
        for i in staged:
            now(ins[i])

    extra = [
        pltpu.VMEM(cuts[i][0] if i in cuts else args[i].shape, args[i].dtype) for i in own
    ]
    if staged:
        extra.append(pltpu.SemaphoreType.DMA((len(staged),)))
    args = tuple(
        pltpu.with_memory_space_constraint(x, pltpu.HBM) if i in staged else x
        for i, x in enumerate(args)
    )
    made = pl.pallas_call(
        kernel,
        out_shape=outs,
        in_specs=[SMEM] + [HBM if i in staged else VMEM for i in range(n_in)],
        out_specs=(VMEM,) * n_out,
        scratch_shapes=list(scratch) + extra,
        compiler_params=pltpu.CompilerParams(vmem_limit_bytes=limit * MIB),
        cost_estimate=pl.CostEstimate(flops=flops, bytes_accessed=MIB, transcendentals=0),
    )(tp, *args)
    return made[0] if single else made


def shape(dims, dtype):
    return jax.ShapeDtypeStruct(dims, dtype)


SMEM = pl.BlockSpec(memory_space=pltpu.SMEM)
VMEM = pl.BlockSpec(memory_space=pltpu.VMEM)
HBM = pl.BlockSpec(memory_space=pltpu.HBM)


def columns_of(width, which):
    return lambda t: (slice(None), pl.ds(pl.multiple_of(which(t) * width, width), width))


def pick_rows_body(t, ins, outs, scr):
    core = t % 2
    r = ins[0][...]
    r0, r1 = r[0:1, :], r[1:2, :]
    expert = iota((SP, TOK), 0)
    named0, named1 = expert == r0, expert == r1
    both = (flag(named0) + flag(named1)).astype(BF)
    before = flag(iota((TOK, TOK), 0) < iota((TOK, TOK), 1)).astype(BF)
    earlier = dot(both, before)
    slot0 = jnp.sum(jnp.where(named0, earlier, 0.0), axis=0, keepdims=True).astype(jnp.int32)
    slot1 = jnp.sum(jnp.where(named1, earlier, 0.0), axis=0, keepdims=True).astype(jnp.int32)
    l0 = jnp.where(slot0 // HALF == core, r0 * HALF + slot0 - HALF * core, -1)
    l1 = jnp.where(slot1 // HALF == core, r1 * HALF + slot1 - HALF * core, -1)
    b0 = r0 * CAP + (slot0 + HALF * core) % CAP
    b1 = r1 * CAP + (slot1 + HALF * core) % CAP
    outs[1][...] = jnp.concatenate([l0, l1, b0, b1, l0, l1, b0, b1], axis=0)
    place = iota((ROWS, TOK), 0)
    pick = flag((place == l0) | (place == l1)).astype(BF)
    outs[0][...] = dot(pick, now(ins[1])[...]).astype(BF)


def pick_rows(tp, routes, stream):
    return call(
        pick_rows_body,
        (pltpu.HBM((ROWS, 512), BF), shape((8, TOK), jnp.int32)),
        tp,
        (routes, stream),
        staged=(1,),
        cuts={1: ((TOK, 512), columns_of(512, lambda t: t // 2))},
        flops=10**9,
    )


def pick_cot_body(t, ins, outs, scr):
    tgt, w = ins[0][...], ins[1][...]
    table = jnp.concatenate([tgt[2:4, :].astype(F32), w, tgt[2:4, :].astype(F32), w], axis=0)
    columns = jnp.transpose(jnp.concatenate([table] * 16, axis=0))
    up = now(ins[2])[...].astype(F32)
    cot0 = (columns[:, 2:3] * up).astype(BF)
    cot1 = (columns[:, 3:4] * up).astype(BF)
    place = iota((ROWS, TOK), 0)
    cot = dot(flag(place == tgt[0:1, :]).astype(BF), cot0)
    cot = cot + dot(flag(place == tgt[1:2, :]).astype(BF), cot1)
    outs[0][...] = cot.astype(BF)
    b0 = columns[:, 0:1].astype(jnp.int32)
    b1 = columns[:, 1:2].astype(jnp.int32)
    spot = iota((TOK, SP * CAP), 1)
    outs[1][...] = flag((spot == b0) | (spot == b1)).astype(BF)


def pick_cot(tp, target, weights, upstream):
    return call(
        pick_cot_body,
        (pltpu.HBM((ROWS, 512), BF), pltpu.HBM((TOK, SP * CAP), BF)),
        tp,
        (target, weights, upstream),
        staged=(2,),
        cuts={2: ((TOK, 512), columns_of(512, lambda t: t // 2))},
        flops=10**9,
    )


def quarters(t):
    y = t // 2
    return y, (y + 3) % 4, (y + 1) % 4, (y + 2) % 4


def first_body(t, ins, outs, scr):
    q = quarters(t)
    x = [ref[:, 0:512] for ref in ins[0:3]]
    for j in range(2):
        cols = slice(256 * j, 256 * j + 256)
        for out, at in ((outs[0], 3), (outs[1], 5)):
            w = now(ins[at + j])
            out[:, cols] = sum(dot(x[i], w[q[i]]) for i in range(3))


def first(tp, near_blocks, weights):
    return call(
        first_body,
        (pltpu.HBM((ROWS, 512), F32),) * 2,
        tp,
        (*near_blocks, *weights),
        staged=(3, 5, 4, 6),
        flops=10**9,
        limit=32,
    )


def forward_body(t, ins, outs, scr):
    act_ref, a1_ref, a2_ref = outs
    pg, pu = scr
    top, bottom = now(ins[2])[...], now(ins[3])[...]
    for j in range(2):
        cols = slice(256 * j, 256 * j + 256)
        for into, at in ((pg, 4), (pu, 6)):
            w = now(ins[at + j])[0]
            into[0:256, cols] = dot(top, w)
            into[256:512, cols] = dot(bottom, w)
    gate_near, up_near = now(ins[0]), now(ins[1])

    @pl.loop(0, ROWS // 32)
    def _(i):
        at = pl.ds(pl.multiple_of(i * 32, 32), 32)
        gate_pre, up_pre = gate_near[at, :] + pg[at, :], up_near[at, :] + pu[at, :]
        capped = jnp.minimum(gate_pre, CLAMP)
        clipped = jnp.clip(up_pre, -CLAMP, CLAMP)
        sig = jax.nn.sigmoid(ALPHA * capped)
        gated = capped * sig
        act_ref[at, :] = (gated * (clipped + 1.0)).astype(BF)
        slope = sig + ALPHA * gated * (1.0 - sig)
        a1_ref[at, :] = jnp.where(gate_pre < CLAMP, (clipped + 1.0) * slope, 0.0)
        a2_ref[at, :] = jnp.where(jnp.abs(up_pre) < CLAMP, gated, 0.0)


def forward(tp, sums, far_blocks, weights):
    rows = ((256, 512), lambda t: (slice(None), pl.ds(0, 512)))
    quarter = ((1, 512, 256), lambda t: (pl.ds((t // 2 + 2) % 4, 1),))
    return call(
        forward_body,
        (pltpu.HBM((ROWS, 512), BF), shape((ROWS, 512), F32), shape((ROWS, 512), F32)),
        tp,
        (*sums, *far_blocks, *weights),
        staged=(2, 3, 4, 6, 5, 7, 0, 1),
        cuts={2: rows, 3: rows} | {i: quarter for i in range(4, 8)},
        scratch=[pltpu.VMEM((ROWS, 512), F32)] * 2,
        flops=2 * 10**9,
        limit=32,
    )


def partial_of(g, u, weights, piece):
    g0, g1, u0, u1 = weights
    return (
        dot(g[:, 0:256], g0[piece], 1, 1)
        + dot(g[:, 256:512], g1[piece], 1, 1)
        + dot(u[:, 0:256], u0[piece], 1, 1)
        + dot(u[:, 256:512], u1[piece], 1, 1)
    )


def down_columns(d, quarter):
    return d[:, pl.ds(pl.multiple_of(quarter * 512, 512), 512)]


def three_body(t, ins, outs, scr):
    q = quarters(t)
    own = ins[0][...]
    sides = [(q[1], ins[1], ins[2]), (q[2], ins[3], ins[4])]
    for j in range(2):
        d = now(ins[5 + j])
        cols = slice(256 * j, 256 * j + 256)
        outs[0][:, cols] = dot(own, down_columns(d, q[0]), 1, 1)
        for at, upper, lower in sides:
            part = down_columns(d, at)
            outs[0][0:256, cols] += dot(upper[...], part, 1, 1)
            outs[0][256:512, cols] += dot(lower[...], part, 1, 1)


def three(tp, blocks, downs):
    return call(
        three_body,
        shape((ROWS, 512), F32),
        tp,
        (*blocks, *downs),
        staged=(5, 6),
        flops=10**9,
        limit=32,
    )


def backward_body(t, ins, outs, scr):
    top_ref, bottom_ref, gg_ref, gu_ref = outs
    top, bottom, ga, a1, a2 = ins[0:5]
    far = scr[0]
    for j in range(2):
        d = now(ins[5 + j])[...]
        cols = slice(256 * j, 256 * j + 256)
        far[0:256, cols] = dot(top[...], d, 1, 1)
        far[256:512, cols] = dot(bottom[...], d, 1, 1)

    @pl.loop(0, ROWS // 32)
    def _(i):
        at = pl.ds(pl.multiple_of(i * 32, 32), 32)
        grad = ga[at, :] + far[at, :]
        gg_ref[at, :] = (grad * a1[at, :]).astype(BF)
        gu_ref[at, :] = (grad * a2[at, :]).astype(BF)

    g, u = gg_ref[...], gu_ref[...]
    weights = [now(w) for w in ins[7:11]]
    for half in range(2):
        part = partial_of(g, u, weights, half).astype(BF)
        top_ref[half] = part[0:256]
        bottom_ref[half] = part[256:512]


def backward(tp, far, ga, downs, a1, a2, weights):
    pieces = ((2, 256, 256), lambda t: (pl.ds(2 * ((t // 2 + 2) % 4), 2),))
    columns = ((256, 512), columns_of(512, lambda t: (t // 2 + 2) % 4))
    return call(
        backward_body,
        (
            shape((2, 256, 256), BF),
            shape((2, 256, 256), BF),
            shape((ROWS, 512), BF),
            shape((ROWS, 512), BF),
        ),
        tp,
        (*far, ga, a1, a2, *downs, *weights),
        staged=(5, 6, 7, 8, 9, 10),
        cuts={5: columns, 6: columns} | {i: pieces for i in range(7, 11)},
        scratch=[pltpu.VMEM((ROWS, 512), F32)],
        flops=2 * 10**9,
        limit=32,
    )


def near_body(t, ins, outs, scr):
    g, u = ins[0][...], ins[1][...]
    weights = [now(w) for w in ins[2:6]]
    right, left = (t + 2) % 8, (t + 6) % 8
    swap = 1 - 2 * (t % 2)
    pieces = (right, right + swap, left, left + swap, t, t + swap)
    for ref, piece in zip(outs, pieces):
        ref[...] = partial_of(g, u, weights, piece).astype(BF)


def near(tp, gg, gu, weights):
    return call(
        near_body,
        (shape((ROWS, 256), BF),) * 6,
        tp,
        (gg, gu, *weights),
        staged=(2, 3, 4, 5),
        flops=3 * 10**9,
    )


def merge_body(t, ins, outs, scr):
    core = t % 2
    top, bottom = ins[0:2]
    for src, dst, got, first in (
        (ins[2], outs[0], top[core], True),
        (ins[3], outs[1], top[1 - core], True),
        (ins[4], outs[2], bottom[core], False),
        (ins[5], outs[3], bottom[1 - core], False),
    ):
        hit, other = (slice(0, 256), slice(256, 512)) if first else (slice(256, 512), slice(0, 256))
        dst[hit, :] = (src[hit, :].astype(F32) + got.astype(F32)).astype(BF)
        dst[other, :] = src[other, :]


def merge(tp, top, bottom, parts):
    return call(
        merge_body, (shape((ROWS, 256), BF),) * 4, tp, (top, bottom, *parts), flops=10**7, limit=16
    )


def settle_body(t, ins, outs, scr):
    a0, a1, a2, b0, b1, b2 = [x[...].astype(F32) for x in ins]
    outs[0][:, 0:HALF, :] = (a0 + a1 + a2).astype(BF).reshape(SP, HALF, 256)
    outs[0][:, HALF:CAP, :] = (b0 + b1 + b2).astype(BF).reshape(SP, HALF, 256)


def settle(tp, parts):
    return call(settle_body, pltpu.HBM((SP, CAP, 256), BF), tp, parts, flops=10**7, limit=16)


def by_column(scr_index, first, halves):
    whole, upper, lower = slice(None), slice(0, 256), slice(256, 512)
    sides = ((3, upper), (3, lower), (1, upper), (1, lower)) if halves else ((3, whole), (1, whole))
    places = ((0, whole), *sides, (2, upper), (2, lower))
    return {
        first + n: (scr_index, lambda t, by=by, rows=rows: ((t // 2 + by) % 4, rows))
        for n, (by, rows) in enumerate(places)
    }


def weights_call(body, outs, tp, args):
    return call(
        body,
        outs,
        tp,
        args,
        staged=tuple(range(len(args))),
        into=by_column(0, 0, False) | by_column(1, 5, True),
        scratch=[pltpu.VMEM((4, ROWS, 512), BF)] * 2,
        flops=2 * 10**9,
    )


def each_quarter(ins, scr, cols, store):
    ins = [now(x) for x in ins]
    gg, gu, act = ins[12:15]
    gu_cols = jnp.concatenate([gg[:, cols], gu[:, cols]], axis=1)
    act_cols = act[:, cols]

    @pl.loop(0, 4)
    def _(q):
        store(q, dot(scr[0][q], gu_cols, 0, 0), dot(act_cols, scr[1][q], 0, 0))


def lend_body(t, ins, outs, scr):
    def store(q, both, down):
        outs[0][q] = both[:, 0:256].astype(BF)
        outs[0][4 + q] = both[:, 256:512].astype(BF)
        outs[0][8 + q, 0:256, :] = down[:, 0:256].astype(BF)
        outs[0][8 + q, 256:512, :] = down[:, 256:512].astype(BF)

    each_quarter(ins, scr, slice(256, 512), store)


def lend(tp, xs, cs, gg, gu, act):
    return weights_call(
        lend_body, shape((12, 512, 256), BF), tp, (*xs, *cs, gg, gu, act)
    )


def keep_body(t, ins, outs, scr):
    gate_ref, up_ref, down_ref = outs

    def store(q, both, down):
        lent = now(ins[15])
        gate_ref[q] = both[:, 0:256] + lent[q].astype(F32)
        up_ref[q] = both[:, 256:512] + lent[4 + q].astype(F32)
        for half in range(2):
            cols = slice(256 * half, 256 * half + 256)
            at = pl.ds(pl.multiple_of(q * 512 + 256 * half, 256), 256)
            down_ref[:, at] = down[:, cols] + lent[8 + q, cols, :].astype(F32)

    each_quarter(ins, scr, slice(0, 256), store)


def keep(tp, xs, cs, gg, gu, act, lent):
    return weights_call(
        keep_body,
        (shape((4, 512, 256), F32), shape((4, 512, 256), F32), shape((256, 2048), F32)),
        tp,
        (*xs, *cs, gg, gu, act, lent),
    )


def hand_out_body(t, ins, outs, scr):
    proj = now(ins[0])
    for d in range(4):
        other = lax.bitwise_xor(t, 2 * d + 1)
        outs[0][d] = proj[:, pl.ds(pl.multiple_of(other * 256, 256), 256)]
    outs[0][4] = ins[1][...]


def hand_out(tp, proj, saved):
    return call(
        hand_out_body, shape((5, 64, TOK), BF), tp, (proj, saved), staged=(0,), limit=16
    )


def hand_on_body(t, ins, outs, scr):
    proj = now(ins[0])
    for d in range(1, 4):
        other = lax.bitwise_xor(t, 2 * d)
        outs[d - 1][0] = proj[:, pl.ds(pl.multiple_of(other * 256, 256), 256)]
        outs[d - 1][1] = ins[2][d]
        outs[d - 1][2] = ins[1][...]
        outs[d - 1][3] = ins[2][4]


def hand_on(tp, proj, saved, got):
    return call(
        hand_on_body,
        (shape((4, 64, TOK), BF),) * 3,
        tp,
        (proj, saved, got),
        staged=(0,),
        limit=16,
    )


def prepare_body(t, ins, outs, scr):
    proj_ref, mixed_ref, slope_ref, slope_n_ref, stat_ref = outs
    all_saved = scr[0]

    def at(d):
        return pl.ds(pl.multiple_of(lax.bitwise_xor(t, d) * 64, 64), 64)

    proj_ref[at(0), :] = now(ins[0])[...]
    all_saved[at(0), :] = ins[1][...]
    proj_ref[at(1), :] = ins[2][0]
    all_saved[at(1), :] = ins[2][4]
    for d in range(1, 4):
        for other in range(2):
            proj_ref[at(2 * d + other), :] = ins[2 + d][other]
            all_saved[at(2 * d + other), :] = ins[2 + d][2 + other]
    saved = all_saved[...].astype(F32)
    mean = jnp.sum(saved, axis=0, keepdims=True) / CW
    var = jnp.sum(saved * saved, axis=0, keepdims=True) / CW - mean * mean
    inv = lax.rsqrt(var + EPS)
    normed = (saved - mean) * inv
    sig = jax.nn.sigmoid(normed)
    mixed_ref[...] = (normed * sig).astype(BF)
    slope = sig * (1.0 + normed * (1.0 - sig))
    slope_ref[...] = slope
    slope_n_ref[...] = slope * normed
    stat_ref[...] = jnp.concatenate([mean, inv, mean, inv, mean, inv, mean, inv], axis=0)


def prepare(tp, proj, saved, got):
    return call(
        prepare_body,
        (
            pltpu.HBM((CW, TOK), BF),
            pltpu.HBM((CW, TOK), BF),
            pltpu.HBM((CW, TOK), F32),
            pltpu.HBM((CW, TOK), F32),
            shape((8, TOK), F32),
        ),
        tp,
        (proj, saved, *got),
        staged=(0,),
        cuts={0: ((64, TOK), columns_of(256, lambda t: t))},
        scratch=[pltpu.VMEM((CW, TOK), BF)],
        flops=10**8,
    )


def tokens_body(t, ins, outs, scr):
    gs_ref, outer_ref, own_ref, lent_ref = outs
    routed = dot(now(ins[0])[...], now(ins[2])[...])
    gs = (now(ins[1])[...].astype(F32) + routed).astype(BF)
    gs_ref[...] = gs
    outer = dot(gs, now(ins[4])[...], 0, 1)
    lane = iota((64, 128), 1) < 64
    for u in range(4):
        for i in range(4):
            block = outer[64 * i : 64 * i + 64, 128 * u : 128 * u + 128]
            turned = pltpu.roll(block, 64, 1)
            even = jnp.where(lane[0:32], block[0:32], turned[32:64])
            odd = jnp.where(lane[0:32], turned[0:32], block[32:64])
            outer_ref[8 * u + i] = even.astype(BF)
            outer_ref[8 * u + 4 + i] = odd.astype(BF)
    part_all = scr[0]
    part = dot(now(ins[3])[...], gs, 1, 1)
    part_all[...] = part
    first = jnp.sum(part * now(ins[5])[...], axis=0, keepdims=True)
    second = jnp.sum(part * now(ins[6])[...], axis=0, keepdims=True)
    sums = jnp.concatenate([first, second], axis=0)
    parted = split_sums(sums)

    def at(d):
        return pl.ds(pl.multiple_of(lax.bitwise_xor(t, d) * 64, 64), 64)

    for d in range(4):
        own_ref[d, 0:64, :] = part_all[at(2 * d), :]
        lent_ref[d, 0:64, :] = part_all[at(2 * d + 1), :].astype(BF)
        lent_ref[d, 64:72, :] = parted
    own_ref[0, 64:72, :] = jnp.concatenate([sums] * 4, axis=0)


def split_sums(sums):
    high = sums.astype(BF).astype(F32)
    low = sums - high
    return jnp.concatenate([high, low, high, low], axis=0).astype(BF)


def fold_body(t, ins, outs, scr):
    own, got = ins
    sums = own[0, 64:66, :] + got[0, 64:66, :].astype(F32) + got[0, 66:68, :].astype(F32)
    outs[0][0:64, :] = own[0, 0:64, :] + got[0, 0:64, :].astype(F32)
    outs[0][64:72, :] = jnp.concatenate([sums] * 4, axis=0)
    parted = split_sums(sums)
    for d in range(1, 4):
        outs[d][0:64, :] = (own[d, 0:64, :] + got[d, 0:64, :].astype(F32)).astype(BF)
        outs[d][64:72, :] = parted


def fold(tp, own, got):
    return call(
        fold_body,
        (shape((72, TOK), F32),) + (shape((72, TOK), BF),) * 3,
        tp,
        (own, got),
        flops=10**7,
        limit=16,
    )


def tokens(tp, back, upstream, ret, proj, mixed, slope, slope_n):
    return call(
        tokens_body,
        (
            shape((TOK, 256), BF),
            pltpu.HBM((SP, 32, 128), BF),
            shape((4, 72, TOK), F32),
            shape((4, 72, TOK), BF),
        ),
        tp,
        (back, upstream, ret, proj, mixed, slope, slope_n),
        staged=(0, 2, 1, 4, 3, 5, 6),
        cuts={1: ((TOK, 256), columns_of(256, lambda t: t))},
        scratch=[pltpu.VMEM((CW, TOK), F32)],
        flops=10**9,
    )


def norm_body(t, ins, outs, scr):
    own, saved, stat = ins[0], ins[4], ins[5]
    mixed, sums = own[0:64, :], own[64:66, :]
    for got in ins[1:4]:
        mixed = mixed + got[0:64, :].astype(F32)
        sums = sums + got[64:66, :].astype(F32) + got[66:68, :].astype(F32)
    first, second = sums[0:1] / CW, sums[1:2] / CW
    mean, inv = stat[0:1, :], stat[1:2, :]
    normed = (saved[...].astype(F32) - mean) * inv
    sig = jax.nn.sigmoid(normed)
    grad = mixed * sig * (1.0 + normed * (1.0 - sig))
    conv_grad = inv * (grad - first - normed * second)
    outs[0][...] = conv_grad
    outs[1][...] = conv_grad[:, 0:128]


def norm(tp, own, got, saved, stat):
    return call(
        norm_body,
        (shape((64, TOK), F32), shape((64, 128), F32)),
        tp,
        (own, *got, saved, stat),
        flops=10**7,
        limit=16,
    )


def tap_sum(padded, taps):
    total = jnp.zeros((64, TOK), F32)
    width = padded.shape[1]
    for j in range(taps.shape[1]):
        turned = padded if j == 0 else pltpu.roll(padded, width - j, 1)
        total = total + taps[:, j : j + 1] * turned[:, 0:TOK]
    return total


def conv_own_body(t, ins, outs, scr):
    grad, taps = ins
    outs[0][...] = tap_sum(jnp.concatenate([grad[...], jnp.zeros((64, 128), F32)], axis=1), taps)


def conv_own(tp, grad, taps):
    return call(conv_own_body, shape((64, TOK), F32), tp, (grad, taps), flops=10**8, limit=16)


def conv_rim_body(t, ins, outs, scr):
    own, rim, taps, value, gate = ins
    dv_ref, dg_ref = outs
    both = jnp.concatenate([jnp.zeros((64, 128), F32), rim[...]], axis=1)
    reach = jnp.zeros((64, 128), F32)
    for j in range(1, taps.shape[1]):
        reach = reach + taps[:, j : j + 1] * pltpu.roll(both, TOK - j, 1)[:, 0:128]
    total = jnp.concatenate([own[:, 0:128], own[:, 128:256] + reach], axis=1)
    sig = jax.nn.sigmoid(gate[...].astype(F32))
    dv_ref[...] = (total * sig).astype(BF)
    dg_ref[...] = (total * value[...].astype(F32) * sig * (1.0 - sig)).astype(BF)


def conv_rim(tp, own, rim, taps, value, gate):
    return call(
        conv_rim_body,
        (shape((64, TOK), BF), shape((64, TOK), BF)),
        tp,
        (own, rim, taps, value, gate),
        flops=10**8,
        limit=16,
    )


def total_body(t, ins, outs, scr):
    whole = jnp.sum(ins[0][...].astype(F32), axis=0)
    outs[0][0:32, :] = whole[:, 0:64]
    outs[0][32:64, :] = whole[:, 64:128]


def total(tp, got):
    return call(total_body, shape((64, 64), F32), tp, (got,), flops=10**7, limit=16)


def moved(x, by):
    return lax.ppermute(x, "tp", [(i, (i + by) % TP) for i in range(TP)])


def swapped(x, by):
    return lax.ppermute(x, "tp", [(i, i ^ by) for i in range(TP)])


def across_moved(x, by):
    return lax.ppermute(x, "tp", [(i, ((i + by) % TP) ^ 1) for i in range(TP)])


def around(block):
    left, right = moved(block, 2), moved(block, -2)
    top, bottom = moved(left[:256], 2), moved(right[256:], -2)
    return block, left, right, top, bottom


def around_in_halves(block):
    upper, lower = block[:256], block[256:]
    left_upper, right_lower = moved(upper, 2), moved(lower, -2)
    left_lower, right_upper = moved(lower, 2), moved(upper, -2)
    top, bottom = moved(left_upper, 2), moved(right_lower, -2)
    return block, left_upper, left_lower, right_upper, right_lower, top, bottom


def exchange(x):
    return lax.all_to_all(x, "sp", 0, 0, tiled=True)


def after(x, *others):
    return lax.optimization_barrier((x, *others))[0]


def step(
    upstream, stream, routes, route_weights, glu_value, glu_gate, conv_taps, conv_saved,
    out_proj, expert_gate, expert_up, expert_down,
):
    tp = lax.axis_index("tp").reshape(1)
    rows_out, target = pick_rows(tp, routes.T, stream)
    rows_in = exchange(rows_out.reshape(SP, HALF, 512)).reshape(ROWS, 512)

    saved, proj = conv_saved.T, out_proj.T
    near_early = swapped(hand_out(tp, proj, saved), 1)
    far_early = hand_on(tp, proj, saved, near_early)
    early = (near_early, *(swapped(x, 2 * d + 2) for d, x in enumerate(far_early)))
    gate_own, up_own, down_own = expert_gate[0], expert_up[0], expert_down[0]
    gate_par, up_par, down_par = (swapped(w, 1) for w in (gate_own, up_own, down_own))

    cot_out, back = pick_cot(tp, target, route_weights.T, upstream)
    cot_out = after(cot_out, *early)
    cot_in = exchange(cot_out.reshape(SP, HALF, 512))
    cot_in = cot_in.reshape(ROWS, 512)
    proj_all, mixed, slope, slope_n, stat = prepare(tp, proj, saved, early)

    xs = around(rows_in)
    by_quarter = [w.reshape(4, 512, 256) for w in (gate_own, gate_par, up_own, up_par)]
    by_piece = [w.reshape(8, 256, 256) for w in (gate_own, gate_par, up_own, up_par)]
    sums = first(tp, xs[:3], by_quarter)
    act, a1, a2 = forward(tp, sums, xs[3:], by_quarter)

    cs = around_in_halves(cot_in)
    downs = (down_own, down_par)
    ga = three(tp, cs[:5], downs)
    far_top, far_bottom, gg, gu = backward(tp, cs[5:], ga, downs, a1, a2, by_piece)
    got_top, got_bottom = moved(far_top, 2), moved(far_bottom, -2)
    parts = near(tp, gg, gu, by_piece)
    rs, rc, ls, lc = merge(tp, got_top, got_bottom, parts[:4])
    lent = lend(tp, xs, cs, gg, gu, after(act, rs))
    came = (moved(rs, 2), moved(ls, -2), across_moved(rc, 2), across_moved(lc, -2))
    own_cross = swapped(parts[5], 1)
    summed = settle(
        tp, (after(parts[4], lent), came[0], came[1], own_cross, came[2], came[3])
    )
    returned = exchange(summed).reshape(SP * CAP, 256)
    grads = keep(tp, xs, cs, gg, gu, act, swapped(lent, 1))
    grad_gate_w, grad_up_w, grad_down_w = grads
    back = after(back, grad_down_w)

    made = tokens(tp, back, upstream, returned, proj_all, mixed, slope, slope_n)
    grad_stream, outer, own_part, lent_part = made
    outer_in = exchange(outer)
    lent_in = swapped(lent_part, 1)
    folded = fold(tp, own_part, lent_in)
    own_part = folded[0]
    part_in = tuple(swapped(x, 2 * d + 2) for d, x in enumerate(folded[1:]))
    grad_conv, rim = norm(tp, own_part, part_in, saved, stat)
    rim_in = lax.ppermute(rim, "sp", [(i, i - 1) for i in range(1, SP)])
    taps = conv_taps.T
    grad_glu = conv_own(tp, grad_conv, taps)
    grad_value, grad_gate = conv_rim(tp, grad_glu, rim_in, taps, glu_value.T, glu_gate.T)
    grad_out_proj = lax.ppermute(
        total(tp, outer_in),
        ("sp", "tp"),
        [
            ((4 * u + i) * TP + t, (4 * t + i) * TP + u)
            for i in range(4)
            for u in range(TP)
            for t in range(TP)
        ],
    )
    return (
        grad_stream,
        grad_value.T,
        grad_gate.T,
        grad_out_proj,
        grad_gate_w.reshape(1, 2048, 256),
        grad_up_w.reshape(1, 2048, 256),
        grad_down_w[None],
    )


def solution(mesh):
    in_specs = (
        P("sp", None),
        P("sp", None),
        P("sp", None),
        P("sp", None),
        P("sp", "tp"),
        P("sp", "tp"),
        P(None, "tp"),
        P("sp", "tp"),
        P(None, "tp"),
        P("sp", None, "tp"),
        P("sp", None, "tp"),
        P("sp", "tp", None),
    )
    out_specs = (
        P("sp", "tp"),
        P("sp", "tp"),
        P("sp", "tp"),
        P("sp", "tp"),
        P("sp", None, "tp"),
        P("sp", None, "tp"),
        P("sp", "tp", None),
    )
    return jax.shard_map(step, mesh=mesh, in_specs=in_specs, out_specs=out_specs, check_vma=False)
```
